32 devices in a mesh: sp: 8 (over z, y), tp: 4 (over x, core).
Axes of the slice: x: 2, y: 2, z: 4, core: 2. Of those that a mesh axis runs over, the one named last changes fastest.
Arguments:
- skip_trunk_vector: bfloat16 [4096, 2048], P('sp', 'tp'), may hold values from -16 to 16
- valve_preactivation: bfloat16 [4096, 2048], P('sp', 'tp'), may hold values from -6 to 6
- projected_heads_payload: bfloat16 [4096, 2048], P('sp', 'tp'), may hold values from -6 to 6
- cluster_ingests: bfloat16 [4096, 1024], P('sp', 'tp'), may hold values from -6 to 6
- cluster_observers: bfloat16 [4096, 1024], P('sp', 'tp'), may hold values from -6 to 6
- pre_softplus_increments: float32 [2, 4096, 32], P(None, 'sp', 'tp'), may hold values from -6 to 6
- attenuation_ln_rate: float32 [2, 32], P(None, 'tp'), may hold values from -13 to -3
- additional_attenuation: float32 [2, 4096, 32], P(None, 'sp', 'tp'), may hold values from -3 to 0
- payload_conv_weights: float32 [7, 2048], P(None, 'tp'), may hold values from -2 to 2
- ingest_conv_weights: float32 [7, 1024], P(None, 'tp'), may hold values from -2 to 2
- observer_conv_weights: float32 [7, 1024], P(None, 'tp'), may hold values from -2 to 2
- valved_cluster_factor: float32 [2048], P('tp'), may hold values from 0.1 to 1.9
- closing_map_matrix: bfloat16 [2048, 2048], P('tp'), may hold values from -0.125 to 0.125
- dense_standardize_factor: float32 [2048], replicated, may hold values from 0.1 to 1.9
- dense_valve_map: bfloat16 [2048, 5120], P('sp', 'tp'), may hold values from -0.125 to 0.125
- dense_payload_map: bfloat16 [2048, 5120], P('sp', 'tp'), may hold values from -0.125 to 0.125
- valve_series_smoother: float32 [3, 5120], P(None, 'tp'), may hold values from -3.5 to 3.5
- payload_series_smoother: float32 [3, 5120], P(None, 'tp'), may hold values from -3.5 to 3.5
- dense_contract_map: bfloat16 [5120, 2048], P('tp', 'sp'), may hold values from -0.078125 to 0.078125
Outputs:
- updated: bfloat16 [4096, 2048], P('sp', 'tp')
The draws below stay inside these ranges and needn't reach their ends.
All inputs are finite; a program needn't handle non-finite values.
Results may differ from the reference program's by a relative error of at most 0.019.
Values may be sent and summed in bfloat16 or wider, within the bound.
A program may use at most 64 MiB of HBM per device.

```python
import jax
import jax.numpy as jnp
from jax import lax

TOK_DEV = 512
D = 2048
HEADS = 32
HEAD_DIM = 64
GROUPS = 8
STATE = 128
CONV = 7
FF = 5120
FF_TAPS = 3
MIXING_WIDTH = 2048
SEQUENCE_SPAN = 4096
N_TP = 4


def draw_skip_trunk_vector(key, part):
    column = jnp.arange(D, dtype=jnp.float32) / D
    scales = 0.5 * jnp.exp(jnp.log(5.0) * column)
    random_part = jax.random.truncated_normal(key, -6.0, 6.0, (SEQUENCE_SPAN, D), jnp.float32)
    return (random_part * scales).astype(jnp.bfloat16)


def draw_pre_softplus_increments(key, part):
    key_one, key_two = jax.random.split(key)
    blocks = SEQUENCE_SPAN // TOK_DEV
    offsets = jax.random.uniform(key_two, (2, blocks, 1, HEADS), jnp.float32, -1.2, 1.2)
    spread = jnp.broadcast_to(offsets, (2, blocks, TOK_DEV, HEADS)).reshape(2, SEQUENCE_SPAN, HEADS)
    random_part = jax.random.truncated_normal(key_one, -4.0, 4.0, (2, SEQUENCE_SPAN, HEADS), jnp.float32)
    return random_part + spread


def draw_attenuation_ln_rate(key, part):
    key_one, key_two, key_three = jax.random.split(key, 3)
    quick = jax.random.bernoulli(key_one, 0.5, (2, HEADS))
    slow_rate = jax.random.uniform(key_two, (2, HEADS), jnp.float32, 0.5, 1.0) * (0.6 / SEQUENCE_SPAN)
    fast_rate = jnp.exp(jax.random.uniform(key_three, (2, HEADS), jnp.float32, jnp.log(1.0 / 60.0), jnp.log(1.0 / 25.0)))
    return jnp.log(jnp.where(quick, fast_rate, slow_rate))


def draw_additional_attenuation(key, part):
    key_one, key_two = jax.random.split(key)
    places = jax.random.randint(key_one, (2, 4), 0, SEQUENCE_SPAN)
    kept_share = jax.random.uniform(key_two, (2, 4, HEADS), jnp.float32, 0.5, 0.8)
    position = jnp.arange(SEQUENCE_SPAN, dtype=jnp.int32)
    matches = (position[None, :, None] == places[:, None, :]).astype(jnp.float32)
    return jnp.einsum('dtk,dkh->dth', matches, jnp.log(kept_share))


def level_of(stream_key, extent, cuts, low, top_value):
    def one(axis_at, parts):
        heights = jax.random.uniform(jax.random.fold_in(jax.random.fold_in(stream_key, 6), axis_at), (parts,), jnp.float32, low / len(cuts), top_value / len(cuts))
        return jnp.repeat(jnp.exp(heights), extent[axis_at] // parts).reshape((-1,) + (1,) * (len(extent) - axis_at - 1))

    level = one(*cuts[0])
    for cut in cuts[1:]:
        level = level * one(*cut)
    return level


def noise(stream_key, extent, width, limit, cuts=(), held_as=jnp.bfloat16):
    factor_of = level_of(stream_key, extent, cuts, -0.22, 0.18) if cuts else 1.0
    array = jax.random.normal(stream_key, extent, jnp.float32) * width * factor_of
    return jnp.minimum(jnp.maximum(array, -limit), limit).astype(held_as)


def setup_inputs(seed: int = 0) -> dict:
    splits = jax.random.split(jax.random.key(seed), 20)
    return {
        "skip_trunk_vector": draw_skip_trunk_vector(jax.random.fold_in(splits[19], 71), 0),
        "valve_preactivation": noise(splits[1], (SEQUENCE_SPAN, MIXING_WIDTH), 1.0, 6.0, ((0, 8), (1, 4))),
        "projected_heads_payload": noise(splits[2], (SEQUENCE_SPAN, MIXING_WIDTH), 1.0, 6.0, ((0, 8), (1, 4))),
        "cluster_ingests": noise(splits[3], (SEQUENCE_SPAN, GROUPS * STATE), 1.0, 6.0, ((0, 8), (1, 4))),
        "cluster_observers": noise(splits[4], (SEQUENCE_SPAN, GROUPS * STATE), 1.0, 6.0, ((0, 8), (1, 4))),
        "pre_softplus_increments": draw_pre_softplus_increments(jax.random.fold_in(splits[19], 71), 0),
        "attenuation_ln_rate": draw_attenuation_ln_rate(jax.random.fold_in(splits[19], 71), 0),
        "additional_attenuation": draw_additional_attenuation(jax.random.fold_in(splits[19], 71), 0),
        "payload_conv_weights": noise(splits[8], (CONV, MIXING_WIDTH), CONV ** -0.5, 2.0, ((1, 4),), jnp.float32),
        "ingest_conv_weights": noise(splits[9], (CONV, GROUPS * STATE), CONV ** -0.5, 2.0, ((1, 4),), jnp.float32),
        "observer_conv_weights": noise(splits[10], (CONV, GROUPS * STATE), CONV ** -0.5, 2.0, ((1, 4),), jnp.float32),
        "valved_cluster_factor": jnp.clip(1.0 + 0.18 * jax.random.normal(splits[11], (MIXING_WIDTH,), jnp.float32), 0.1, 1.9),
        "closing_map_matrix": noise(splits[12], (MIXING_WIDTH, D), MIXING_WIDTH ** -0.5, 0.125, ((0, 4),)),
        "dense_standardize_factor": jnp.clip(1.0 + 0.18 * jax.random.normal(splits[13], (D,), jnp.float32), 0.1, 1.9),
        "dense_valve_map": noise(splits[14], (D, FF), D ** -0.5, 0.125, ((0, 8), (1, 4))),
        "dense_payload_map": noise(splits[15], (D, FF), D ** -0.5, 0.125, ((0, 8), (1, 4))),
        "valve_series_smoother": noise(splits[16], (FF_TAPS, FF), FF_TAPS ** -0.5, 3.5, ((1, 4),), jnp.float32),
        "payload_series_smoother": noise(splits[17], (FF_TAPS, FF), FF_TAPS ** -0.5, 3.5, ((1, 4),), jnp.float32),
        "dense_contract_map": noise(splits[18], (FF, D), FF ** -0.5, 0.078125, ((0, 4), (1, 8))),
    }


EPSILON = 1e-06

def centred_conv(data, kernel):
    margin = kernel.shape[0] // 2
    length = data.shape[0]
    padded = jnp.pad(data, ((margin, margin), (0, 0)))
    summed = padded[0:length] * kernel[0]
    for offset in range(1, kernel.shape[0]):
        summed = summed + padded[offset:offset + length] * kernel[offset]
    return summed

def one_way(values_f, inputs_h, readout_h, stride_lengths_change, fading_exponent):
    blocks = SEQUENCE_SPAN // TOK_DEV
    places = jnp.arange(TOK_DEV, dtype=jnp.int32)
    lower_mask = places[:, None] >= places[None, :]

    def advance(carried, pieces):
        block_values, block_inputs, block_readout, block_steps, block_logs = pieces
        running = jnp.cumsum(block_logs, axis=0)
        log_gaps = running.T[:, :, None] - running.T[:, None, :]
        decays = jnp.exp(jnp.where(lower_mask[None], log_gaps, -jnp.inf))
        scores = jnp.einsum('thn,shn->hts', block_readout, block_inputs, precision=lax.Precision.HIGHEST)
        weights = scores * decays * block_steps.T[:, None, :]
        within = jnp.einsum('hts,shp->thp', weights, block_values, precision=lax.Precision.HIGHEST)
        outer = jnp.einsum('thn,hpn->thp', block_readout, carried, precision=lax.Precision.HIGHEST)
        outer = outer * jnp.exp(running)[:, :, None]
        to_end = jnp.exp(running[-1][None, :] - running) * block_steps
        block_state = jnp.einsum('sh,shp,shn->hpn', to_end, block_values, block_inputs, precision=lax.Precision.HIGHEST)
        carried = carried * jnp.exp(running[-1])[:, None, None] + block_state
        return (carried, within + outer)
    pieces = (values_f.reshape(blocks, TOK_DEV, HEADS, HEAD_DIM), inputs_h.reshape(blocks, TOK_DEV, HEADS, STATE), readout_h.reshape(blocks, TOK_DEV, HEADS, STATE), stride_lengths_change.reshape(blocks, TOK_DEV, HEADS), fading_exponent.reshape(blocks, TOK_DEV, HEADS))
    start_state = jnp.zeros((HEADS, HEAD_DIM, STATE), jnp.float32)
    final_state, results = lax.scan(advance, start_state, pieces)
    return results.reshape(SEQUENCE_SPAN, HEADS, HEAD_DIM)

def split_product(left, right, part_width, out_width):

    def add_part(summed, index):
        start = index * part_width
        columns = lax.dynamic_slice_in_dim(left, start, part_width, 1)
        rows_part = lax.dynamic_slice_in_dim(right, start, part_width, 0)
        term = jnp.dot(columns, rows_part, preferred_element_type=jnp.float32).astype(jnp.bfloat16)
        return (summed + lax.optimization_barrier(term).astype(jnp.float32), index)
    zero_sum = jnp.zeros((left.shape[0], out_width), jnp.float32)
    summed, indices = lax.scan(add_part, zero_sum, jnp.arange(N_TP, dtype=jnp.int32))
    return summed

def reference(skip_trunk_vector, valve_preactivation, projected_heads_payload, cluster_ingests, cluster_observers, pre_softplus_increments, attenuation_ln_rate, additional_attenuation, payload_conv_weights, ingest_conv_weights, observer_conv_weights, valved_cluster_factor, closing_map_matrix, dense_standardize_factor, dense_valve_map, dense_payload_map, valve_series_smoother, payload_series_smoother, dense_contract_map):
    per_group = HEADS // GROUPS
    mixed_values = jax.nn.silu(centred_conv(projected_heads_payload.astype(jnp.float32), payload_conv_weights)).astype(jnp.bfloat16)
    mixed_inputs = jax.nn.silu(centred_conv(cluster_ingests.astype(jnp.float32), ingest_conv_weights)).astype(jnp.bfloat16)
    mixed_readout = jax.nn.silu(centred_conv(cluster_observers.astype(jnp.float32), observer_conv_weights)).astype(jnp.bfloat16)
    values_f = mixed_values.astype(jnp.float32).reshape(SEQUENCE_SPAN, HEADS, HEAD_DIM)
    inputs_h = jnp.repeat(mixed_inputs.astype(jnp.float32).reshape(SEQUENCE_SPAN, GROUPS, STATE), per_group, axis=1)
    readout_h = jnp.repeat(mixed_readout.astype(jnp.float32).reshape(SEQUENCE_SPAN, GROUPS, STATE), per_group, axis=1)
    stride_lengths_change = jax.nn.softplus(pre_softplus_increments)
    fading_exponent = additional_attenuation - stride_lengths_change * jnp.exp(attenuation_ln_rate)[:, None, :]
    forward = one_way(values_f, inputs_h, readout_h, stride_lengths_change[0], fading_exponent[0])
    backward = jnp.flip(one_way(jnp.flip(values_f, 0), jnp.flip(inputs_h, 0), jnp.flip(readout_h, 0), jnp.flip(stride_lengths_change[1], 0), jnp.flip(fading_exponent[1], 0)), 0)
    gated = (forward + backward).reshape(SEQUENCE_SPAN, MIXING_WIDTH) * jax.nn.silu(valve_preactivation.astype(jnp.float32))
    grouped = gated.reshape(SEQUENCE_SPAN, GROUPS, MIXING_WIDTH // GROUPS)
    standardized = grouped * lax.rsqrt(lax.optimization_barrier(jnp.mean(grouped * grouped, axis=2, keepdims=True)) + EPSILON)
    blending_result = (standardized.reshape(SEQUENCE_SPAN, MIXING_WIDTH) * valved_cluster_factor).astype(jnp.bfloat16)
    mapped_vector = split_product(blending_result, closing_map_matrix, MIXING_WIDTH // N_TP, D)
    intermediate_hidden = (skip_trunk_vector.astype(jnp.float32) + mapped_vector).astype(jnp.bfloat16)
    middle_f = intermediate_hidden.astype(jnp.float32)
    scaled = middle_f * lax.rsqrt(lax.optimization_barrier(jnp.mean(middle_f * middle_f, axis=1, keepdims=True)) + EPSILON)
    normed_rows = (scaled * dense_standardize_factor).astype(jnp.bfloat16)
    gate_rows = jnp.dot(normed_rows, dense_valve_map, preferred_element_type=jnp.float32).astype(jnp.bfloat16)
    value_rows = jnp.dot(normed_rows, dense_payload_map, preferred_element_type=jnp.float32).astype(jnp.bfloat16)
    gate_conv = centred_conv(gate_rows.astype(jnp.float32), valve_series_smoother)
    value_conv = centred_conv(value_rows.astype(jnp.float32), payload_series_smoother)
    hidden = (jax.nn.silu(gate_conv) * value_conv).astype(jnp.bfloat16)
    down_sum = split_product(hidden, dense_contract_map, FF // N_TP, D)
    return (middle_f + down_sum).astype(jnp.bfloat16)
```

```python
import functools
import math

import jax
import jax.numpy as jnp
from jax import lax
from jax.experimental import pallas as pl
from jax.experimental.pallas import tpu as pltpu
from jax.sharding import Mesh
from jax.sharding import PartitionSpec as P

HEADS = 32
GROUPS = 8
STATE = 128
EPSILON = 1e-06
SP = ("z", "y")
TP = ("x", "core")


def shifted(block, axis, step):
    count = lax.axis_size(axis)
    return lax.ppermute(block, axis, [(i, (i + step) % count) for i in range(count)])


def moved(block, axis, step):
    count = lax.axis_size(axis)
    pairs = [(i, i + step) for i in range(count) if 0 <= i + step < count]
    return lax.ppermute(block, axis, pairs)


def grid_shifted(block, axes, steps):
    sizes = [lax.axis_size(a) for a in axes]
    pairs = []
    for source in range(sizes[0] * sizes[1]):
        first, second = divmod(source, sizes[1])
        target = ((first + steps[0]) % sizes[0]) * sizes[1] + (second + steps[1]) % sizes[1]
        pairs.append((source, target))
    return lax.ppermute(block, axes, pairs)


def ordered(by_step, index):
    count = len(by_step)
    result = []
    for owner in range(count):
        back = lax.rem(index - owner + count, count)
        block = by_step[0]
        for step in range(1, count):
            block = jnp.where(back == step, by_step[step], block)
        result.append(block)
    return result


def extended(block, axis, width):
    low = moved(block[-width:], axis, 1)
    high = moved(block[:width], axis, -1)
    return jnp.concatenate([low, block, high], axis=0)


def conv_rows(padded, kernel, length):
    summed = padded[0:length] * kernel[0]
    for offset in range(1, kernel.shape[0]):
        summed = summed + padded[offset : offset + length] * kernel[offset]
    return summed


def bdot(pattern, one, two):
    return jnp.einsum(pattern, one, two, preferred_element_type=jnp.float32)


def pack(decay, state):
    heads, width, depth = state.shape
    rows = jnp.broadcast_to(decay[:, None, None], (heads, 16, depth)).astype(jnp.bfloat16)
    return jnp.concatenate([state.astype(jnp.bfloat16), rows], axis=1)


def unpack(packed, width):
    body = packed.astype(jnp.float32)
    return body[:, width, 0], body[:, :width]


def carried_in(decay, state, sign):
    width = state.shape[1]
    count = lax.axis_size(SP)
    own = pack(decay, state)
    index = lax.axis_index(SP)

    def from_back(array, step):
        back, value = unpack(moved(array, SP, sign * step), width)
        source = index - sign * step
        inside = (source >= 0) & (source < count)
        return jnp.where(inside, back, 1.0), value

    near, far = from_back(own, 1), from_back(own, 2)
    total = near[1] + near[0][:, None, None] * far[1]
    product = near[0] * far[0]
    covered = 2
    while covered < count - 1:
        back, value = from_back(pack(product, total), covered)
        total = total + product[:, None, None] * value
        product = product * back
        covered *= 2
    return total


def tied(value, *others):
    marks = [other[(slice(0, 1),) * other.ndim] for other in others]
    return lax.optimization_barrier((value, *marks))[0]


def shared_rows(weight, axis_dim, out_dim, mark):
    count = lax.axis_size("y")
    index = lax.axis_index("y")
    part = weight.shape[axis_dim] // count
    received = []
    for step in range(count):
        at = lax.rem(index + step, count) * part
        block = lax.dynamic_slice_in_dim(weight, at, part, axis_dim)
        received.append(shifted(block, "y", step) if step else block)
    received = [tied(block, mark) for block in received]
    return jnp.concatenate(ordered(received, index), axis=out_dim)


def shards(
    skip_trunk_vector,
    valve_preactivation,
    projected_heads_payload,
    cluster_ingests,
    cluster_observers,
    pre_softplus_increments,
    attenuation_ln_rate,
    additional_attenuation,
    payload_conv_weights,
    ingest_conv_weights,
    observer_conv_weights,
    valved_cluster_factor,
    closing_map_matrix,
    dense_standardize_factor,
    dense_valve_map,
    dense_payload_map,
    valve_series_smoother,
    payload_series_smoother,
    dense_contract_map,
):
    rows = skip_trunk_vector.shape[0]
    own_cols = skip_trunk_vector.shape[1]
    head_count = pre_softplus_increments.shape[2]
    per_group = HEADS // GROUPS
    nx, nc, ny = lax.axis_size("x"), lax.axis_size("core"), lax.axis_size("y")
    ix, ic, iy = lax.axis_index("x"), lax.axis_index("core"), lax.axis_index("y")

    joined = jnp.concatenate([projected_heads_payload, cluster_ingests, cluster_observers], axis=1)
    taps_all = jnp.concatenate(
        [payload_conv_weights, ingest_conv_weights, observer_conv_weights], axis=1
    )
    padded = extended(joined, SP, taps_all.shape[0] // 2)

    convolved = jax.nn.silu(conv_rows(padded.astype(jnp.float32), taps_all, rows)).astype(
        jnp.bfloat16
    )
    gate_w = lax.all_gather(shared_rows(dense_valve_map, 1, 0, convolved), "z", axis=0, tiled=True)
    value_w = lax.all_gather(
        shared_rows(dense_payload_map, 1, 0, convolved), "z", axis=0, tiled=True
    )

    payload_columns = projected_heads_payload.shape[1]
    input_cols = cluster_ingests.shape[1]
    width = payload_columns // head_count
    groups = input_cols // STATE
    values = convolved[:, :payload_columns]
    inputs_g = convolved[:, payload_columns : payload_columns + input_cols].reshape(
        rows, groups, STATE
    )
    readout_g = convolved[:, payload_columns + input_cols :].reshape(rows, groups, STATE)

    steps = jax.nn.softplus(pre_softplus_increments)
    logs = additional_attenuation - steps * jnp.exp(attenuation_ln_rate)[:, None, :]
    running = jnp.cumsum(logs, axis=1)
    run_f = running[0]
    exc_b = running[1] - logs[1]
    total_f, total_b = running[0, -1], running[1, -1]

    end_f = jnp.exp(total_f[None] - run_f) * steps[0]
    end_b = jnp.exp(exc_b) * steps[1]
    ends = jnp.stack([end_f, end_b], axis=1)
    scaled = (
        ends[:, :, :, None] * values.astype(jnp.float32).reshape(rows, 1, head_count, width)
    ).astype(jnp.bfloat16)
    scaled = scaled.reshape(rows, 2, groups, per_group, width)
    summary = bdot("sdgep,sgn->dgepn", scaled, inputs_g).reshape(2, head_count, width, STATE)
    in_f = carried_in(jnp.exp(total_f), summary[0], 1)
    in_b = carried_in(jnp.exp(total_b), summary[1], -1)

    down_part = shared_rows(dense_contract_map, 0, 1, in_f)
    down_w = lax.all_gather(down_part, "z", axis=1, tiled=True)

    places = jnp.arange(rows, dtype=jnp.int32)
    after = places[:, None] > places[None, :]
    same = places[:, None] == places[None, :]
    run_fT, exc_bT = run_f.T, exc_b.T
    step_f, step_b = steps[0].T, steps[1].T
    gaps = jnp.where(
        after[None],
        run_fT[:, :, None] - run_fT[:, None, :],
        exc_bT[:, None, :] - exc_bT[:, :, None],
    )
    factor = jnp.where(
        after[None],
        step_f[:, None, :],
        jnp.where(same[None], (step_f + step_b)[:, None, :], step_b[:, None, :]),
    )
    scores = jnp.repeat(bdot("tgn,sgn->gts", readout_g, inputs_g), per_group, axis=0)
    weights = (scores * jnp.exp(gaps) * factor).astype(jnp.bfloat16)
    within = bdot("hts,shp->thp", weights, values.reshape(rows, head_count, width))

    def outer(state):
        grouped = state.astype(jnp.bfloat16).reshape(groups, per_group, width, STATE)
        return bdot("gepn,tgn->tgep", grouped, readout_g).reshape(rows, head_count, width)

    mixed = within + outer(in_f) * jnp.exp(run_f)[:, :, None]
    mixed = mixed + outer(in_b) * jnp.exp(total_b[None] - exc_b)[:, :, None]
    gated = mixed.reshape(rows, payload_columns) * jax.nn.silu(
        valve_preactivation.astype(jnp.float32)
    )
    grouped = gated.reshape(rows, groups, per_group * width)
    standardized = grouped * lax.rsqrt(jnp.mean(grouped * grouped, axis=2, keepdims=True) + EPSILON)
    blended = (standardized.reshape(rows, payload_columns) * valved_cluster_factor).astype(
        jnp.bfloat16
    )

    def column_block(matrix, dx, dc):
        at = (lax.rem(ix + dx, nx) * nc + lax.rem(ic + dc, nc)) * own_cols
        return lax.dynamic_slice_in_dim(matrix, at, own_cols, 1)

    def over_cores(terms):
        total = terms[0].astype(jnp.bfloat16).astype(jnp.float32)
        for dc in range(1, nc):
            total = total + shifted(terms[dc].astype(jnp.bfloat16), "core", dc).astype(jnp.float32)
        return total

    mapped = None
    for dx in list(range(1, nx)) + [0]:
        terms = [
            jnp.dot(
                blended,
                column_block(closing_map_matrix, dx, dc),
                preferred_element_type=jnp.float32,
            )
            for dc in range(nc)
        ]
        part = over_cores(terms)
        if dx:
            part = shifted(part.astype(jnp.bfloat16), "x", dx).astype(jnp.float32)
        mapped = part if mapped is None else mapped + part
    middle = (skip_trunk_vector.astype(jnp.float32) + mapped).astype(jnp.bfloat16)

    margin = valve_series_smoother.shape[0] // 2
    room = -(-margin // 16) * 16
    low = moved(middle[-margin:], SP, 1)
    high = moved(middle[:margin], SP, -1)
    blank = jnp.zeros((room - margin, own_cols), middle.dtype)
    wide = jnp.concatenate([blank, low, middle, high, blank], axis=0)

    def everywhere(block):
        by_y = []
        for dy in range(ny):
            by_x = []
            for dx in range(nx):
                got = grid_shifted(block, ("y", "x"), (dy, dx)) if dy or dx else block
                by_core = [got] + [shifted(got, "core", dc) for dc in range(1, nc)]
                by_x.append(jnp.concatenate(ordered(by_core, ic), axis=1))
            by_y.append(jnp.concatenate(ordered(by_x, ix), axis=1))
        return jnp.stack(ordered(by_y, iy))

    line = everywhere(wide).reshape(ny * (rows + 2 * room), -1).astype(jnp.float32)
    inverse = lax.rsqrt(jnp.mean(line * line, axis=1, keepdims=True) + EPSILON)
    normed = (line * inverse * dense_standardize_factor).astype(jnp.bfloat16)

    hidden_cols = gate_w.shape[1]
    gate_taps = lax.dynamic_slice_in_dim(valve_series_smoother, iy * hidden_cols, hidden_cols, 1)
    value_taps = lax.dynamic_slice_in_dim(payload_series_smoother, iy * hidden_cols, hidden_cols, 1)

    def spread(weight, taps):
        made = jnp.dot(normed, weight, preferred_element_type=jnp.float32).astype(jnp.bfloat16)
        made = made.reshape(ny, rows + 2 * room, hidden_cols).astype(jnp.float32)
        summed = None
        for offset in range(taps.shape[0]):
            start = room - margin + offset
            term = made[:, start : start + rows] * taps[offset]
            summed = term if summed is None else summed + term
        return summed

    gate_rows = spread(gate_w, gate_taps)
    value_rows = spread(value_w, value_taps)
    hidden = (jax.nn.silu(gate_rows) * value_rows).astype(jnp.bfloat16)

    order = [(dy, dx) for dy in range(ny) for dx in range(nx)]
    down = None
    for dy, dx in order[1:] + order[:1]:
        wanted = lax.dynamic_index_in_dim(hidden, lax.rem(iy + dy, ny), 0, keepdims=False)
        terms = [
            jnp.dot(wanted, column_block(down_w, dx, dc), preferred_element_type=jnp.float32)
            for dc in range(nc)
        ]
        part = over_cores(terms)
        if dy or dx:
            part = grid_shifted(part.astype(jnp.bfloat16), ("y", "x"), (dy, dx)).astype(jnp.float32)
        down = part if down is None else down + part
    return (middle.astype(jnp.float32) + down).astype(jnp.bfloat16)


MESH = pl.DeviceIdType.MESH
BF = jnp.bfloat16
F32 = jnp.float32


def dot(one, two, dims=((1,), (0,)), precision=None):
    return lax.dot_general(
        one, two, (dims, ((), ())), preferred_element_type=F32, precision=precision
    )


def layer(
    skip,
    valve,
    payload,
    ingest,
    observe,
    pre,
    rate,
    extra,
    taps_p,
    taps_i,
    taps_o,
    gain,
    closing,
    norm_gain,
    gate_w,
    value_w,
    gate_taps,
    value_taps,
    down_w,
    out,
    halo,
    wide,
    conv,
    run_s,
    exc_s,
    run_t,
    exc_t,
    step_t,
    ends,
    scaled,
    sum_f,
    sum_h,
    sum_y,
    totals,
    plane_out,
    plane_in,
    carry,
    carry_all,
    entering,
    scores,
    mixed,
    skip_all,
    blend,
    close_all,
    rows_n,
    wg,
    wv,
    wd,
    made_g,
    made_v,
    hidden,
    part,
    part_f,
    part_in,
    own_sum,
    far_in,
    halo_s,
    halo_r,
    tp_s,
    tp_r,
    w_s,
    w_r,
    w_fwd,
    tot_s,
    tot_r,
    sy_s,
    sy_r,
    pl_s,
    pl_r,
    ca_s,
    ca_r,
    nr_s,
    nr_r,
    edge_s,
    edge_r,
    core_s,
    core_r,
    own_s,
    own_r,
    local,
):
    nz, ny, nx, nc = (lax.axis_size(a) for a in ("z", "y", "x", "core"))
    z, y, x, c = (lax.axis_index(a) for a in ("z", "y", "x", "core"))
    place, lane_at = z * ny + y, x * nc + c
    rows, cols = skip.shape
    width_all = skip_all.shape[1]
    heads = pre.shape[2]
    groups = ingest.shape[1] // STATE
    per = heads // groups
    head_w = payload.shape[1] // heads
    gw = per * head_w
    hid = wg.shape[1]
    kb = gate_w.shape[0]
    ob = down_w.shape[1]
    tile = 16
    other_y, other_x, other_c = (z, 1 - y, x, c), (z, y, 1 - x, c), (z, y, x, 1 - c)
    half = z // 2
    near = z * (1 - 2 * half) + (nz - 1) * half
    relay = near == 1
    far, end = (nz - 1) * (1 - half), (nz - 1) * half

    def remote(src, dst, send, recv, to):
        return pltpu.make_async_remote_copy(
            src_ref=src,
            dst_ref=dst,
            send_sem=send,
            recv_sem=recv,
            device_id=to,
            device_id_type=MESH,
        )

    barrier = pltpu.get_barrier_semaphore()
    greeted = 0
    for k in range(1, nz * ny):
        to = (lax.rem(z + k // ny, nz), lax.rem(y + k % ny, ny), x, c)
        pl.semaphore_signal(barrier, inc=1, device_id=to, device_id_type=MESH)
        greeted += 1
    for k in range(1, nx * nc):
        for dy in range(ny):
            to = (z, lax.rem(y + dy, ny), lax.rem(x + k // nc, nx), lax.rem(c + k % nc, nc))
            pl.semaphore_signal(barrier, inc=1, device_id=to, device_id_type=MESH)
            greeted += 1
    pl.semaphore_wait(barrier, greeted)

    pieces = []
    at = 0
    for source in (payload, ingest, observe):
        pieces.append((source, at, source.shape[1]))
        at += source.shape[1]

    def halo_copy(side, i):
        source, start, size = pieces[i]
        other = place + 1 if side == 0 else place - 1
        to = (other // ny, lax.rem(other + ny, ny), x, c)
        src = source.at[pl.ds(rows - tile, tile)] if side == 0 else source.at[pl.ds(0, tile)]
        return remote(
            src,
            halo.at[side, :, pl.ds(start, size)],
            halo_s.at[side, i],
            halo_r.at[side, i],
            to,
        )

    last = nz * ny - 1

    @pl.when(place < last)
    def _():
        for i in range(3):
            halo_copy(0, i).start()

    @pl.when(place > 0)
    def _():
        for i in range(3):
            halo_copy(1, i).start()

    def column(ref, to_y, matrix):
        at = pl.multiple_of(to_y * hid, 128)
        if matrix == 2:
            return ref.at[pl.ds(at, hid), :]
        return ref.at[:, pl.ds(at, hid)]

    given = (gate_w, value_w, down_w)

    def landing(matrix, index):
        if matrix == 2:
            return wd.at[index]
        return (wg, wv)[matrix].at[pl.ds(pl.multiple_of(index * kb, kb), kb), :]

    def weight_copy(matrix, to_z, to_y):
        index = to_z * ny + to_y
        return remote(
            column(given[matrix], to_y, matrix),
            landing(matrix, place),
            w_s.at[matrix, index],
            w_r.at[matrix, place],
            (to_z, to_y, x, c),
        )

    def weight_arrival(matrix, index):
        return remote(
            landing(matrix, index),
            landing(matrix, index),
            w_s.at[matrix, index],
            w_r.at[matrix, index],
            other_y,
        )

    def weight_relay(matrix, far_y):
        index = far * ny + far_y
        return remote(
            landing(matrix, index),
            landing(matrix, index),
            w_fwd.at[matrix, far_y],
            w_r.at[matrix, index],
            (end, y, x, c),
        )

    def send_weights(matrix, distance, do):
        if distance == 0:
            do(weight_copy(matrix, z, 1 - y))
            return
        for sign in (1, -1):
            to = z + sign * distance

            @pl.when((to >= 0) & (to < nz))
            def _():
                for dy in range(ny):
                    do(weight_copy(matrix, to, lax.rem(y + dy, ny)))

    def start(copy):
        copy.start()

    def relay_weights(matrix):
        @pl.when(relay)
        def _():
            for far_y in range(ny):
                weight_arrival(matrix, far * ny + far_y).wait_recv()
                weight_relay(matrix, far_y).start()

    def own_copy(matrix):
        return pltpu.make_async_copy(
            column(given[matrix], y, matrix), landing(matrix, place), local.at[matrix]
        )

    def await_weights(matrix, to_z):
        for to_y in range(ny):
            index = to_z * ny + to_y

            @pl.when((index != place) & jnp.logical_not(relay & (to_z == far)))
            def _():
                weight_arrival(matrix, index).wait_recv()

    def strip(ref, index, size, first=0):
        return ref.at[:, pl.ds(pl.multiple_of(index * cols + first, 128), size)]

    def tp_views(family):
        if family == 0:
            return skip, lambda i: strip(skip_all, i, cols)
        if family == 1:
            return closing, lambda i: close_all.at[pl.ds(pl.multiple_of(i * cols, cols), cols), :]
        first = (family - 2) * gw
        view = lambda i: strip(blend, i, gw, first)
        return view(lane_at), view

    side_x = (1 - x) * nc + c

    def tp_copy(family, which):
        own, view = tp_views(family)
        index, source = ((lane_at, own), (lane_at, own), (side_x, view(side_x)))[which]
        return remote(
            source,
            view(index),
            tp_s.at[family, which],
            tp_r.at[family, which],
            (other_x, other_c, other_c)[which],
        )

    def tp_arrival(family, which):
        _, view = tp_views(family)
        index = (side_x, x * nc + 1 - c, (1 - x) * nc + 1 - c)[which]
        return remote(
            view(index), view(index), tp_s.at[family, which], tp_r.at[family, which], other_c
        )

    for family in range(2):
        tp_copy(family, 0).start()
        tp_copy(family, 1).start()

    for matrix in range(3):
        own_copy(matrix).start()
    close_own = pltpu.make_async_copy(
        closing, close_all.at[pl.ds(pl.multiple_of(lane_at * cols, cols), cols), :], local.at[3]
    )
    close_own.start()
    send_weights(0, 1, start)
    send_weights(0, 0, start)

    edge = wide.shape[0] - tile
    for source, start_at, size in pieces:
        wide[tile : tile + rows, start_at : start_at + size] = source[...].astype(F32)

    @pl.when(place > 0)
    def _():
        for i in range(3):
            halo_copy(0, i).wait_recv()
        wide[0:tile, :] = halo[0].astype(F32)

    @pl.when(place == 0)
    def _():
        wide[0:tile, :] = jnp.zeros((tile, wide.shape[1]), F32)

    @pl.when(place < last)
    def _():
        for i in range(3):
            halo_copy(1, i).wait_recv()
        wide[edge:, :] = halo[1].astype(F32)

    @pl.when(place == last)
    def _():
        wide[edge:, :] = jnp.zeros((tile, wide.shape[1]), F32)

    margin = taps_p.shape[0] // 2
    for (source, start_at, size), taps in zip(pieces, (taps_p, taps_i, taps_o)):

        def conv_columns(i, carried, start_at=start_at, taps=taps):
            into = pl.ds(pl.multiple_of(start_at + i * 128, 128), 128)
            tap = taps[:, pl.ds(pl.multiple_of(i * 128, 128), 128)]
            for r in range(0, rows, 128):
                summed = None
                for k in range(tap.shape[0]):
                    first = tile - margin + k + r
                    term = wide[first : first + 128, into] * tap[k : k + 1]
                    summed = term if summed is None else summed + term
                conv[r : r + 128, into] = jax.nn.silu(summed).astype(BF)
            return carried

        lax.fori_loop(0, size // 128, conv_columns, 0)

    def lanes(ref):
        blank = jnp.zeros((ref.shape[1], 128 - 2 * heads), F32)
        return jnp.concatenate([ref[0], ref[1], blank], axis=1)

    raw = lanes(pre)
    steps = jnp.maximum(raw, 0.0) + jnp.log1p(jnp.exp(-jnp.abs(raw)))
    rates = jnp.concatenate(
        [rate[0:1], rate[1:2], jnp.zeros((1, 128 - 2 * heads), F32)], axis=1
    )
    logs = lanes(extra) - steps * jnp.exp(rates)
    earlier = lax.broadcasted_iota(jnp.int32, (rows, rows), 0) >= lax.broadcasted_iota(
        jnp.int32, (rows, rows), 1
    )
    running = dot(earlier.astype(F32), logs, precision=lax.Precision.HIGHEST)
    before = running - logs
    run_s[...] = running
    exc_s[...] = before
    run_t[...] = running.T
    exc_t[...] = before.T
    step_t[...] = steps.T
    whole = running[rows - 1 : rows]
    lane = lax.broadcasted_iota(jnp.int32, (rows, 128), 1)
    ends[...] = jnp.exp(jnp.where(lane < heads, whole - running, before)) * steps
    totals[place] = jnp.broadcast_to(whole, (8, 128))

    def spread(columns, first):
        low = lax.broadcasted_iota(jnp.int32, (columns.shape[0], 2 * head_w), 1) < head_w
        shape = (columns.shape[0], 2 * head_w)
        return jnp.where(
            low,
            jnp.broadcast_to(columns[:, first : first + 1], shape),
            jnp.broadcast_to(columns[:, first + 1 : first + 2], shape),
        )

    def scale_rows(i, carried):
        at = pl.ds(pl.multiple_of(i * 128, 128), 128)
        factors = ends[at, :]
        for d in range(2):
            for p in range(heads // 2):
                into = slice(p * 2 * head_w, (p + 1) * 2 * head_w)
                made = conv[at, into].astype(F32) * spread(factors, d * heads + 2 * p)
                start_at = d * heads * head_w + p * 2 * head_w
                scaled[at, start_at : start_at + 2 * head_w] = made.astype(BF)
        return carried

    lax.fori_loop(0, rows // 128, scale_rows, 0)
    in_at = payload.shape[1]
    out_at = in_at + ingest.shape[1]
    for d in range(2):
        for g in range(groups):
            first = d * heads * head_w + g * gw
            state = dot(
                scaled[:, first : first + gw],
                conv[:, in_at + g * STATE : in_at + (g + 1) * STATE],
                ((0,), (0,)),
            )
            sum_f[d, g] = state
            sum_h[d, g] = state.astype(BF)

    state_y = remote(sum_h, sum_y, sy_s, sy_r, other_y)
    state_y.start()

    def total_copy(k):
        to = (lax.rem(z + k // ny, nz), lax.rem(y + k % ny, ny), x, c)
        to_place = to[0] * ny + to[1]
        return remote(totals.at[place], totals.at[place], tot_s.at[k], tot_r.at[place], to)

    def total_arrival(k):
        index = lax.rem(z + k // ny, nz) * ny + lax.rem(y + k % ny, ny)
        return remote(totals.at[index], totals.at[index], tot_s.at[k], tot_r.at[index], other_y)

    for k in range(1, nz * ny):
        total_copy(k).start()

    state_y.wait_recv()
    for k in range(1, nz * ny):
        total_arrival(k).wait_recv()

    def head_rows(ref_value, factors):
        return jnp.concatenate(
            [ref_value[e * head_w : (e + 1) * head_w] * factors[e] for e in range(per)], axis=0
        )

    def of_heads(row, d, g=None):
        result = []
        for e in range(per):
            picks = [
                row[:, d * heads + k * per + e : d * heads + k * per + e + 1] for k in range(groups)
            ]
            if g is None:
                result.append(jnp.where(y == 0, picks[0], picks[1]))
            else:
                result.append(picks[g])
        return result

    one_row = jnp.ones((1, 128), F32)
    plane_low = jnp.exp(totals[z * ny, 0:1])
    plane_high = jnp.exp(totals[z * ny + 1, 0:1])
    forward_own = of_heads(jnp.where(y == 0, plane_high, one_row), 0)
    forward_far = of_heads(jnp.where(y == 0, one_row, plane_high), 0)
    back_own = of_heads(jnp.where(y == 0, one_row, plane_low), 1)
    back_far = of_heads(jnp.where(y == 0, plane_low, one_row), 1)
    plane_out[0] = (
        head_rows(sum_f[0, y], forward_own) + head_rows(sum_y[0, y].astype(F32), forward_far)
    ).astype(BF)
    plane_out[1] = (
        head_rows(sum_f[1, y], back_own) + head_rows(sum_y[1, y].astype(F32), back_far)
    ).astype(BF)

    def plane_copy(k, d):
        return remote(
            plane_out.at[d], plane_in.at[z], pl_s.at[k], pl_r.at[z], (k, y, x, c)
        )

    for k in range(nz):
        for d in range(2):

            @pl.when((k > z) if d == 0 else (k < z))
            def _():
                plane_copy(k, d).start()

    send_weights(0, 2, start)
    send_weights(1, 2, start)
    send_weights(1, 1, start)
    send_weights(1, 0, start)

    def within(g):
        read = conv[:, out_at + g * STATE : out_at + (g + 1) * STATE]
        write = conv[:, in_at + g * STATE : in_at + (g + 1) * STATE]
        scores[...] = dot(read, write, ((1,), (1,)))
        for p in range(per // 2):
            pair = g * per + 2 * p
            into = slice(pair * head_w, (pair + 2) * head_w)

            def chunk(i, carried):
                at = pl.ds(pl.multiple_of(i * 128, 128), 128)
                t = lax.broadcasted_iota(jnp.int32, (128, rows), 0) + i * 128
                s = lax.broadcasted_iota(jnp.int32, (128, rows), 1)
                after, same = t > s, t == s
                values = conv[:, into]
                low = lax.broadcasted_iota(jnp.int32, values.shape, 1) < head_w
                summed = None
                for e in range(2):
                    f, b = pair + e, heads + pair + e
                    gap = jnp.where(
                        after,
                        run_s[at, f : f + 1] - run_t[f : f + 1, :],
                        exc_t[b : b + 1, :] - exc_s[at, b : b + 1],
                    )
                    step_f, step_b = step_t[f : f + 1, :], step_t[b : b + 1, :]
                    factor = jnp.where(after, step_f, jnp.where(same, step_f + step_b, step_b))
                    made = (scores[at, :] * jnp.exp(gap) * factor).astype(BF)
                    kept = jnp.where(low if e == 0 else jnp.logical_not(low), values, 0)
                    term = dot(made, kept.astype(BF))
                    summed = term if summed is None else summed + term
                mixed[at, into] = summed
                return carried

            lax.fori_loop(0, rows // 128, chunk, 0)

    within(0)
    tp_arrival(0, 0).wait_recv()
    tp_copy(0, 2).start()

    carry[...] = jnp.zeros_like(carry)
    for k in range(nz):
        for d in range(2):

            @pl.when((k < z) if d == 0 else (k > z))
            def _():
                remote(
                    plane_out.at[d], plane_in.at[k], pl_s.at[k], pl_r.at[k], other_y
                ).wait_recv()
                gone = jnp.zeros((1, 128), F32)
                for q in range(nz * ny):
                    if d == 0:
                        between = (q >= ny * (k + 1)) & (q < ny * z)
                    else:
                        between = (q >= ny * (z + 1)) & (q < ny * k)
                    gone = gone + jnp.where(between, totals[q, 0:1], 0.0)
                weights = of_heads(jnp.exp(gone), d)
                carry[d] = carry[d] + head_rows(plane_in[k].astype(F32), weights)

    for d in range(2):
        carry_all[d, y] = carry[d].astype(BF)

    def carry_copy(d):
        return remote(carry_all.at[d, y], carry_all.at[d, y], ca_s.at[d], ca_r.at[d], other_y)

    for d in range(2):
        carry_copy(d).start()

    within(1)
    relay_weights(0)

    for d in range(2):
        remote(
            carry_all.at[d, 1 - y], carry_all.at[d, 1 - y], ca_s.at[d], ca_r.at[d], other_y
        ).wait_recv()
    for g in range(groups):
        for d in range(2):
            through = plane_low if d == 0 else plane_high
            adds = y == 1 if d == 0 else y == 0
            weights = of_heads(jnp.where(adds, through, one_row), d, g)
            body = head_rows(carry_all[d, g].astype(F32), weights)
            entering[d, g] = (body + jnp.where(adds, sum_y[d, g].astype(F32), 0.0)).astype(BF)

    for g in range(groups):

        def finish(i, carried):
            at = pl.ds(pl.multiple_of(i * 128, 128), 128)
            read = conv[at, out_at + g * STATE : out_at + (g + 1) * STATE]
            fore = dot(read, entering[0, g], ((1,), (1,)))
            back = dot(read, entering[1, g], ((1,), (1,)))
            grown = jnp.exp(run_s[at, :])
            shrunk = jnp.exp(run_s[rows - 1 : rows, :] - exc_s[at, :])
            parts = []
            for p in range(per // 2):
                pair = g * per + 2 * p
                into = slice(pair * head_w, (pair + 2) * head_w)
                inner = slice(2 * p * head_w, 2 * (p + 1) * head_w)
                total = mixed[at, into] + fore[:, inner] * spread(grown, pair)
                total = total + back[:, inner] * spread(shrunk, heads + pair)
                parts.append(total * jax.nn.silu(valve[at, into].astype(F32)))
            gated = jnp.concatenate(parts, axis=1)
            mean = jnp.mean(gated * gated, axis=1, keepdims=True)
            made = gated * lax.rsqrt(mean + EPSILON) * gain[:, g * gw : (g + 1) * gw]
            blend[at, pl.ds(pl.multiple_of(lane_at * cols + g * gw, 128), gw)] = made.astype(BF)
            return carried

        lax.fori_loop(0, rows // 128, finish, 0)
        tp_copy(2 + g, 0).start()
        tp_copy(2 + g, 1).start()

    skip_all[:, pl.ds(pl.multiple_of(lane_at * cols, 128), cols)] = skip[...]
    tp_arrival(0, 1).wait_recv()
    tp_arrival(0, 2).wait_recv()
    tp_arrival(1, 0).wait_recv()
    tp_copy(1, 2).start()
    for g in range(groups):
        tp_arrival(2 + g, 0).wait_recv()
        tp_copy(2 + g, 2).start()
    close_own.wait()
    tp_arrival(1, 1).wait_recv()
    tp_arrival(1, 2).wait_recv()
    for g in range(groups):
        tp_arrival(2 + g, 1).wait_recv()
        tp_arrival(2 + g, 2).wait_recv()

    tp_copy(0, 2).wait_send()

    def project(i, squares):
        into = pl.ds(pl.multiple_of(i * 256, 256), 256)
        made = dot(blend[...], close_all[:, into]) + skip_all[:, into].astype(F32)
        rounded = made.astype(BF)
        skip_all[:, into] = rounded
        again = rounded.astype(F32)
        return squares + jnp.sum(again * again, axis=1, keepdims=True)

    squares = lax.fori_loop(0, width_all // 256, project, jnp.zeros((rows, 1), F32))
    inverse = lax.rsqrt(squares / width_all + EPSILON)
    own_rows = pl.ds(pl.multiple_of(tile + y * rows, tile), rows)
    for i in range(0, width_all, 256):
        made = skip_all[:, i : i + 256].astype(F32) * inverse * norm_gain[:, i : i + 256]
        rows_n[own_rows, i : i + 256] = made.astype(BF)

    span = width_all // nc

    def row_view(which_y, which_c):
        return rows_n.at[
            pl.ds(pl.multiple_of(tile + which_y * rows, tile), rows),
            pl.ds(pl.multiple_of(which_c * span, 128), span),
        ]

    row_y = remote(row_view(y, c), row_view(y, c), nr_s.at[0], nr_r.at[0], other_y)
    row_y.start()
    bottom = tile + ny * rows

    def edge_copy(side, to_y):
        if side == 0:
            src = rows_n.at[pl.ds(bottom - tile, tile)]
            dst = rows_n.at[pl.ds(0, tile)]
            to = (z + 1, to_y, x, c)
        else:
            src = rows_n.at[pl.ds(tile, tile)]
            dst = rows_n.at[pl.ds(bottom, tile)]
            to = (z - 1, to_y, x, c)
        return remote(src, dst, edge_s.at[to_y], edge_r.at[side], to)

    sends_up = (y == ny - 1) & (z < nz - 1)
    sends_down = (y == 0) & (z > 0)
    for side, cond in ((0, sends_up), (1, sends_down)):

        @pl.when(cond)
        def _():
            for to_y in range(ny):
                edge_copy(side, to_y).start()

    for distance in (2, 1, 0):
        send_weights(2, distance, start)

    row_in = remote(row_view(1 - y, c), row_view(1 - y, c), nr_s.at[0], nr_r.at[0], other_y)
    row_in.wait_recv()
    row_pass = remote(row_view(1 - y, c), row_view(1 - y, c), nr_s.at[1], nr_r.at[1], other_c)
    row_pass.start()

    @pl.when(z > 0)
    def _():
        edge_copy(0, 0).wait_recv()

    @pl.when(z == 0)
    def _():
        rows_n[0:tile, :] = jnp.zeros((tile, width_all), BF)

    @pl.when(z < nz - 1)
    def _():
        edge_copy(1, 0).wait_recv()

    @pl.when(z == nz - 1)
    def _():
        rows_n[bottom:, :] = jnp.zeros((tile, width_all), BF)

    row_last = remote(
        row_view(1 - y, 1 - c), row_view(1 - y, 1 - c), nr_s.at[1], nr_r.at[1], other_c
    )
    row_last.wait_recv()

    high = rows_n.shape[0] // 3
    for matrix, (weight, made) in enumerate(((wg, made_g), (wv, made_v))):
        if matrix == 1:
            relay_weights(1)
        own_copy(matrix).wait()
        for k in range(nz):
            await_weights(matrix, k)

        def units(i, carried):
            at = pl.ds(pl.multiple_of(i * high, tile), high)
            made[at, :] = dot(rows_n[at, :], weight[...]).astype(BF).astype(F32)
            return carried

        lax.fori_loop(0, 3, units, 0)

    ff_margin = gate_taps.shape[0] // 2

    def activate(i, carried):
        into = pl.ds(pl.multiple_of(i * 128, 128), 128)
        tap_at = pl.ds(pl.multiple_of(y * hid + i * 128, 128), 128)
        tap_g, tap_v = gate_taps[:, tap_at], value_taps[:, tap_at]
        for r in range(0, ny * rows, 128):
            pair = []
            for made, tap in ((made_g, tap_g), (made_v, tap_v)):
                summed = None
                for k in range(tap.shape[0]):
                    first = tile - ff_margin + k + r
                    term = made[first : first + 128, into] * tap[k : k + 1]
                    summed = term if summed is None else summed + term
                pair.append(summed)
            hidden[r : r + 128, into] = (jax.nn.silu(pair[0]) * pair[1]).astype(BF)
        return carried

    lax.fori_loop(0, hid // 128, activate, 0)

    own_copy(2).wait()

    def order(k):
        if k < 2:
            kept = near * (1 - 2 * k) + k
        else:
            kept = k * (1 - near) + (5 - k) * near
        return kept * (1 - 2 * half) + (nz - 1) * half

    order_near = lambda k: order(k)

    def core_copy(i):
        return remote(part.at[i], part_in.at[i], core_s.at[i], core_r.at[i], other_c)

    def own_to(i, owner_x, to_y, owner_c):
        slot = y * nx + x
        return remote(
            part.at[i, pl.ds(to_y * rows, rows)],
            far_in.at[slot, i % ny],
            own_s.at[i, to_y],
            own_r.at[slot, i % ny],
            (z, to_y, owner_x, owner_c),
        )

    count = nz * ny

    def settle(i):
        to_z = order(i // ny)
        owner_x, owner_c = to_z // nc, lax.rem(to_z, nc)

        @pl.when(c == owner_c)
        def _():
            core_copy(i).wait_recv()
            for to_y in range(ny):
                at = slice(to_y * rows, (to_y + 1) * rows)
                mine = (to_y == y) & (owner_x == x)

                @pl.when(mine)
                def _():
                    own_sum[i % ny] = part_f[i % 2, at] + part_in[i, at].astype(F32)

                @pl.when(jnp.logical_not(mine))
                def _():
                    part[i, at] = (part_f[i % 2, at] + part_in[i, at].astype(F32)).astype(BF)
                    own_to(i, owner_x, to_y, owner_c).start()

    for i in range(count):
        to_z, to_y = order(i // ny), i % ny
        owner_c = lax.rem(to_z, nc)
        index = to_z * ny + to_y

        @pl.when(relay & (to_z == far))
        def _():
            weight_arrival(2, index).wait_recv()
            weight_relay(2, to_y).start()

        @pl.when((index != place) & jnp.logical_not(relay & (to_z == far)))
        def _():
            weight_arrival(2, index).wait_recv()

        made = dot(hidden[...], wd[index])

        @pl.when(c == owner_c)
        def _():
            part_f[i % 2] = made

        @pl.when(c != owner_c)
        def _():
            part[i] = made.astype(BF)
            core_copy(i).start()

        if i:
            settle(i - 1)
    settle(count - 1)

    for q in range(ny):
        at = pl.ds(pl.multiple_of(lane_at * cols + q * ob, 128), ob)
        total = own_sum[q]
        for k in range(1, ny * nx):
            from_y = lax.rem(y + k // nx, ny)
            from_x = lax.rem(x + k % nx, nx)
            slot = from_y * nx + from_x
            remote(
                far_in.at[slot, q], far_in.at[slot, q], own_s.at[0, 0], own_r.at[slot, q], other_c
            ).wait_recv()
            total = total + far_in[slot, q].astype(F32)
        out[:, q * ob : (q + 1) * ob] = (skip_all[:, at].astype(F32) + total).astype(BF)

    def done(copy):
        copy.wait_send()

    @pl.when(place < last)
    def _():
        for i in range(3):
            halo_copy(0, i).wait_send()

    @pl.when(place > 0)
    def _():
        for i in range(3):
            halo_copy(1, i).wait_send()

    for matrix in range(3):
        for distance in range(3):
            send_weights(matrix, distance, done)

        @pl.when(relay)
        def _():
            for far_y in range(ny):
                weight_relay(matrix, far_y).wait_send()

    for family in range(2 + groups):
        for which in range(3 if family else 2):
            tp_copy(family, which).wait_send()
    state_y.wait_send()
    for k in range(1, nz * ny):
        total_copy(k).wait_send()
    for k in range(nz):

        @pl.when(k != z)
        def _():
            plane_copy(k, 0).wait_send()

    for d in range(2):
        carry_copy(d).wait_send()
    row_y.wait_send()
    row_pass.wait_send()
    for cond in (sends_up, sends_down):

        @pl.when(cond)
        def _():
            for to_y in range(ny):
                edge_copy(0, to_y).wait_send()

    for i in range(count):
        to_z = order(i // ny)
        owner_x, owner_c = to_z // nc, lax.rem(to_z, nc)

        @pl.when(c != owner_c)
        def _():
            core_copy(i).wait_send()

        for to_y in range(ny):

            @pl.when((c == owner_c) & jnp.logical_not((to_y == y) & (owner_x == x)))
            def _():
                own_to(i, owner_x, to_y, owner_c).wait_send()


def one_kernel(*args):
    (skip, valve, payload, ingest, observe, pre, rate, extra, tp_taps, ti_taps, to_taps) = args[:11]
    gain, closing, norm_gain, gate_w, value_w, gate_taps, value_taps, down_w = args[11:]
    nz, ny, nx, nc = (lax.axis_size(a) for a in ("z", "y", "x", "core"))
    rows, cols = skip.shape
    width = norm_gain.shape[0]
    heads = pre.shape[2]
    groups = ingest.shape[1] // STATE
    gw = payload.shape[1] // groups
    joined = payload.shape[1] + ingest.shape[1] + observe.shape[1]
    hid = gate_w.shape[1] // ny
    ob = down_w.shape[1]
    count = nz * ny
    tile = 16
    tall = ny * rows + 2 * tile
    vmem, anywhere = pl.BlockSpec(memory_space=pltpu.VMEM), pl.BlockSpec(memory_space=pl.ANY)
    v = pltpu.VMEM
    sem = pltpu.SemaphoreType.DMA
    scratch = [
        v((2, tile, joined), BF),
        v((rows + 2 * tile, joined), F32),
        v((rows, joined), BF),
        v((rows, 128), F32),
        v((rows, 128), F32),
        v((128, rows), F32),
        v((128, rows), F32),
        v((128, rows), F32),
        v((rows, 128), F32),
        v((rows, 2 * payload.shape[1]), BF),
        v((2, groups, gw, STATE), F32),
        v((2, groups, gw, STATE), BF),
        v((2, groups, gw, STATE), BF),
        v((count, 8, 128), F32),
        v((2, gw, STATE), BF),
        v((nz, gw, STATE), BF),
        v((2, gw, STATE), F32),
        v((2, groups, gw, STATE), BF),
        v((2, groups, gw, STATE), BF),
        v((rows, rows), F32),
        v((rows, payload.shape[1]), F32),
        v((rows, width), BF),
        v((rows, width), BF),
        v((width, width), BF),
        v((tall, width), BF),
        v((width, hid), BF),
        v((width, hid), BF),
        v((count, hid, ob), BF),
        v((tall, hid), F32),
        v((tall, hid), F32),
        v((ny * rows, hid), BF),
        v((count, ny * rows, ob), BF),
        v((2, ny * rows, ob), F32),
        v((count, ny * rows, ob), BF),
        v((ny, rows, ob), F32),
        v((ny * nx, ny, rows, ob), BF),
        sem((2, 3)),
        sem((2, 3)),
        sem((2 + groups, 3)),
        sem((2 + groups, 3)),
        sem((3, count)),
        sem((3, count)),
        sem((3, ny)),
        sem((count,)),
        sem((count,)),
        sem(()),
        sem(()),
        sem((nz,)),
        sem((nz,)),
        sem((2,)),
        sem((2,)),
        sem((2,)),
        sem((2,)),
        sem((ny,)),
        sem((2,)),
        sem((count,)),
        sem((count,)),
        sem((count, ny)),
        sem((ny * nx, ny)),
        sem((4,)),
    ]
    specs = [vmem] * 12 + [anywhere, vmem, anywhere, anywhere, vmem, vmem, anywhere]
    flops = 2 * rows * width * (width + 3 * hid * ny)
    return pl.pallas_call(
        layer,
        out_shape=jax.ShapeDtypeStruct((rows, cols), BF),
        in_specs=specs,
        out_specs=vmem,
        scratch_shapes=scratch,
        compiler_params=pltpu.CompilerParams(
            collective_id=0, has_side_effects=True, vmem_limit_bytes=67043328
        ),
        cost_estimate=pl.CostEstimate(flops=flops, bytes_accessed=2**24, transcendentals=0),
        name="layer",
    )(
        skip,
        valve,
        payload,
        ingest,
        observe,
        pre,
        rate,
        extra,
        tp_taps,
        ti_taps,
        to_taps,
        gain.reshape(1, -1),
        closing,
        norm_gain.reshape(1, -1),
        gate_w,
        value_w,
        gate_taps,
        value_taps,
        down_w,
    )


def body_for(grid):
    sizes = tuple(grid.shape[a] for a in ("z", "y", "x", "core"))
    return one_kernel if sizes == (4, 2, 2, 2) else shards


def solution(mesh):
    sp, tp = mesh.shape["sp"], mesh.shape["tp"]
    ny = 2 ** (int(math.log2(sp)) // 2)
    nc = 2 if tp % 2 == 0 else 1
    grid = Mesh(
        mesh.devices.reshape(sp // ny, ny, tp // nc, nc), ("z", "y", "x", "core")
    )
    return jax.shard_map(
        body_for(grid),
        mesh=grid,
        in_specs=(
            P(SP, TP),
            P(SP, TP),
            P(SP, TP),
            P(SP, TP),
            P(SP, TP),
            P(None, SP, TP),
            P(None, TP),
            P(None, SP, TP),
            P(None, TP),
            P(None, TP),
            P(None, TP),
            P(TP),
            P(TP, None),
            P(),
            P(SP, TP),
            P(SP, TP),
            P(None, TP),
            P(None, TP),
            P(TP, SP),
        ),
        out_specs=P(SP, TP),
        check_vma=False,
    )
```

```python
import functools
import math

import jax
import jax.numpy as jnp
from jax import lax
from jax.experimental import pallas as pl
from jax.experimental.pallas import tpu as pltpu
from jax.sharding import Mesh
from jax.sharding import PartitionSpec as P

HEADS = 32
GROUPS = 8
STATE = 128
EPSILON = 1e-06
SP = ("z", "y")
TP = ("x", "core")


def shifted(block, axis, step):
    count = lax.axis_size(axis)
    return lax.ppermute(block, axis, [(i, (i + step) % count) for i in range(count)])


def moved(block, axis, step):
    count = lax.axis_size(axis)
    pairs = [(i, i + step) for i in range(count) if 0 <= i + step < count]
    return lax.ppermute(block, axis, pairs)


def grid_shifted(block, axes, steps):
    sizes = [lax.axis_size(a) for a in axes]
    pairs = []
    for source in range(sizes[0] * sizes[1]):
        first, second = divmod(source, sizes[1])
        target = ((first + steps[0]) % sizes[0]) * sizes[1] + (second + steps[1]) % sizes[1]
        pairs.append((source, target))
    return lax.ppermute(block, axes, pairs)


def ordered(by_step, index):
    count = len(by_step)
    result = []
    for owner in range(count):
        back = lax.rem(index - owner + count, count)
        block = by_step[0]
        for step in range(1, count):
            block = jnp.where(back == step, by_step[step], block)
        result.append(block)
    return result


def extended(block, axis, width):
    low = moved(block[-width:], axis, 1)
    high = moved(block[:width], axis, -1)
    return jnp.concatenate([low, block, high], axis=0)


def conv_rows(padded, kernel, length):
    summed = padded[0:length] * kernel[0]
    for offset in range(1, kernel.shape[0]):
        summed = summed + padded[offset : offset + length] * kernel[offset]
    return summed


def bdot(pattern, one, two):
    return jnp.einsum(pattern, one, two, preferred_element_type=jnp.float32)


def pack(decay, state):
    heads, width, depth = state.shape
    rows = jnp.broadcast_to(decay[:, None, None], (heads, 16, depth)).astype(jnp.bfloat16)
    return jnp.concatenate([state.astype(jnp.bfloat16), rows], axis=1)


def unpack(packed, width):
    body = packed.astype(jnp.float32)
    return body[:, width, 0], body[:, :width]


def carried_in(decay, state, sign):
    width = state.shape[1]
    count = lax.axis_size(SP)
    own = pack(decay, state)
    index = lax.axis_index(SP)

    def from_back(array, step):
        back, value = unpack(moved(array, SP, sign * step), width)
        source = index - sign * step
        inside = (source >= 0) & (source < count)
        return jnp.where(inside, back, 1.0), value

    near, far = from_back(own, 1), from_back(own, 2)
    total = near[1] + near[0][:, None, None] * far[1]
    product = near[0] * far[0]
    covered = 2
    while covered < count - 1:
        back, value = from_back(pack(product, total), covered)
        total = total + product[:, None, None] * value
        product = product * back
        covered *= 2
    return total


def tied(value, *others):
    marks = [other[(slice(0, 1),) * other.ndim] for other in others]
    return lax.optimization_barrier((value, *marks))[0]


def shared_rows(weight, axis_dim, out_dim, mark):
    count = lax.axis_size("y")
    index = lax.axis_index("y")
    part = weight.shape[axis_dim] // count
    received = []
    for step in range(count):
        at = lax.rem(index + step, count) * part
        block = lax.dynamic_slice_in_dim(weight, at, part, axis_dim)
        received.append(shifted(block, "y", step) if step else block)
    received = [tied(block, mark) for block in received]
    return jnp.concatenate(ordered(received, index), axis=out_dim)


def shards(
    skip_trunk_vector,
    valve_preactivation,
    projected_heads_payload,
    cluster_ingests,
    cluster_observers,
    pre_softplus_increments,
    attenuation_ln_rate,
    additional_attenuation,
    payload_conv_weights,
    ingest_conv_weights,
    observer_conv_weights,
    valved_cluster_factor,
    closing_map_matrix,
    dense_standardize_factor,
    dense_valve_map,
    dense_payload_map,
    valve_series_smoother,
    payload_series_smoother,
    dense_contract_map,
):
    rows = skip_trunk_vector.shape[0]
    own_cols = skip_trunk_vector.shape[1]
    head_count = pre_softplus_increments.shape[2]
    per_group = HEADS // GROUPS
    nx, nc, ny = lax.axis_size("x"), lax.axis_size("core"), lax.axis_size("y")
    ix, ic, iy = lax.axis_index("x"), lax.axis_index("core"), lax.axis_index("y")

    joined = jnp.concatenate([projected_heads_payload, cluster_ingests, cluster_observers], axis=1)
    taps_all = jnp.concatenate(
        [payload_conv_weights, ingest_conv_weights, observer_conv_weights], axis=1
    )
    padded = extended(joined, SP, taps_all.shape[0] // 2)

    convolved = jax.nn.silu(conv_rows(padded.astype(jnp.float32), taps_all, rows)).astype(
        jnp.bfloat16
    )
    gate_w = lax.all_gather(shared_rows(dense_valve_map, 1, 0, convolved), "z", axis=0, tiled=True)
    value_w = lax.all_gather(
        shared_rows(dense_payload_map, 1, 0, convolved), "z", axis=0, tiled=True
    )

    payload_columns = projected_heads_payload.shape[1]
    input_cols = cluster_ingests.shape[1]
    width = payload_columns // head_count
    groups = input_cols // STATE
    values = convolved[:, :payload_columns]
    inputs_g = convolved[:, payload_columns : payload_columns + input_cols].reshape(
        rows, groups, STATE
    )
    readout_g = convolved[:, payload_columns + input_cols :].reshape(rows, groups, STATE)

    steps = jax.nn.softplus(pre_softplus_increments)
    logs = additional_attenuation - steps * jnp.exp(attenuation_ln_rate)[:, None, :]
    running = jnp.cumsum(logs, axis=1)
    run_f = running[0]
    exc_b = running[1] - logs[1]
    total_f, total_b = running[0, -1], running[1, -1]

    end_f = jnp.exp(total_f[None] - run_f) * steps[0]
    end_b = jnp.exp(exc_b) * steps[1]
    ends = jnp.stack([end_f, end_b], axis=1)
    scaled = (
        ends[:, :, :, None] * values.astype(jnp.float32).reshape(rows, 1, head_count, width)
    ).astype(jnp.bfloat16)
    scaled = scaled.reshape(rows, 2, groups, per_group, width)
    summary = bdot("sdgep,sgn->dgepn", scaled, inputs_g).reshape(2, head_count, width, STATE)
    in_f = carried_in(jnp.exp(total_f), summary[0], 1)
    in_b = carried_in(jnp.exp(total_b), summary[1], -1)

    down_part = shared_rows(dense_contract_map, 0, 1, in_f)
    down_w = lax.all_gather(down_part, "z", axis=1, tiled=True)

    places = jnp.arange(rows, dtype=jnp.int32)
    after = places[:, None] > places[None, :]
    same = places[:, None] == places[None, :]
    run_fT, exc_bT = run_f.T, exc_b.T
    step_f, step_b = steps[0].T, steps[1].T
    gaps = jnp.where(
        after[None],
        run_fT[:, :, None] - run_fT[:, None, :],
        exc_bT[:, None, :] - exc_bT[:, :, None],
    )
    factor = jnp.where(
        after[None],
        step_f[:, None, :],
        jnp.where(same[None], (step_f + step_b)[:, None, :], step_b[:, None, :]),
    )
    scores = jnp.repeat(bdot("tgn,sgn->gts", readout_g, inputs_g), per_group, axis=0)
    weights = (scores * jnp.exp(gaps) * factor).astype(jnp.bfloat16)
    within = bdot("hts,shp->thp", weights, values.reshape(rows, head_count, width))

    def outer(state):
        grouped = state.astype(jnp.bfloat16).reshape(groups, per_group, width, STATE)
        return bdot("gepn,tgn->tgep", grouped, readout_g).reshape(rows, head_count, width)

    mixed = within + outer(in_f) * jnp.exp(run_f)[:, :, None]
    mixed = mixed + outer(in_b) * jnp.exp(total_b[None] - exc_b)[:, :, None]
    gated = mixed.reshape(rows, payload_columns) * jax.nn.silu(
        valve_preactivation.astype(jnp.float32)
    )
    grouped = gated.reshape(rows, groups, per_group * width)
    standardized = grouped * lax.rsqrt(jnp.mean(grouped * grouped, axis=2, keepdims=True) + EPSILON)
    blended = (standardized.reshape(rows, payload_columns) * valved_cluster_factor).astype(
        jnp.bfloat16
    )

    def column_block(matrix, dx, dc):
        at = (lax.rem(ix + dx, nx) * nc + lax.rem(ic + dc, nc)) * own_cols
        return lax.dynamic_slice_in_dim(matrix, at, own_cols, 1)

    def over_cores(terms):
        total = terms[0].astype(jnp.bfloat16).astype(jnp.float32)
        for dc in range(1, nc):
            total = total + shifted(terms[dc].astype(jnp.bfloat16), "core", dc).astype(jnp.float32)
        return total

    mapped = None
    for dx in list(range(1, nx)) + [0]:
        terms = [
            jnp.dot(
                blended,
                column_block(closing_map_matrix, dx, dc),
                preferred_element_type=jnp.float32,
            )
            for dc in range(nc)
        ]
        part = over_cores(terms)
        if dx:
            part = shifted(part.astype(jnp.bfloat16), "x", dx).astype(jnp.float32)
        mapped = part if mapped is None else mapped + part
    middle = (skip_trunk_vector.astype(jnp.float32) + mapped).astype(jnp.bfloat16)

    margin = valve_series_smoother.shape[0] // 2
    room = -(-margin // 16) * 16
    low = moved(middle[-margin:], SP, 1)
    high = moved(middle[:margin], SP, -1)
    blank = jnp.zeros((room - margin, own_cols), middle.dtype)
    wide = jnp.concatenate([blank, low, middle, high, blank], axis=0)

    def everywhere(block):
        by_y = []
        for dy in range(ny):
            by_x = []
            for dx in range(nx):
                got = grid_shifted(block, ("y", "x"), (dy, dx)) if dy or dx else block
                by_core = [got] + [shifted(got, "core", dc) for dc in range(1, nc)]
                by_x.append(jnp.concatenate(ordered(by_core, ic), axis=1))
            by_y.append(jnp.concatenate(ordered(by_x, ix), axis=1))
        return jnp.stack(ordered(by_y, iy))

    line = everywhere(wide).reshape(ny * (rows + 2 * room), -1).astype(jnp.float32)
    inverse = lax.rsqrt(jnp.mean(line * line, axis=1, keepdims=True) + EPSILON)
    normed = (line * inverse * dense_standardize_factor).astype(jnp.bfloat16)

    hidden_cols = gate_w.shape[1]
    gate_taps = lax.dynamic_slice_in_dim(valve_series_smoother, iy * hidden_cols, hidden_cols, 1)
    value_taps = lax.dynamic_slice_in_dim(payload_series_smoother, iy * hidden_cols, hidden_cols, 1)

    def spread(weight, taps):
        made = jnp.dot(normed, weight, preferred_element_type=jnp.float32).astype(jnp.bfloat16)
        made = made.reshape(ny, rows + 2 * room, hidden_cols).astype(jnp.float32)
        summed = None
        for offset in range(taps.shape[0]):
            start = room - margin + offset
            term = made[:, start : start + rows] * taps[offset]
            summed = term if summed is None else summed + term
        return summed

    gate_rows = spread(gate_w, gate_taps)
    value_rows = spread(value_w, value_taps)
    hidden = (jax.nn.silu(gate_rows) * value_rows).astype(jnp.bfloat16)

    order = [(dy, dx) for dy in range(ny) for dx in range(nx)]
    down = None
    for dy, dx in order[1:] + order[:1]:
        wanted = lax.dynamic_index_in_dim(hidden, lax.rem(iy + dy, ny), 0, keepdims=False)
        terms = [
            jnp.dot(wanted, column_block(down_w, dx, dc), preferred_element_type=jnp.float32)
            for dc in range(nc)
        ]
        part = over_cores(terms)
        if dy or dx:
            part = grid_shifted(part.astype(jnp.bfloat16), ("y", "x"), (dy, dx)).astype(jnp.float32)
        down = part if down is None else down + part
    return (middle.astype(jnp.float32) + down).astype(jnp.bfloat16)


MESH = pl.DeviceIdType.MESH
BF = jnp.bfloat16
F32 = jnp.float32


def dot(one, two, dims=((1,), (0,)), precision=None):
    return lax.dot_general(
        one, two, (dims, ((), ())), preferred_element_type=F32, precision=precision
    )


def layer(
    skip,
    valve,
    payload,
    ingest,
    observe,
    pre,
    rate,
    extra,
    taps_p,
    taps_i,
    taps_o,
    gain,
    closing,
    norm_gain,
    gate_w,
    value_w,
    gate_taps,
    value_taps,
    down_w,
    out,
    halo,
    wide,
    conv,
    run_s,
    exc_s,
    run_t,
    exc_t,
    step_t,
    ends,
    scaled,
    sum_f,
    sum_h,
    sum_y,
    totals,
    plane_out,
    plane_in,
    carry,
    carry_all,
    entering,
    scores,
    mixed,
    blend,
    mid_own,
    close_all,
    rows_n,
    wg,
    wv,
    wd,
    made_g,
    made_v,
    hidden,
    part,
    part_f,
    part_in,
    own_sum,
    far_in,
    halo_s,
    halo_r,
    tp_s,
    tp_r,
    w_s,
    w_r,
    w_y,
    w_fwd,
    cl_s,
    cl_r,
    tot_s,
    tot_r,
    sy_s,
    sy_r,
    pl_s,
    pl_r,
    ca_s,
    ca_r,
    nb_s,
    nb_r,
    nf_s,
    nf_r,
    edge_s,
    edge_r,
    core_s,
    core_r,
    own_s,
    own_r,
    local,
):
    nz, ny, nx, nc = (lax.axis_size(a) for a in ("z", "y", "x", "core"))
    z, y, x, c = (lax.axis_index(a) for a in ("z", "y", "x", "core"))
    place, lane_at = z * ny + y, x * nc + c
    rows, cols = skip.shape
    width_all = blend.shape[1]
    heads = pre.shape[1]
    groups = ingest.shape[1] // STATE
    per = heads // groups
    head_w = payload.shape[1] // heads
    gw = per * head_w
    hid = wg.shape[1]
    kb = gate_w.shape[0]
    ob = down_w.shape[1]
    tile = 16
    other_y, other_x, other_c = (z, 1 - y, x, c), (z, y, 1 - x, c), (z, y, x, 1 - c)
    half = z // 2
    near = z * (1 - 2 * half) + (nz - 1) * half
    relay = near == 1
    far, end = (nz - 1) * (1 - half), (nz - 1) * half

    def remote(src, dst, send, recv, to):
        return pltpu.make_async_remote_copy(
            src_ref=src,
            dst_ref=dst,
            send_sem=send,
            recv_sem=recv,
            device_id=to,
            device_id_type=MESH,
        )

    barrier = pltpu.get_barrier_semaphore()
    greeted = 0
    for k in range(1, nz * ny):
        to = (lax.rem(z + k // ny, nz), lax.rem(y + k % ny, ny), x, c)
        pl.semaphore_signal(barrier, inc=1, device_id=to, device_id_type=MESH)
        greeted += 1
    for k in range(1, nx * nc):
        for dy in range(ny):
            to = (z, lax.rem(y + dy, ny), lax.rem(x + k // nc, nx), lax.rem(c + k % nc, nc))
            pl.semaphore_signal(barrier, inc=1, device_id=to, device_id_type=MESH)
            greeted += 1
    pl.semaphore_wait(barrier, greeted)

    pieces = []
    at = 0
    for source in (payload, ingest, observe):
        pieces.append((source, at, source.shape[1]))
        at += source.shape[1]

    def halo_copy(side, i):
        source, start, size = pieces[i]
        other = place + 1 if side == 0 else place - 1
        to = (other // ny, lax.rem(other + ny, ny), x, c)
        src = source.at[pl.ds(rows - tile, tile)] if side == 0 else source.at[pl.ds(0, tile)]
        return remote(
            src,
            halo.at[side, :, pl.ds(start, size)],
            halo_s.at[side, i],
            halo_r.at[side, i],
            to,
        )

    last = nz * ny - 1

    @pl.when(place < last)
    def _():
        for i in range(3):
            halo_copy(0, i).start()

    @pl.when(place > 0)
    def _():
        for i in range(3):
            halo_copy(1, i).start()

    def column(ref, to_y, matrix):
        at = pl.multiple_of(to_y * hid, 128)
        if matrix == 2:
            return ref.at[pl.ds(at, hid), :]
        return ref.at[:, pl.ds(at, hid)]

    given = (gate_w, value_w, down_w)

    def landing(matrix, index):
        if matrix == 2:
            return wd.at[index]
        return (wg, wv)[matrix].at[pl.ds(pl.multiple_of(index * kb, kb), kb), :]

    beside = z * ny + 1 - y

    def weight_y(matrix):
        return remote(
            column(given[matrix], 1 - y, matrix),
            landing(matrix, place),
            w_y.at[matrix],
            w_r.at[matrix, place],
            other_y,
        )

    def weight_arrival(matrix, index):
        return remote(
            landing(matrix, index),
            landing(matrix, index),
            w_y.at[matrix],
            w_r.at[matrix, index],
            other_y,
        )

    def weight_copy(matrix, to_z, passed):
        index = beside if passed else place
        source = landing(matrix, index) if passed else column(given[matrix], y, matrix)
        return remote(
            source,
            landing(matrix, index),
            w_s.at[matrix, to_z * ny + passed],
            w_r.at[matrix, index],
            (to_z, y, x, c),
        )

    def weight_relay(matrix, passed):
        index = far * ny + (1 - y if passed else y)
        return remote(
            landing(matrix, index),
            landing(matrix, index),
            w_fwd.at[matrix, passed],
            w_r.at[matrix, index],
            (end, y, x, c),
        )

    def send_weights(matrix, passed, do, distances=(2, 1)):
        for distance in distances:
            for sign in (1, -1):
                to = z + sign * distance

                @pl.when((to >= 0) & (to < nz))
                def _():
                    do(weight_copy(matrix, to, passed))

    def start(copy):
        copy.start()

    def pass_weights(matrix):
        weight_arrival(matrix, beside).wait_recv()
        send_weights(matrix, 1, start)

    def relay_weights(matrix, passed):
        @pl.when(relay)
        def _():
            weight_arrival(matrix, far * ny + (1 - y if passed else y)).wait_recv()
            weight_relay(matrix, passed).start()

    def own_copy(matrix):
        return pltpu.make_async_copy(
            column(given[matrix], y, matrix), landing(matrix, place), local.at[matrix]
        )

    def await_weights(matrix, to_z):
        for to_y in range(ny):

            @pl.when((to_z != z) & jnp.logical_not(relay & (to_z == far)))
            def _():
                weight_arrival(matrix, to_z * ny + to_y).wait_recv()

    def tp_index(k):
        return lax.rem(x + k // nc, nx), lax.rem(c + k % nc, nc)

    def close_copy(k):
        to_x, to_c = tp_index(k)
        at = pl.ds(pl.multiple_of((to_x * nc + to_c) * cols, 128), cols)
        return remote(
            closing.at[:, at], close_rows(lane_at), cl_s.at[k], cl_r.at[k], (z, y, to_x, to_c)
        )

    def close_rows(index):
        return close_all.at[pl.ds(pl.multiple_of(index * cols, cols), cols), :]

    def close_arrival(k):
        at_x, at_c = tp_index(k)
        view = close_rows(at_x * nc + at_c)
        return remote(view, view, cl_s.at[k], cl_r.at[k], other_c)

    side_x = (1 - x) * nc + c

    def blend_view(g, index):
        return blend.at[:, pl.ds(pl.multiple_of(index * cols + g * gw, 128), gw)]

    def tp_copy(g, which):
        view = blend_view(g, (lane_at, lane_at, side_x)[which])
        to = (other_x, other_c, other_c)[which]
        return remote(view, view, tp_s.at[g, which], tp_r.at[g, which], to)

    def tp_arrival(g, which):
        view = blend_view(g, (side_x, x * nc + 1 - c, (1 - x) * nc + 1 - c)[which])
        return remote(view, view, tp_s.at[g, which], tp_r.at[g, which], other_c)

    weight_y(0).start()
    send_weights(0, 0, start, (1,))
    send_weights(1, 0, start, (1,))
    for k in (2, 3, 1):
        close_copy(k).start()
    for matrix in range(3):
        own_copy(matrix).start()
    close_own = pltpu.make_async_copy(
        closing.at[:, pl.ds(pl.multiple_of(lane_at * cols, 128), cols)],
        close_rows(lane_at),
        local.at[3],
    )
    close_own.start()

    edge = wide.shape[0] - tile
    for source, start_at, size in pieces:
        wide[tile : tile + rows, start_at : start_at + size] = source[...].astype(F32)

    @pl.when(place > 0)
    def _():
        for i in range(3):
            halo_copy(0, i).wait_recv()
        wide[0:tile, :] = halo[0].astype(F32)

    @pl.when(place == 0)
    def _():
        wide[0:tile, :] = jnp.zeros((tile, wide.shape[1]), F32)

    @pl.when(place < last)
    def _():
        for i in range(3):
            halo_copy(1, i).wait_recv()
        wide[edge:, :] = halo[1].astype(F32)

    @pl.when(place == last)
    def _():
        wide[edge:, :] = jnp.zeros((tile, wide.shape[1]), F32)

    margin = taps_p.shape[0] // 2
    for (source, start_at, size), taps in zip(pieces, (taps_p, taps_i, taps_o)):

        def conv_columns(i, carried, start_at=start_at, taps=taps):
            into = pl.ds(pl.multiple_of(start_at + i * 128, 128), 128)
            tap = taps[:, pl.ds(pl.multiple_of(i * 128, 128), 128)]
            for r in range(0, rows, 128):
                summed = None
                for k in range(tap.shape[0]):
                    first = tile - margin + k + r
                    term = wide[first : first + 128, into] * tap[k : k + 1]
                    summed = term if summed is None else summed + term
                conv[r : r + 128, into] = jax.nn.silu(summed).astype(BF)
            return carried

        lax.fori_loop(0, size // 128, conv_columns, 0)

    def upright(row):
        shape = (heads, heads)
        same = lax.broadcasted_iota(jnp.int32, shape, 0) == lax.broadcasted_iota(
            jnp.int32, shape, 1
        )
        return jnp.sum(
            jnp.where(same, jnp.broadcast_to(row, shape), 0.0), axis=1, keepdims=True
        )

    def turned(array):
        blank = jnp.zeros((128 - 2 * heads, rows), F32)
        return jnp.concatenate([array, blank], axis=0).T

    raw = jnp.concatenate([pre[0], pre[1]], axis=0)
    steps_t = jnp.maximum(raw, 0.0) + jnp.log1p(jnp.exp(-jnp.abs(raw)))
    rates = jnp.exp(jnp.concatenate([upright(rate[0:1]), upright(rate[1:2])], axis=0))
    logs_t = jnp.concatenate([extra[0], extra[1]], axis=0) - steps_t * rates
    earlier = lax.broadcasted_iota(jnp.int32, (rows, rows), 0) <= lax.broadcasted_iota(
        jnp.int32, (rows, rows), 1
    )
    running_t = dot(logs_t, earlier.astype(F32), precision=lax.Precision.HIGHEST)
    before_t = running_t - logs_t
    run_t[...] = running_t
    exc_t[...] = before_t
    step_t[...] = steps_t
    running, before, steps = turned(running_t), turned(before_t), turned(steps_t)
    run_s[...] = running
    exc_s[...] = before
    whole = running[rows - 1 : rows]
    lane = lax.broadcasted_iota(jnp.int32, (rows, 128), 1)
    ends[...] = jnp.exp(jnp.where(lane < heads, whole - running, before)) * steps
    totals[place] = jnp.broadcast_to(whole, (8, 128))

    def spread(columns, first):
        low = lax.broadcasted_iota(jnp.int32, (columns.shape[0], 2 * head_w), 1) < head_w
        shape = (columns.shape[0], 2 * head_w)
        return jnp.where(
            low,
            jnp.broadcast_to(columns[:, first : first + 1], shape),
            jnp.broadcast_to(columns[:, first + 1 : first + 2], shape),
        )

    def scale_rows(i, carried):
        at = pl.ds(pl.multiple_of(i * 128, 128), 128)
        factors = ends[at, :]
        for d in range(2):
            for p in range(heads // 2):
                into = slice(p * 2 * head_w, (p + 1) * 2 * head_w)
                made = conv[at, into].astype(F32) * spread(factors, d * heads + 2 * p)
                start_at = d * heads * head_w + p * 2 * head_w
                scaled[at, start_at : start_at + 2 * head_w] = made.astype(BF)
        return carried

    lax.fori_loop(0, rows // 128, scale_rows, 0)
    in_at = payload.shape[1]
    out_at = in_at + ingest.shape[1]
    for d in range(2):
        for g in range(groups):
            first = d * heads * head_w + g * gw
            state = dot(
                scaled[:, first : first + gw],
                conv[:, in_at + g * STATE : in_at + (g + 1) * STATE],
                ((0,), (0,)),
            )
            sum_f[d, g] = state
            sum_h[d, g] = state.astype(BF)

    state_y = remote(sum_h, sum_y, sy_s, sy_r, other_y)
    state_y.start()

    def total_copy(k):
        to = (lax.rem(z + k // ny, nz), lax.rem(y + k % ny, ny), x, c)
        to_place = to[0] * ny + to[1]
        return remote(totals.at[place], totals.at[place], tot_s.at[k], tot_r.at[place], to)

    def total_arrival(k):
        index = lax.rem(z + k // ny, nz) * ny + lax.rem(y + k % ny, ny)
        return remote(totals.at[index], totals.at[index], tot_s.at[k], tot_r.at[index], other_y)

    for k in range(1, nz * ny):
        total_copy(k).start()

    state_y.wait_recv()
    total_arrival(1).wait_recv()

    def head_rows(ref_value, factors):
        return jnp.concatenate(
            [ref_value[e * head_w : (e + 1) * head_w] * factors[e] for e in range(per)], axis=0
        )

    def of_heads(row, d, g=None):
        result = []
        for e in range(per):
            picks = [
                row[:, d * heads + k * per + e : d * heads + k * per + e + 1] for k in range(groups)
            ]
            if g is None:
                result.append(jnp.where(y == 0, picks[0], picks[1]))
            else:
                result.append(picks[g])
        return result

    one_row = jnp.ones((1, 128), F32)
    plane_low = jnp.exp(totals[z * ny, 0:1])
    plane_high = jnp.exp(totals[z * ny + 1, 0:1])
    forward_own = of_heads(jnp.where(y == 0, plane_high, one_row), 0)
    forward_far = of_heads(jnp.where(y == 0, one_row, plane_high), 0)
    back_own = of_heads(jnp.where(y == 0, one_row, plane_low), 1)
    back_far = of_heads(jnp.where(y == 0, plane_low, one_row), 1)
    plane_out[0] = (
        head_rows(sum_f[0, y], forward_own) + head_rows(sum_y[0, y].astype(F32), forward_far)
    ).astype(BF)
    plane_out[1] = (
        head_rows(sum_f[1, y], back_own) + head_rows(sum_y[1, y].astype(F32), back_far)
    ).astype(BF)

    def plane_copy(k, d):
        return remote(
            plane_out.at[d], plane_in.at[z], pl_s.at[k], pl_r.at[z], (k, y, x, c)
        )

    for k in range(nz):
        for d in range(2):

            @pl.when((k > z) if d == 0 else (k < z))
            def _():
                plane_copy(k, d).start()

    weight_y(1).start()
    weight_y(2).start()
    send_weights(0, 0, start, (2,))
    pass_weights(0)
    send_weights(1, 0, start, (2,))

    def within(g):
        read = conv[:, out_at + g * STATE : out_at + (g + 1) * STATE]
        write = conv[:, in_at + g * STATE : in_at + (g + 1) * STATE]
        scores[...] = dot(read, write, ((1,), (1,)))
        for p in range(per // 2):
            pair = g * per + 2 * p
            into = slice(pair * head_w, (pair + 2) * head_w)

            def chunk(i, carried):
                at = pl.ds(pl.multiple_of(i * 128, 128), 128)
                t = lax.broadcasted_iota(jnp.int32, (128, rows), 0) + i * 128
                s = lax.broadcasted_iota(jnp.int32, (128, rows), 1)
                after, same = t > s, t == s
                values = conv[:, into]
                low = lax.broadcasted_iota(jnp.int32, values.shape, 1) < head_w
                summed = None
                for e in range(2):
                    f, b = pair + e, heads + pair + e
                    gap = jnp.where(
                        after,
                        run_s[at, f : f + 1] - run_t[f : f + 1, :],
                        exc_t[b : b + 1, :] - exc_s[at, b : b + 1],
                    )
                    step_f, step_b = step_t[f : f + 1, :], step_t[b : b + 1, :]
                    factor = jnp.where(after, step_f, jnp.where(same, step_f + step_b, step_b))
                    made = (scores[at, :] * jnp.exp(gap) * factor).astype(BF)
                    kept = jnp.where(low if e == 0 else jnp.logical_not(low), values, 0)
                    term = dot(made, kept.astype(BF))
                    summed = term if summed is None else summed + term
                mixed[at, into] = summed
                return carried

            lax.fori_loop(0, rows // 128, chunk, 0)

    within(0)
    for k in range(2, nz * ny):
        total_arrival(k).wait_recv()
    carry[...] = jnp.zeros_like(carry)
    for k in range(nz):
        for d in range(2):

            @pl.when((k < z) if d == 0 else (k > z))
            def _():
                remote(
                    plane_out.at[d], plane_in.at[k], pl_s.at[k], pl_r.at[k], other_y
                ).wait_recv()
                gone = jnp.zeros((1, 128), F32)
                for q in range(nz * ny):
                    if d == 0:
                        between = (q >= ny * (k + 1)) & (q < ny * z)
                    else:
                        between = (q >= ny * (z + 1)) & (q < ny * k)
                    gone = gone + jnp.where(between, totals[q, 0:1], 0.0)
                weights = of_heads(jnp.exp(gone), d)
                carry[d] = carry[d] + head_rows(plane_in[k].astype(F32), weights)

    for d in range(2):
        carry_all[d, y] = carry[d].astype(BF)

    def carry_copy(d):
        return remote(carry_all.at[d, y], carry_all.at[d, y], ca_s.at[d], ca_r.at[d], other_y)

    for d in range(2):
        carry_copy(d).start()

    within(1)
    relay_weights(0, 0)
    pass_weights(1)

    for d in range(2):
        remote(
            carry_all.at[d, 1 - y], carry_all.at[d, 1 - y], ca_s.at[d], ca_r.at[d], other_y
        ).wait_recv()
    for g in range(groups):
        for d in range(2):
            through = plane_low if d == 0 else plane_high
            adds = y == 1 if d == 0 else y == 0
            weights = of_heads(jnp.where(adds, through, one_row), d, g)
            body = head_rows(carry_all[d, g].astype(F32), weights)
            entering[d, g] = (body + jnp.where(adds, sum_y[d, g].astype(F32), 0.0)).astype(BF)

    for g in range(groups):

        def finish(i, carried):
            at = pl.ds(pl.multiple_of(i * 128, 128), 128)
            read = conv[at, out_at + g * STATE : out_at + (g + 1) * STATE]
            fore = dot(read, entering[0, g], ((1,), (1,)))
            back = dot(read, entering[1, g], ((1,), (1,)))
            grown = jnp.exp(run_s[at, :])
            shrunk = jnp.exp(run_s[rows - 1 : rows, :] - exc_s[at, :])
            parts = []
            for p in range(per // 2):
                pair = g * per + 2 * p
                into = slice(pair * head_w, (pair + 2) * head_w)
                inner = slice(2 * p * head_w, 2 * (p + 1) * head_w)
                total = mixed[at, into] + fore[:, inner] * spread(grown, pair)
                total = total + back[:, inner] * spread(shrunk, heads + pair)
                parts.append(total * jax.nn.silu(valve[at, into].astype(F32)))
            gated = jnp.concatenate(parts, axis=1)
            mean = jnp.mean(gated * gated, axis=1, keepdims=True)
            made = gated * lax.rsqrt(mean + EPSILON) * gain[:, g * gw : (g + 1) * gw]
            blend[at, pl.ds(pl.multiple_of(lane_at * cols + g * gw, 128), gw)] = made.astype(BF)
            return carried

        lax.fori_loop(0, rows // 128, finish, 0)
        tp_copy(g, 0).start()
        tp_copy(g, 1).start()

    close_own.wait()
    for k in range(1, nx * nc):
        close_arrival(k).wait_recv()
    for g in range(groups):
        tp_arrival(g, 0).wait_recv()
        tp_copy(g, 2).start()
    for g in range(groups):
        tp_arrival(g, 1).wait_recv()
        tp_arrival(g, 2).wait_recv()

    def row_view(which_y, index):
        return rows_n.at[
            pl.ds(pl.multiple_of(tile + which_y * rows, tile), rows),
            pl.ds(pl.multiple_of(index * cols, 128), cols),
        ]

    relay_weights(0, 1)
    made = dot(blend[...], close_all[...]) + skip[...].astype(F32)
    mid_own[...] = made.astype(BF)
    rows_n[
        pl.ds(pl.multiple_of(tile + y * rows, tile), rows),
        pl.ds(pl.multiple_of(lane_at * cols, 128), cols),
    ] = mid_own[...]

    other_xy = (z, 1 - y, 1 - x, c)
    froms = ((y, x), (y, 1 - x), (1 - y, x), (1 - y, 1 - x))

    def row_copy(k):
        view = row_view(y, lane_at)
        to = (other_c, other_x, other_y, other_xy)[k]
        return remote(view, view, nb_s.at[k], nb_r.at[k], to)

    def row_pass(k, core, arriving=False):
        view = row_view(froms[k][0], froms[k][1] * nc + core)
        sem = (nb_r if arriving else nf_r).at[k]
        return remote(view, view, nf_s.at[k], sem, other_c)

    for k in (1, 2, 3, 0):
        row_copy(k).start()
    for k in (1, 2, 3):
        row_pass(k, c, arriving=True).wait_recv()
        row_pass(k, c).start()
        if k == 1:
            relay_weights(1, 0)
    row_pass(0, 1 - c, arriving=True).wait_recv()
    for k in (1, 2, 3):
        row_pass(k, 1 - c).wait_recv()
    for k in range(4):
        row_copy(k).wait_send()
        if k:
            row_pass(k, c).wait_send()
    relay_weights(1, 1)

    def normalize(i, carried):
        at = pl.ds(pl.multiple_of(tile + i * 128, tile), 128)
        squares = jnp.zeros((128, 1), F32)
        for first in range(0, width_all, 256):
            piece = rows_n[at, first : first + 256].astype(F32)
            squares = squares + jnp.sum(piece * piece, axis=1, keepdims=True)
        inverse = lax.rsqrt(squares / width_all + EPSILON)
        for first in range(0, width_all, 256):
            piece = rows_n[at, first : first + 256].astype(F32)
            piece = piece * inverse * norm_gain[:, first : first + 256]
            rows_n[at, first : first + 256] = piece.astype(BF)
        return carried

    lax.fori_loop(0, ny * rows // 128, normalize, 0)

    bottom = tile + ny * rows

    def edge_copy(side):
        if side == 0:
            src, dst = rows_n.at[pl.ds(bottom - tile, tile)], rows_n.at[pl.ds(0, tile)]
        else:
            src, dst = rows_n.at[pl.ds(tile, tile)], rows_n.at[pl.ds(bottom, tile)]
        to = (z + 1 if side == 0 else z - 1, y, x, c)
        return remote(src, dst, edge_s.at[side], edge_r.at[side], to)

    sends_up, sends_down = z < nz - 1, z > 0
    for side, cond in ((0, sends_up), (1, sends_down)):

        @pl.when(cond)
        def _():
            edge_copy(side).start()

    send_weights(2, 0, start)
    pass_weights(2)

    for matrix, (weight, made) in enumerate(((wg, made_g), (wv, made_v))):
        own_copy(matrix).wait()
        for k in range(nz):
            await_weights(matrix, k)

        def units(i, carried):
            at = pl.ds(pl.multiple_of(tile + i * rows, tile), rows)
            made[at, :] = dot(rows_n[at, :], weight[...]).astype(BF).astype(F32)
            return carried

        lax.fori_loop(0, ny, units, 0)

    @pl.when(z > 0)
    def _():
        edge_copy(0).wait_recv()

    @pl.when(z == 0)
    def _():
        rows_n[0:tile, :] = jnp.zeros((tile, width_all), BF)

    @pl.when(z < nz - 1)
    def _():
        edge_copy(1).wait_recv()

    @pl.when(z == nz - 1)
    def _():
        rows_n[bottom:, :] = jnp.zeros((tile, width_all), BF)

    both = jnp.concatenate([rows_n[0:tile, :], rows_n[bottom:, :]], axis=0)
    for weight, made in ((wg, made_g), (wv, made_v)):
        edges = dot(both, weight[...]).astype(BF).astype(F32)
        made[0:tile, :] = edges[0:tile]
        made[bottom:, :] = edges[tile:]

    ff_margin = gate_taps.shape[0] // 2

    def activate(i, carried):
        into = pl.ds(pl.multiple_of(i * 128, 128), 128)
        tap_at = pl.ds(pl.multiple_of(y * hid + i * 128, 128), 128)
        tap_g, tap_v = gate_taps[:, tap_at], value_taps[:, tap_at]
        for r in range(0, ny * rows, 128):
            pair = []
            for made, tap in ((made_g, tap_g), (made_v, tap_v)):
                summed = None
                for k in range(tap.shape[0]):
                    first = tile - ff_margin + k + r
                    term = made[first : first + 128, into] * tap[k : k + 1]
                    summed = term if summed is None else summed + term
                pair.append(summed)
            hidden[r : r + 128, into] = (jax.nn.silu(pair[0]) * pair[1]).astype(BF)
        return carried

    lax.fori_loop(0, hid // 128, activate, 0)

    own_copy(2).wait()

    def order(k):
        if k < 2:
            kept = near * (1 - 2 * k) + k
        else:
            kept = k * (1 - near) + (5 - k) * near
        return kept * (1 - 2 * half) + (nz - 1) * half

    def core_copy(i):
        return remote(part.at[i], part_in.at[i], core_s.at[i], core_r.at[i], other_c)

    def block_y(i):
        return y if i % ny == 0 else 1 - y

    def own_to(i, owner_x, to_y, owner_c):
        slot = y * nx + x
        return remote(
            part.at[i, pl.ds(to_y * rows, rows)],
            far_in.at[slot, block_y(i)],
            own_s.at[i, to_y],
            own_r.at[slot, block_y(i)],
            (z, to_y, owner_x, owner_c),
        )

    count = nz * ny

    def settle(i):
        to_z = order(i // ny)
        owner_x, owner_c = to_z // nc, lax.rem(to_z, nc)

        @pl.when(c == owner_c)
        def _():
            core_copy(i).wait_recv()
            for to_y in range(ny):
                at = slice(to_y * rows, (to_y + 1) * rows)
                mine = (to_y == y) & (owner_x == x)

                @pl.when(mine)
                def _():
                    own_sum[block_y(i)] = part_f[i % 2, at] + part_in[i, at].astype(F32)

                @pl.when(jnp.logical_not(mine))
                def _():
                    part[i, at] = (part_f[i % 2, at] + part_in[i, at].astype(F32)).astype(BF)
                    own_to(i, owner_x, to_y, owner_c).start()

    for i in range(count):
        to_z, to_y = order(i // ny), block_y(i)
        owner_c = lax.rem(to_z, nc)
        index = to_z * ny + to_y

        @pl.when(relay & (to_z == far))
        def _():
            weight_arrival(2, index).wait_recv()
            weight_relay(2, i % ny).start()

        @pl.when((to_z != z) & jnp.logical_not(relay & (to_z == far)))
        def _():
            weight_arrival(2, index).wait_recv()

        made = dot(hidden[...], wd[index])

        @pl.when(c == owner_c)
        def _():
            part_f[i % 2] = made

        @pl.when(c != owner_c)
        def _():
            part[i] = made.astype(BF)
            core_copy(i).start()

        if i:
            settle(i - 1)
    settle(count - 1)

    for q in range(ny):
        total = own_sum[q]
        for k in range(1, ny * nx):
            from_y = lax.rem(y + k // nx, ny)
            from_x = lax.rem(x + k % nx, nx)
            slot = from_y * nx + from_x
            remote(
                far_in.at[slot, q], far_in.at[slot, q], own_s.at[0, 0], own_r.at[slot, q], other_c
            ).wait_recv()
            total = total + far_in[slot, q].astype(F32)
        out[:, q * ob : (q + 1) * ob] = (mid_own[:, q * ob : (q + 1) * ob].astype(F32) + total).astype(BF)

    def done(copy):
        copy.wait_send()

    @pl.when(place < last)
    def _():
        for i in range(3):
            halo_copy(0, i).wait_send()

    @pl.when(place > 0)
    def _():
        for i in range(3):
            halo_copy(1, i).wait_send()

    for matrix in range(3):
        weight_y(matrix).wait_send()
        for passed in range(2):
            send_weights(matrix, passed, done)

        @pl.when(relay)
        def _():
            for passed in range(2):
                weight_relay(matrix, passed).wait_send()

    for g in range(groups):
        for which in range(3):
            tp_copy(g, which).wait_send()
    for k in range(1, nx * nc):
        close_copy(k).wait_send()
    state_y.wait_send()
    for k in range(1, nz * ny):
        total_copy(k).wait_send()
    for k in range(nz):

        @pl.when(k != z)
        def _():
            plane_copy(k, 0).wait_send()

    for d in range(2):
        carry_copy(d).wait_send()
    for side, cond in ((0, sends_up), (1, sends_down)):

        @pl.when(cond)
        def _():
            edge_copy(side).wait_send()

    for i in range(count):
        to_z = order(i // ny)
        owner_x, owner_c = to_z // nc, lax.rem(to_z, nc)

        @pl.when(c != owner_c)
        def _():
            core_copy(i).wait_send()

        for to_y in range(ny):

            @pl.when((c == owner_c) & jnp.logical_not((to_y == y) & (owner_x == x)))
            def _():
                own_to(i, owner_x, to_y, owner_c).wait_send()


def one_kernel(*args):
    (skip, valve, payload, ingest, observe, pre, rate, extra, tp_taps, ti_taps, to_taps) = args[:11]
    gain, closing, norm_gain, gate_w, value_w, gate_taps, value_taps, down_w = args[11:]
    nz, ny, nx, nc = (lax.axis_size(a) for a in ("z", "y", "x", "core"))
    rows, cols = skip.shape
    width = norm_gain.shape[0]
    groups = ingest.shape[1] // STATE
    gw = payload.shape[1] // groups
    joined = payload.shape[1] + ingest.shape[1] + observe.shape[1]
    hid = gate_w.shape[1] // ny
    ob = down_w.shape[1]
    count = nz * ny
    lanes_used = 2 * pre.shape[2]
    tile = 16
    tall = ny * rows + 2 * tile
    vmem, anywhere = pl.BlockSpec(memory_space=pltpu.VMEM), pl.BlockSpec(memory_space=pl.ANY)
    v = pltpu.VMEM
    sem = pltpu.SemaphoreType.DMA
    scratch = [
        v((2, tile, joined), BF),
        v((rows + 2 * tile, joined), F32),
        v((rows, joined), BF),
        v((rows, 128), F32),
        v((rows, 128), F32),
        v((lanes_used, rows), F32),
        v((lanes_used, rows), F32),
        v((lanes_used, rows), F32),
        v((rows, 128), F32),
        v((rows, 2 * payload.shape[1]), BF),
        v((2, groups, gw, STATE), F32),
        v((2, groups, gw, STATE), BF),
        v((2, groups, gw, STATE), BF),
        v((count, 8, 128), F32),
        v((2, gw, STATE), BF),
        v((nz, gw, STATE), BF),
        v((2, gw, STATE), F32),
        v((2, groups, gw, STATE), BF),
        v((2, groups, gw, STATE), BF),
        v((rows, rows), F32),
        v((rows, payload.shape[1]), F32),
        v((rows, width), BF),
        v((rows, cols), BF),
        v((width, cols), BF),
        v((tall, width), BF),
        v((width, hid), BF),
        v((width, hid), BF),
        v((count, hid, ob), BF),
        v((tall, hid), F32),
        v((tall, hid), F32),
        v((ny * rows, hid), BF),
        v((count, ny * rows, ob), BF),
        v((2, ny * rows, ob), F32),
        v((count, ny * rows, ob), BF),
        v((ny, rows, ob), F32),
        v((ny * nx, ny, rows, ob), BF),
        sem((2, 3)),
        sem((2, 3)),
        sem((groups, 3)),
        sem((groups, 3)),
        sem((3, count)),
        sem((3, count)),
        sem((3,)),
        sem((3, 2)),
        sem((nx * nc,)),
        sem((nx * nc,)),
        sem((count,)),
        sem((count,)),
        sem(()),
        sem(()),
        sem((nz,)),
        sem((nz,)),
        sem((2,)),
        sem((2,)),
        sem((4,)),
        sem((4,)),
        sem((4,)),
        sem((4,)),
        sem((2,)),
        sem((2,)),
        sem((count,)),
        sem((count,)),
        sem((count, ny)),
        sem((ny * nx, ny)),
        sem((4,)),
    ]
    specs = [vmem] * 12 + [anywhere, vmem, anywhere, anywhere, vmem, vmem, anywhere]
    flops = 2 * rows * width * (width + 3 * hid * ny)
    return pl.pallas_call(
        layer,
        out_shape=jax.ShapeDtypeStruct((rows, cols), BF),
        in_specs=specs,
        out_specs=vmem,
        scratch_shapes=scratch,
        compiler_params=pltpu.CompilerParams(
            collective_id=0, has_side_effects=True, vmem_limit_bytes=67043328
        ),
        cost_estimate=pl.CostEstimate(flops=flops, bytes_accessed=2**24, transcendentals=0),
        name="layer",
    )(
        skip,
        valve,
        payload,
        ingest,
        observe,
        jnp.swapaxes(pre, 1, 2),
        rate,
        jnp.swapaxes(extra, 1, 2),
        tp_taps,
        ti_taps,
        to_taps,
        gain.reshape(1, -1),
        closing,
        norm_gain.reshape(1, -1),
        gate_w,
        value_w,
        gate_taps,
        value_taps,
        down_w,
    )


def body_for(grid):
    sizes = tuple(grid.shape[a] for a in ("z", "y", "x", "core"))
    return one_kernel if sizes == (4, 2, 2, 2) else shards


def solution(mesh):
    sp, tp = mesh.shape["sp"], mesh.shape["tp"]
    ny = 2 ** (int(math.log2(sp)) // 2)
    nc = 2 if tp % 2 == 0 else 1
    grid = Mesh(
        mesh.devices.reshape(sp // ny, ny, tp // nc, nc), ("z", "y", "x", "core")
    )
    return jax.shard_map(
        body_for(grid),
        mesh=grid,
        in_specs=(
            P(SP, TP),
            P(SP, TP),
            P(SP, TP),
            P(SP, TP),
            P(SP, TP),
            P(None, SP, TP),
            P(None, TP),
            P(None, SP, TP),
            P(None, TP),
            P(None, TP),
            P(None, TP),
            P(TP),
            P(TP, None),
            P(),
            P(SP, TP),
            P(SP, TP),
            P(None, TP),
            P(None, TP),
            P(TP, SP),
        ),
        out_specs=P(SP, TP),
        check_vma=False,
    )
```

```python
import functools
import math

import jax
import jax.numpy as jnp
from jax import lax
from jax.experimental import pallas as pl
from jax.experimental.pallas import tpu as pltpu
from jax.sharding import Mesh
from jax.sharding import PartitionSpec as P

HEADS = 32
GROUPS = 8
STATE = 128
EPSILON = 1e-06
SP = ("z", "y")
TP = ("x", "core")


def shifted(block, axis, step):
    count = lax.axis_size(axis)
    return lax.ppermute(block, axis, [(i, (i + step) % count) for i in range(count)])


def moved(block, axis, step):
    count = lax.axis_size(axis)
    pairs = [(i, i + step) for i in range(count) if 0 <= i + step < count]
    return lax.ppermute(block, axis, pairs)


def grid_shifted(block, axes, steps):
    sizes = [lax.axis_size(a) for a in axes]
    pairs = []
    for source in range(sizes[0] * sizes[1]):
        first, second = divmod(source, sizes[1])
        target = ((first + steps[0]) % sizes[0]) * sizes[1] + (second + steps[1]) % sizes[1]
        pairs.append((source, target))
    return lax.ppermute(block, axes, pairs)


def ordered(by_step, index):
    count = len(by_step)
    result = []
    for owner in range(count):
        back = lax.rem(index - owner + count, count)
        block = by_step[0]
        for step in range(1, count):
            block = jnp.where(back == step, by_step[step], block)
        result.append(block)
    return result


def extended(block, axis, width):
    low = moved(block[-width:], axis, 1)
    high = moved(block[:width], axis, -1)
    return jnp.concatenate([low, block, high], axis=0)


def conv_rows(padded, kernel, length):
    summed = padded[0:length] * kernel[0]
    for offset in range(1, kernel.shape[0]):
        summed = summed + padded[offset : offset + length] * kernel[offset]
    return summed


def bdot(pattern, one, two):
    return jnp.einsum(pattern, one, two, preferred_element_type=jnp.float32)


def pack(decay, state):
    heads, width, depth = state.shape
    rows = jnp.broadcast_to(decay[:, None, None], (heads, 16, depth)).astype(jnp.bfloat16)
    return jnp.concatenate([state.astype(jnp.bfloat16), rows], axis=1)


def unpack(packed, width):
    body = packed.astype(jnp.float32)
    return body[:, width, 0], body[:, :width]


def carried_in(decay, state, sign):
    width = state.shape[1]
    count = lax.axis_size(SP)
    own = pack(decay, state)
    index = lax.axis_index(SP)

    def from_back(array, step):
        back, value = unpack(moved(array, SP, sign * step), width)
        source = index - sign * step
        inside = (source >= 0) & (source < count)
        return jnp.where(inside, back, 1.0), value

    near, far = from_back(own, 1), from_back(own, 2)
    total = near[1] + near[0][:, None, None] * far[1]
    product = near[0] * far[0]
    covered = 2
    while covered < count - 1:
        back, value = from_back(pack(product, total), covered)
        total = total + product[:, None, None] * value
        product = product * back
        covered *= 2
    return total


def tied(value, *others):
    marks = [other[(slice(0, 1),) * other.ndim] for other in others]
    return lax.optimization_barrier((value, *marks))[0]


def shared_rows(weight, axis_dim, out_dim, mark):
    count = lax.axis_size("y")
    index = lax.axis_index("y")
    part = weight.shape[axis_dim] // count
    received = []
    for step in range(count):
        at = lax.rem(index + step, count) * part
        block = lax.dynamic_slice_in_dim(weight, at, part, axis_dim)
        received.append(shifted(block, "y", step) if step else block)
    received = [tied(block, mark) for block in received]
    return jnp.concatenate(ordered(received, index), axis=out_dim)


def shards(
    skip_trunk_vector,
    valve_preactivation,
    projected_heads_payload,
    cluster_ingests,
    cluster_observers,
    pre_softplus_increments,
    attenuation_ln_rate,
    additional_attenuation,
    payload_conv_weights,
    ingest_conv_weights,
    observer_conv_weights,
    valved_cluster_factor,
    closing_map_matrix,
    dense_standardize_factor,
    dense_valve_map,
    dense_payload_map,
    valve_series_smoother,
    payload_series_smoother,
    dense_contract_map,
):
    rows = skip_trunk_vector.shape[0]
    own_cols = skip_trunk_vector.shape[1]
    head_count = pre_softplus_increments.shape[2]
    per_group = HEADS // GROUPS
    nx, nc, ny = lax.axis_size("x"), lax.axis_size("core"), lax.axis_size("y")
    ix, ic, iy = lax.axis_index("x"), lax.axis_index("core"), lax.axis_index("y")

    joined = jnp.concatenate([projected_heads_payload, cluster_ingests, cluster_observers], axis=1)
    taps_all = jnp.concatenate(
        [payload_conv_weights, ingest_conv_weights, observer_conv_weights], axis=1
    )
    padded = extended(joined, SP, taps_all.shape[0] // 2)

    convolved = jax.nn.silu(conv_rows(padded.astype(jnp.float32), taps_all, rows)).astype(
        jnp.bfloat16
    )
    gate_w = lax.all_gather(shared_rows(dense_valve_map, 1, 0, convolved), "z", axis=0, tiled=True)
    value_w = lax.all_gather(
        shared_rows(dense_payload_map, 1, 0, convolved), "z", axis=0, tiled=True
    )

    payload_columns = projected_heads_payload.shape[1]
    input_cols = cluster_ingests.shape[1]
    width = payload_columns // head_count
    groups = input_cols // STATE
    values = convolved[:, :payload_columns]
    inputs_g = convolved[:, payload_columns : payload_columns + input_cols].reshape(
        rows, groups, STATE
    )
    readout_g = convolved[:, payload_columns + input_cols :].reshape(rows, groups, STATE)

    steps = jax.nn.softplus(pre_softplus_increments)
    logs = additional_attenuation - steps * jnp.exp(attenuation_ln_rate)[:, None, :]
    running = jnp.cumsum(logs, axis=1)
    run_f = running[0]
    exc_b = running[1] - logs[1]
    total_f, total_b = running[0, -1], running[1, -1]

    end_f = jnp.exp(total_f[None] - run_f) * steps[0]
    end_b = jnp.exp(exc_b) * steps[1]
    ends = jnp.stack([end_f, end_b], axis=1)
    scaled = (
        ends[:, :, :, None] * values.astype(jnp.float32).reshape(rows, 1, head_count, width)
    ).astype(jnp.bfloat16)
    scaled = scaled.reshape(rows, 2, groups, per_group, width)
    summary = bdot("sdgep,sgn->dgepn", scaled, inputs_g).reshape(2, head_count, width, STATE)
    in_f = carried_in(jnp.exp(total_f), summary[0], 1)
    in_b = carried_in(jnp.exp(total_b), summary[1], -1)

    down_part = shared_rows(dense_contract_map, 0, 1, in_f)
    down_w = lax.all_gather(down_part, "z", axis=1, tiled=True)

    places = jnp.arange(rows, dtype=jnp.int32)
    after = places[:, None] > places[None, :]
    same = places[:, None] == places[None, :]
    run_fT, exc_bT = run_f.T, exc_b.T
    step_f, step_b = steps[0].T, steps[1].T
    gaps = jnp.where(
        after[None],
        run_fT[:, :, None] - run_fT[:, None, :],
        exc_bT[:, None, :] - exc_bT[:, :, None],
    )
    factor = jnp.where(
        after[None],
        step_f[:, None, :],
        jnp.where(same[None], (step_f + step_b)[:, None, :], step_b[:, None, :]),
    )
    scores = jnp.repeat(bdot("tgn,sgn->gts", readout_g, inputs_g), per_group, axis=0)
    weights = (scores * jnp.exp(gaps) * factor).astype(jnp.bfloat16)
    within = bdot("hts,shp->thp", weights, values.reshape(rows, head_count, width))

    def outer(state):
        grouped = state.astype(jnp.bfloat16).reshape(groups, per_group, width, STATE)
        return bdot("gepn,tgn->tgep", grouped, readout_g).reshape(rows, head_count, width)

    mixed = within + outer(in_f) * jnp.exp(run_f)[:, :, None]
    mixed = mixed + outer(in_b) * jnp.exp(total_b[None] - exc_b)[:, :, None]
    gated = mixed.reshape(rows, payload_columns) * jax.nn.silu(
        valve_preactivation.astype(jnp.float32)
    )
    grouped = gated.reshape(rows, groups, per_group * width)
    standardized = grouped * lax.rsqrt(jnp.mean(grouped * grouped, axis=2, keepdims=True) + EPSILON)
    blended = (standardized.reshape(rows, payload_columns) * valved_cluster_factor).astype(
        jnp.bfloat16
    )

    def column_block(matrix, dx, dc):
        at = (lax.rem(ix + dx, nx) * nc + lax.rem(ic + dc, nc)) * own_cols
        return lax.dynamic_slice_in_dim(matrix, at, own_cols, 1)

    def over_cores(terms):
        total = terms[0].astype(jnp.bfloat16).astype(jnp.float32)
        for dc in range(1, nc):
            total = total + shifted(terms[dc].astype(jnp.bfloat16), "core", dc).astype(jnp.float32)
        return total

    mapped = None
    for dx in list(range(1, nx)) + [0]:
        terms = [
            jnp.dot(
                blended,
                column_block(closing_map_matrix, dx, dc),
                preferred_element_type=jnp.float32,
            )
            for dc in range(nc)
        ]
        part = over_cores(terms)
        if dx:
            part = shifted(part.astype(jnp.bfloat16), "x", dx).astype(jnp.float32)
        mapped = part if mapped is None else mapped + part
    middle = (skip_trunk_vector.astype(jnp.float32) + mapped).astype(jnp.bfloat16)

    margin = valve_series_smoother.shape[0] // 2
    room = -(-margin // 16) * 16
    low = moved(middle[-margin:], SP, 1)
    high = moved(middle[:margin], SP, -1)
    blank = jnp.zeros((room - margin, own_cols), middle.dtype)
    wide = jnp.concatenate([blank, low, middle, high, blank], axis=0)

    def everywhere(block):
        by_y = []
        for dy in range(ny):
            by_x = []
            for dx in range(nx):
                got = grid_shifted(block, ("y", "x"), (dy, dx)) if dy or dx else block
                by_core = [got] + [shifted(got, "core", dc) for dc in range(1, nc)]
                by_x.append(jnp.concatenate(ordered(by_core, ic), axis=1))
            by_y.append(jnp.concatenate(ordered(by_x, ix), axis=1))
        return jnp.stack(ordered(by_y, iy))

    line = everywhere(wide).reshape(ny * (rows + 2 * room), -1).astype(jnp.float32)
    inverse = lax.rsqrt(jnp.mean(line * line, axis=1, keepdims=True) + EPSILON)
    normed = (line * inverse * dense_standardize_factor).astype(jnp.bfloat16)

    hidden_cols = gate_w.shape[1]
    gate_taps = lax.dynamic_slice_in_dim(valve_series_smoother, iy * hidden_cols, hidden_cols, 1)
    value_taps = lax.dynamic_slice_in_dim(payload_series_smoother, iy * hidden_cols, hidden_cols, 1)

    def spread(weight, taps):
        made = jnp.dot(normed, weight, preferred_element_type=jnp.float32).astype(jnp.bfloat16)
        made = made.reshape(ny, rows + 2 * room, hidden_cols).astype(jnp.float32)
        summed = None
        for offset in range(taps.shape[0]):
            start = room - margin + offset
            term = made[:, start : start + rows] * taps[offset]
            summed = term if summed is None else summed + term
        return summed

    gate_rows = spread(gate_w, gate_taps)
    value_rows = spread(value_w, value_taps)
    hidden = (jax.nn.silu(gate_rows) * value_rows).astype(jnp.bfloat16)

    order = [(dy, dx) for dy in range(ny) for dx in range(nx)]
    down = None
    for dy, dx in order[1:] + order[:1]:
        wanted = lax.dynamic_index_in_dim(hidden, lax.rem(iy + dy, ny), 0, keepdims=False)
        terms = [
            jnp.dot(wanted, column_block(down_w, dx, dc), preferred_element_type=jnp.float32)
            for dc in range(nc)
        ]
        part = over_cores(terms)
        if dy or dx:
            part = grid_shifted(part.astype(jnp.bfloat16), ("y", "x"), (dy, dx)).astype(jnp.float32)
        down = part if down is None else down + part
    return (middle.astype(jnp.float32) + down).astype(jnp.bfloat16)


MESH = pl.DeviceIdType.MESH
BF = jnp.bfloat16
F32 = jnp.float32


def dot(one, two, dims=((1,), (0,)), precision=None):
    return lax.dot_general(
        one, two, (dims, ((), ())), preferred_element_type=F32, precision=precision
    )


def layer(
    loads,
    skip,
    valve,
    payload,
    ingest,
    observe,
    pre,
    rate,
    extra,
    taps_p,
    taps_i,
    taps_o,
    gain,
    closing,
    norm_gain,
    gate_w,
    value_w,
    gate_taps,
    value_taps,
    down_w,
    out,
    halo,
    wide,
    conv,
    run_s,
    exc_s,
    run_t,
    exc_t,
    step_t,
    ends,
    scaled,
    sum_f,
    sum_h,
    sum_y,
    totals,
    plane_out,
    plane_in,
    carry,
    carry_all,
    entering,
    scores,
    mixed,
    blend,
    mid_own,
    close_all,
    rows_n,
    wg,
    wv,
    wd,
    made_g,
    made_v,
    hidden,
    part,
    part_f,
    part_in,
    own_sum,
    far_in,
    halo_s,
    halo_r,
    tp_s,
    tp_r,
    w_s,
    w_r,
    w_y,
    w_fwd,
    cl_s,
    cl_r,
    tot_s,
    tot_r,
    sy_s,
    sy_r,
    pl_s,
    pl_r,
    ca_s,
    ca_r,
    nb_s,
    nb_r,
    nf_s,
    nf_r,
    edge_s,
    edge_r,
    core_s,
    core_r,
    own_s,
    own_r,
    local,
):
    nz, ny, nx, nc = (lax.axis_size(a) for a in ("z", "y", "x", "core"))
    z, y, x, c = (lax.axis_index(a) for a in ("z", "y", "x", "core"))
    place, lane_at = z * ny + y, x * nc + c
    rows, cols = skip.shape
    width_all = blend.shape[1]
    heads = pre.shape[1]
    groups = ingest.shape[1] // STATE
    per = heads // groups
    head_w = payload.shape[1] // heads
    gw = per * head_w
    hid = wg.shape[1]
    kb = gate_w.shape[0]
    ob = down_w.shape[1]
    tile = 16
    other_y, other_x, other_c = (z, 1 - y, x, c), (z, y, 1 - x, c), (z, y, x, 1 - c)
    half = z // 2
    near = z * (1 - 2 * half) + (nz - 1) * half
    middle = (z > 0) & (z < nz - 1)

    def remote(src, dst, send, recv, to):
        return pltpu.make_async_remote_copy(
            src_ref=src,
            dst_ref=dst,
            send_sem=send,
            recv_sem=recv,
            device_id=to,
            device_id_type=MESH,
        )

    for load in loads:
        load.start()
    barrier = pltpu.get_barrier_semaphore()
    greeted = 0
    for k in range(1, nz * ny):
        to = (lax.rem(z + k // ny, nz), lax.rem(y + k % ny, ny), x, c)
        pl.semaphore_signal(barrier, inc=1, device_id=to, device_id_type=MESH)
        greeted += 1
    for k in range(1, nx * nc):
        for dy in range(ny):
            to = (z, lax.rem(y + dy, ny), lax.rem(x + k // nc, nx), lax.rem(c + k % nc, nc))
            pl.semaphore_signal(barrier, inc=1, device_id=to, device_id_type=MESH)
            greeted += 1
    pl.semaphore_wait(barrier, greeted)
    for load in loads:
        load.wait()

    pieces = []
    at = 0
    for source in (payload, ingest, observe):
        pieces.append((source, at, source.shape[1]))
        at += source.shape[1]

    def halo_copy(side, i):
        source, start, size = pieces[i]
        other = place + 1 if side == 0 else place - 1
        to = (other // ny, lax.rem(other + ny, ny), x, c)
        src = source.at[pl.ds(rows - tile, tile)] if side == 0 else source.at[pl.ds(0, tile)]
        return remote(
            src,
            halo.at[side, :, pl.ds(start, size)],
            halo_s.at[side, i],
            halo_r.at[side, i],
            to,
        )

    last = nz * ny - 1

    @pl.when(place < last)
    def _():
        for i in range(3):
            halo_copy(0, i).start()

    @pl.when(place > 0)
    def _():
        for i in range(3):
            halo_copy(1, i).start()

    def column(ref, to_y, matrix):
        at = pl.multiple_of(to_y * hid, 128)
        if matrix == 2:
            return ref.at[pl.ds(at, hid), :]
        return ref.at[:, pl.ds(at, hid)]

    given = (gate_w, value_w, down_w)

    def landing(matrix, index):
        if matrix == 2:
            return wd.at[index]
        return (wg, wv)[matrix].at[pl.ds(pl.multiple_of(index * kb, kb), kb), :]

    beside = z * ny + 1 - y

    def weight_y(matrix):
        return remote(
            column(given[matrix], 1 - y, matrix),
            landing(matrix, place),
            w_y.at[matrix],
            w_r.at[matrix, place],
            other_y,
        )

    def weight_arrival(matrix, index):
        return remote(
            landing(matrix, index),
            landing(matrix, index),
            w_y.at[matrix],
            w_r.at[matrix, index],
            other_y,
        )

    def weight_copy(matrix, to_z, passed):
        index = beside if passed else place
        source = landing(matrix, index) if passed else column(given[matrix], y, matrix)
        return remote(
            source,
            landing(matrix, index),
            w_s.at[matrix, to_z * ny + passed],
            w_r.at[matrix, index],
            (to_z, y, x, c),
        )

    def weight_relay(matrix, distance, passed, side):
        sign = 1 - 2 * side
        index = (z - sign * distance) * ny + (1 - y if passed else y)
        return remote(
            landing(matrix, index),
            landing(matrix, index),
            w_fwd.at[matrix, (distance - 1) * 4 + passed * 2 + side],
            w_r.at[matrix, index],
            (z + sign, y, x, c),
        )

    def relays(distance, side):
        sign = 1 - 2 * side
        source, to = z - sign * distance, z + sign
        return (source >= 0) & (source < nz) & (to >= 0) & (to < nz)

    def send_weights(matrix, passed, do):
        for sign in (1, -1):
            to = z + sign

            @pl.when((to >= 0) & (to < nz))
            def _():
                do(weight_copy(matrix, to, passed))

    def start(copy):
        copy.start()

    def pass_weights(matrix):
        weight_arrival(matrix, beside).wait_recv()
        send_weights(matrix, 1, start)

    def relay_weights(matrix, distance, passed):
        for side in range(2):

            @pl.when(relays(distance, side))
            def _():
                source = z - distance if side == 0 else z + distance
                weight_arrival(matrix, source * ny + (1 - y if passed else y)).wait_recv()
                weight_relay(matrix, distance, passed, side).start()

    def own_copy(matrix):
        return pltpu.make_async_copy(
            column(given[matrix], y, matrix), landing(matrix, place), local.at[matrix]
        )

    def await_weights(matrix, to_z):
        for to_y in range(ny):

            @pl.when((to_z != z) & jnp.logical_not(middle))
            def _():
                weight_arrival(matrix, to_z * ny + to_y).wait_recv()

    def tp_index(k):
        return lax.rem(x + k // nc, nx), lax.rem(c + k % nc, nc)

    def close_copy(k):
        to_x, to_c = tp_index(k)
        at = pl.ds(pl.multiple_of((to_x * nc + to_c) * cols, 128), cols)
        return remote(
            closing.at[:, at], close_rows(lane_at), cl_s.at[k], cl_r.at[k], (z, y, to_x, to_c)
        )

    def close_rows(index):
        return close_all.at[pl.ds(pl.multiple_of(index * cols, cols), cols), :]

    def close_arrival(k):
        at_x, at_c = tp_index(k)
        view = close_rows(at_x * nc + at_c)
        return remote(view, view, cl_s.at[k], cl_r.at[k], other_c)

    side_x = (1 - x) * nc + c

    def blend_view(g, index):
        return blend.at[:, pl.ds(pl.multiple_of(index * cols + g * gw, 128), gw)]

    def tp_copy(g, which):
        view = blend_view(g, (lane_at, lane_at, side_x)[which])
        to = (other_x, other_c, other_c)[which]
        return remote(view, view, tp_s.at[g, which], tp_r.at[g, which], to)

    def tp_arrival(g, which):
        view = blend_view(g, (side_x, x * nc + 1 - c, (1 - x) * nc + 1 - c)[which])
        return remote(view, view, tp_s.at[g, which], tp_r.at[g, which], other_c)

    weight_y(0).start()
    for matrix in range(3):
        send_weights(matrix, 0, start)
    for k in (2, 3, 1):
        close_copy(k).start()
    for matrix in range(3):
        own_copy(matrix).start()
    close_own = pltpu.make_async_copy(
        closing.at[:, pl.ds(pl.multiple_of(lane_at * cols, 128), cols)],
        close_rows(lane_at),
        local.at[3],
    )
    close_own.start()

    edge = wide.shape[0] - tile
    for source, start_at, size in pieces:
        wide[tile : tile + rows, start_at : start_at + size] = source[...].astype(F32)

    @pl.when(place > 0)
    def _():
        for i in range(3):
            halo_copy(0, i).wait_recv()
        wide[0:tile, :] = halo[0].astype(F32)

    @pl.when(place == 0)
    def _():
        wide[0:tile, :] = jnp.zeros((tile, wide.shape[1]), F32)

    @pl.when(place < last)
    def _():
        for i in range(3):
            halo_copy(1, i).wait_recv()
        wide[edge:, :] = halo[1].astype(F32)

    @pl.when(place == last)
    def _():
        wide[edge:, :] = jnp.zeros((tile, wide.shape[1]), F32)

    margin = taps_p.shape[0] // 2
    for (source, start_at, size), taps in zip(pieces, (taps_p, taps_i, taps_o)):

        def conv_columns(i, carried, start_at=start_at, taps=taps):
            into = pl.ds(pl.multiple_of(start_at + i * 128, 128), 128)
            tap = taps[:, pl.ds(pl.multiple_of(i * 128, 128), 128)]
            for r in range(0, rows, 128):
                summed = None
                for k in range(tap.shape[0]):
                    first = tile - margin + k + r
                    term = wide[first : first + 128, into] * tap[k : k + 1]
                    summed = term if summed is None else summed + term
                conv[r : r + 128, into] = jax.nn.silu(summed).astype(BF)
            return carried

        lax.fori_loop(0, size // 128, conv_columns, 0)

    def upright(row):
        shape = (heads, heads)
        same = lax.broadcasted_iota(jnp.int32, shape, 0) == lax.broadcasted_iota(
            jnp.int32, shape, 1
        )
        return jnp.sum(
            jnp.where(same, jnp.broadcast_to(row, shape), 0.0), axis=1, keepdims=True
        )

    def turned(array):
        blank = jnp.zeros((128 - 2 * heads, rows), F32)
        return jnp.concatenate([array, blank], axis=0).T

    raw = jnp.concatenate([pre[0], pre[1]], axis=0)
    steps_t = jnp.maximum(raw, 0.0) + jnp.log1p(jnp.exp(-jnp.abs(raw)))
    rates = jnp.exp(jnp.concatenate([upright(rate[0:1]), upright(rate[1:2])], axis=0))
    logs_t = jnp.concatenate([extra[0], extra[1]], axis=0) - steps_t * rates
    earlier = lax.broadcasted_iota(jnp.int32, (rows, rows), 0) <= lax.broadcasted_iota(
        jnp.int32, (rows, rows), 1
    )
    running_t = dot(logs_t, earlier.astype(F32), precision=lax.Precision.HIGHEST)
    before_t = running_t - logs_t
    run_t[...] = running_t
    exc_t[...] = before_t
    step_t[...] = steps_t
    running, before, steps = turned(running_t), turned(before_t), turned(steps_t)
    run_s[...] = running
    exc_s[...] = before
    whole = running[rows - 1 : rows]
    lane = lax.broadcasted_iota(jnp.int32, (rows, 128), 1)
    ends[...] = jnp.exp(jnp.where(lane < heads, whole - running, before)) * steps
    totals[place] = jnp.broadcast_to(whole, (8, 128))

    def spread(columns, first):
        low = lax.broadcasted_iota(jnp.int32, (columns.shape[0], 2 * head_w), 1) < head_w
        shape = (columns.shape[0], 2 * head_w)
        return jnp.where(
            low,
            jnp.broadcast_to(columns[:, first : first + 1], shape),
            jnp.broadcast_to(columns[:, first + 1 : first + 2], shape),
        )

    def scale_rows(i, carried):
        at = pl.ds(pl.multiple_of(i * 128, 128), 128)
        factors = ends[at, :]
        for d in range(2):
            for p in range(heads // 2):
                into = slice(p * 2 * head_w, (p + 1) * 2 * head_w)
                made = conv[at, into].astype(F32) * spread(factors, d * heads + 2 * p)
                start_at = d * heads * head_w + p * 2 * head_w
                scaled[at, start_at : start_at + 2 * head_w] = made.astype(BF)
        return carried

    lax.fori_loop(0, rows // 128, scale_rows, 0)
    in_at = payload.shape[1]
    out_at = in_at + ingest.shape[1]
    for d in range(2):
        for g in range(groups):
            first = d * heads * head_w + g * gw
            state = dot(
                scaled[:, first : first + gw],
                conv[:, in_at + g * STATE : in_at + (g + 1) * STATE],
                ((0,), (0,)),
            )
            sum_f[d, g] = state
            sum_h[d, g] = state.astype(BF)

    state_y = remote(sum_h, sum_y, sy_s, sy_r, other_y)
    state_y.start()

    def total_copy(k):
        to = (lax.rem(z + k // ny, nz), lax.rem(y + k % ny, ny), x, c)
        to_place = to[0] * ny + to[1]
        return remote(totals.at[place], totals.at[place], tot_s.at[k], tot_r.at[place], to)

    def total_arrival(k):
        index = lax.rem(z + k // ny, nz) * ny + lax.rem(y + k % ny, ny)
        return remote(totals.at[index], totals.at[index], tot_s.at[k], tot_r.at[index], other_y)

    for k in range(1, nz * ny):
        total_copy(k).start()

    state_y.wait_recv()
    total_arrival(1).wait_recv()

    def head_rows(ref_value, factors):
        return jnp.concatenate(
            [ref_value[e * head_w : (e + 1) * head_w] * factors[e] for e in range(per)], axis=0
        )

    def of_heads(row, d, g=None):
        result = []
        for e in range(per):
            picks = [
                row[:, d * heads + k * per + e : d * heads + k * per + e + 1] for k in range(groups)
            ]
            if g is None:
                result.append(jnp.where(y == 0, picks[0], picks[1]))
            else:
                result.append(picks[g])
        return result

    one_row = jnp.ones((1, 128), F32)
    plane_low = jnp.exp(totals[z * ny, 0:1])
    plane_high = jnp.exp(totals[z * ny + 1, 0:1])
    forward_own = of_heads(jnp.where(y == 0, plane_high, one_row), 0)
    forward_far = of_heads(jnp.where(y == 0, one_row, plane_high), 0)
    back_own = of_heads(jnp.where(y == 0, one_row, plane_low), 1)
    back_far = of_heads(jnp.where(y == 0, plane_low, one_row), 1)
    plane_out[0] = (
        head_rows(sum_f[0, y], forward_own) + head_rows(sum_y[0, y].astype(F32), forward_far)
    ).astype(BF)
    plane_out[1] = (
        head_rows(sum_f[1, y], back_own) + head_rows(sum_y[1, y].astype(F32), back_far)
    ).astype(BF)

    def plane_copy(k, d):
        return remote(
            plane_out.at[d], plane_in.at[z], pl_s.at[k], pl_r.at[z], (k, y, x, c)
        )

    for k in range(nz):
        for d in range(2):

            @pl.when((k > z) if d == 0 else (k < z))
            def _():
                plane_copy(k, d).start()

    weight_y(1).start()
    weight_y(2).start()
    relay_weights(0, 1, 0)
    relay_weights(1, 1, 0)
    pass_weights(0)

    def within(g):
        read = conv[:, out_at + g * STATE : out_at + (g + 1) * STATE]
        write = conv[:, in_at + g * STATE : in_at + (g + 1) * STATE]
        scores[...] = dot(read, write, ((1,), (1,)))
        for p in range(per // 2):
            pair = g * per + 2 * p
            into = slice(pair * head_w, (pair + 2) * head_w)

            def chunk(i, carried):
                at = pl.ds(pl.multiple_of(i * 128, 128), 128)
                t = lax.broadcasted_iota(jnp.int32, (128, rows), 0) + i * 128
                s = lax.broadcasted_iota(jnp.int32, (128, rows), 1)
                after, same = t > s, t == s
                values = conv[:, into]
                low = lax.broadcasted_iota(jnp.int32, values.shape, 1) < head_w
                summed = None
                for e in range(2):
                    f, b = pair + e, heads + pair + e
                    gap = jnp.where(
                        after,
                        run_s[at, f : f + 1] - run_t[f : f + 1, :],
                        exc_t[b : b + 1, :] - exc_s[at, b : b + 1],
                    )
                    step_f, step_b = step_t[f : f + 1, :], step_t[b : b + 1, :]
                    factor = jnp.where(after, step_f, jnp.where(same, step_f + step_b, step_b))
                    made = (scores[at, :] * jnp.exp(gap) * factor).astype(BF)
                    kept = jnp.where(low if e == 0 else jnp.logical_not(low), values, 0)
                    term = dot(made, kept.astype(BF))
                    summed = term if summed is None else summed + term
                mixed[at, into] = summed
                return carried

            lax.fori_loop(0, rows // 128, chunk, 0)

    within(0)
    for k in range(2, nz * ny):
        total_arrival(k).wait_recv()
    carry[...] = jnp.zeros_like(carry)
    for k in range(nz):
        for d in range(2):

            @pl.when((k < z) if d == 0 else (k > z))
            def _():
                remote(
                    plane_out.at[d], plane_in.at[k], pl_s.at[k], pl_r.at[k], other_y
                ).wait_recv()
                gone = jnp.zeros((1, 128), F32)
                for q in range(nz * ny):
                    if d == 0:
                        between = (q >= ny * (k + 1)) & (q < ny * z)
                    else:
                        between = (q >= ny * (z + 1)) & (q < ny * k)
                    gone = gone + jnp.where(between, totals[q, 0:1], 0.0)
                weights = of_heads(jnp.exp(gone), d)
                carry[d] = carry[d] + head_rows(plane_in[k].astype(F32), weights)

    for d in range(2):
        carry_all[d, y] = carry[d].astype(BF)

    def carry_copy(d):
        return remote(carry_all.at[d, y], carry_all.at[d, y], ca_s.at[d], ca_r.at[d], other_y)

    for d in range(2):
        carry_copy(d).start()

    within(1)
    pass_weights(1)

    for d in range(2):
        remote(
            carry_all.at[d, 1 - y], carry_all.at[d, 1 - y], ca_s.at[d], ca_r.at[d], other_y
        ).wait_recv()
    for g in range(groups):
        for d in range(2):
            through = plane_low if d == 0 else plane_high
            adds = y == 1 if d == 0 else y == 0
            weights = of_heads(jnp.where(adds, through, one_row), d, g)
            body = head_rows(carry_all[d, g].astype(F32), weights)
            entering[d, g] = (body + jnp.where(adds, sum_y[d, g].astype(F32), 0.0)).astype(BF)

    for g in range(groups):

        def finish(i, carried):
            at = pl.ds(pl.multiple_of(i * 128, 128), 128)
            read = conv[at, out_at + g * STATE : out_at + (g + 1) * STATE]
            fore = dot(read, entering[0, g], ((1,), (1,)))
            back = dot(read, entering[1, g], ((1,), (1,)))
            grown = jnp.exp(run_s[at, :])
            shrunk = jnp.exp(run_s[rows - 1 : rows, :] - exc_s[at, :])
            parts = []
            for p in range(per // 2):
                pair = g * per + 2 * p
                into = slice(pair * head_w, (pair + 2) * head_w)
                inner = slice(2 * p * head_w, 2 * (p + 1) * head_w)
                total = mixed[at, into] + fore[:, inner] * spread(grown, pair)
                total = total + back[:, inner] * spread(shrunk, heads + pair)
                parts.append(total * jax.nn.silu(valve[at, into].astype(F32)))
            gated = jnp.concatenate(parts, axis=1)
            mean = jnp.mean(gated * gated, axis=1, keepdims=True)
            made = gated * lax.rsqrt(mean + EPSILON) * gain[:, g * gw : (g + 1) * gw]
            blend[at, pl.ds(pl.multiple_of(lane_at * cols + g * gw, 128), gw)] = made.astype(BF)
            return carried

        lax.fori_loop(0, rows // 128, finish, 0)
        tp_copy(g, 0).start()
        tp_copy(g, 1).start()

    for matrix in range(2):
        relay_weights(matrix, 2, 0)
    relay_weights(0, 1, 1)

    close_own.wait()
    for k in range(1, nx * nc):
        close_arrival(k).wait_recv()
    for g in range(groups):
        tp_arrival(g, 0).wait_recv()
        tp_copy(g, 2).start()
    for g in range(groups):
        tp_arrival(g, 1).wait_recv()
        tp_arrival(g, 2).wait_recv()

    def row_view(which_y, index):
        return rows_n.at[
            pl.ds(pl.multiple_of(tile + which_y * rows, tile), rows),
            pl.ds(pl.multiple_of(index * cols, 128), cols),
        ]

    relay_weights(1, 1, 1)
    relay_weights(2, 1, 0)
    made = dot(blend[...], close_all[...]) + skip[...].astype(F32)
    mid_own[...] = made.astype(BF)
    rows_n[
        pl.ds(pl.multiple_of(tile + y * rows, tile), rows),
        pl.ds(pl.multiple_of(lane_at * cols, 128), cols),
    ] = mid_own[...]

    other_xy = (z, 1 - y, 1 - x, c)
    froms = ((y, x), (y, 1 - x), (1 - y, x), (1 - y, 1 - x))

    def row_copy(k):
        view = row_view(y, lane_at)
        to = (other_c, other_x, other_y, other_xy)[k]
        return remote(view, view, nb_s.at[k], nb_r.at[k], to)

    def row_pass(k, core, arriving=False):
        view = row_view(froms[k][0], froms[k][1] * nc + core)
        sem = (nb_r if arriving else nf_r).at[k]
        return remote(view, view, nf_s.at[k], sem, other_c)

    for k in (1, 2, 3, 0):
        row_copy(k).start()
    for k in (1, 2, 3):
        row_pass(k, c, arriving=True).wait_recv()
        row_pass(k, c).start()
        if k == 1:
            relay_weights(0, 2, 1)
            relay_weights(1, 2, 1)
    row_pass(0, 1 - c, arriving=True).wait_recv()
    for k in (1, 2, 3):
        row_pass(k, 1 - c).wait_recv()
    for k in range(4):
        row_copy(k).wait_send()
        if k:
            row_pass(k, c).wait_send()

    def normalize(i, carried):
        at = pl.ds(pl.multiple_of(tile + i * 128, tile), 128)
        squares = jnp.zeros((128, 1), F32)
        for first in range(0, width_all, 256):
            piece = rows_n[at, first : first + 256].astype(F32)
            squares = squares + jnp.sum(piece * piece, axis=1, keepdims=True)
        inverse = lax.rsqrt(squares / width_all + EPSILON)
        for first in range(0, width_all, 256):
            piece = rows_n[at, first : first + 256].astype(F32)
            piece = piece * inverse * norm_gain[:, first : first + 256]
            rows_n[at, first : first + 256] = piece.astype(BF)
        return carried

    lax.fori_loop(0, ny * rows // 128, normalize, 0)

    bottom = tile + ny * rows

    def edge_copy(side):
        if side == 0:
            src, dst = rows_n.at[pl.ds(bottom - tile, tile)], rows_n.at[pl.ds(0, tile)]
        else:
            src, dst = rows_n.at[pl.ds(tile, tile)], rows_n.at[pl.ds(bottom, tile)]
        to = (z + 1 if side == 0 else z - 1, y, x, c)
        return remote(src, dst, edge_s.at[side], edge_r.at[side], to)

    sends_up, sends_down = z < nz - 1, z > 0
    for side, cond in ((0, sends_up), (1, sends_down)):

        @pl.when(cond)
        def _():
            edge_copy(side).start()

    pass_weights(2)
    relay_weights(2, 2, 0)

    for matrix, (weight, made) in enumerate(((wg, made_g), (wv, made_v))):
        own_copy(matrix).wait()
        for k in range(nz):
            await_weights(matrix, k)

        def units(i, carried):
            at = pl.ds(pl.multiple_of(tile + i * rows, tile), rows)
            made[at, :] = dot(rows_n[at, :], weight[...]).astype(BF).astype(F32)
            return carried

        lax.fori_loop(0, ny, units, 0)

    relay_weights(2, 1, 1)

    @pl.when(z > 0)
    def _():
        edge_copy(0).wait_recv()

    @pl.when(z == 0)
    def _():
        rows_n[0:tile, :] = jnp.zeros((tile, width_all), BF)

    @pl.when(z < nz - 1)
    def _():
        edge_copy(1).wait_recv()

    @pl.when(z == nz - 1)
    def _():
        rows_n[bottom:, :] = jnp.zeros((tile, width_all), BF)

    both = jnp.concatenate([rows_n[0:tile, :], rows_n[bottom:, :]], axis=0)
    for weight, made in ((wg, made_g), (wv, made_v)):
        edges = dot(both, weight[...]).astype(BF).astype(F32)
        made[0:tile, :] = edges[0:tile]
        made[bottom:, :] = edges[tile:]

    ff_margin = gate_taps.shape[0] // 2

    def activate(i, carried):
        into = pl.ds(pl.multiple_of(i * 128, 128), 128)
        tap_at = pl.ds(pl.multiple_of(y * hid + i * 128, 128), 128)
        tap_g, tap_v = gate_taps[:, tap_at], value_taps[:, tap_at]
        for r in range(0, ny * rows, 128):
            pair = []
            for made, tap in ((made_g, tap_g), (made_v, tap_v)):
                summed = None
                for k in range(tap.shape[0]):
                    first = tile - ff_margin + k + r
                    term = made[first : first + 128, into] * tap[k : k + 1]
                    summed = term if summed is None else summed + term
                pair.append(summed)
            hidden[r : r + 128, into] = (jax.nn.silu(pair[0]) * pair[1]).astype(BF)
        return carried

    lax.fori_loop(0, hid // 128, activate, 0)

    own_copy(2).wait()

    def order(k):
        kept = near * (1 - 2 * k) + k if k < 2 else k
        return kept * (1 - 2 * half) + (nz - 1) * half

    def half_at(core):
        return pl.ds(pl.multiple_of(core * rows, tile), rows)

    def core_copy(i):
        return remote(
            part.at[i, half_at(1 - c)], part_in.at[i], core_s.at[i], core_r.at[i], other_c
        )

    def block_y(i):
        return y if i < nz else 1 - y

    def own_to(i):
        to_z = order(i % nz)
        slot, q = y * nx + x, block_y(i)
        return remote(
            part.at[i, half_at(c)],
            far_in.at[slot, q],
            own_s.at[i],
            own_r.at[slot, q],
            (z, c, to_z // nc, lax.rem(to_z, nc)),
        )

    def stays(i):
        to_z = order(i % nz)
        return (y == c) & (to_z // nc == x) & (lax.rem(to_z, nc) == c)

    count = nz * ny
    early = count // 2

    def settle(i):
        core_copy(i).wait_recv()

        @pl.when(stays(i))
        def _():
            own_sum[block_y(i)] = part_f[i % 2] + part_in[i].astype(F32)

        @pl.when(jnp.logical_not(stays(i)))
        def _():
            part[i, half_at(c)] = (part_f[i % 2] + part_in[i].astype(F32)).astype(BF)
            own_to(i).start()

    for i in range(count):
        to_z, to_y = order(i % nz), block_y(i)
        index = to_z * ny + to_y
        if i >= early:
            settle(i - 1)
        if i == early:
            relay_weights(2, 2, 1)

        @pl.when((to_z != z) & jnp.logical_not(middle))
        def _():
            weight_arrival(2, index).wait_recv()

        made = dot(hidden[...], wd[index])

        for core in range(nc):

            @pl.when(c == core)
            def _():
                away = (1 - core) * rows
                part[i, away : away + rows] = made[away : away + rows].astype(BF)
                core_copy(i).start()
                part_f[i % 2] = made[core * rows : (core + 1) * rows]

        if 0 < i < early:
            settle(i - 1)
    settle(count - 1)

    def far_wait(slot, q):
        view = far_in.at[slot, q]
        remote(view, view, own_s.at[0], own_r.at[slot, q], other_c).wait_recv()

    own_slot = y * nx + x
    for q in range(ny):

        @pl.when(c != y)
        def _():
            far_wait(own_slot, q)
            own_sum[q] = far_in[own_slot, q].astype(F32)

    for q in range(ny):
        total = own_sum[q]
        for k in range(1, ny * nx):
            slot = lax.rem(y + k // nx, ny) * nx + lax.rem(x + k % nx, nx)
            far_wait(slot, q)
            total = total + far_in[slot, q].astype(F32)
        into = slice(q * ob, (q + 1) * ob)
        out[:, into] = (mid_own[:, into].astype(F32) + total).astype(BF)

    def done(copy):
        copy.wait_send()

    @pl.when(place < last)
    def _():
        for i in range(3):
            halo_copy(0, i).wait_send()

    @pl.when(place > 0)
    def _():
        for i in range(3):
            halo_copy(1, i).wait_send()

    for matrix in range(3):
        weight_y(matrix).wait_send()
        for passed in range(2):
            send_weights(matrix, passed, done)

        for distance in range(1, nz - 1):
            for passed in range(2):
                for side in range(2):

                    @pl.when(relays(distance, side))
                    def _():
                        weight_relay(matrix, distance, passed, side).wait_send()

    for g in range(groups):
        for which in range(3):
            tp_copy(g, which).wait_send()
    for k in range(1, nx * nc):
        close_copy(k).wait_send()
    state_y.wait_send()
    for k in range(1, nz * ny):
        total_copy(k).wait_send()
    for k in range(nz):

        @pl.when(k != z)
        def _():
            plane_copy(k, 0).wait_send()

    for d in range(2):
        carry_copy(d).wait_send()
    for side, cond in ((0, sends_up), (1, sends_down)):

        @pl.when(cond)
        def _():
            edge_copy(side).wait_send()

    for i in range(count):
        core_copy(i).wait_send()

        @pl.when(jnp.logical_not(stays(i)))
        def _():
            own_to(i).wait_send()


def one_kernel(*args):
    (skip, valve, payload, ingest, observe, pre, rate, extra, tp_taps, ti_taps, to_taps) = args[:11]
    gain, closing, norm_gain, gate_w, value_w, gate_taps, value_taps, down_w = args[11:]
    nz, ny, nx, nc = (lax.axis_size(a) for a in ("z", "y", "x", "core"))
    rows, cols = skip.shape
    width = norm_gain.shape[0]
    groups = ingest.shape[1] // STATE
    gw = payload.shape[1] // groups
    joined = payload.shape[1] + ingest.shape[1] + observe.shape[1]
    hid = gate_w.shape[1] // ny
    ob = down_w.shape[1]
    count = nz * ny
    lanes_used = 2 * pre.shape[2]
    tile = 16
    tall = ny * rows + 2 * tile
    vmem, anywhere = pl.BlockSpec(memory_space=pltpu.VMEM), pl.BlockSpec(memory_space=pl.ANY)
    v = pltpu.VMEM
    sem = pltpu.SemaphoreType.DMA
    scratch = [
        v((2, tile, joined), BF),
        v((rows + 2 * tile, joined), F32),
        v((rows, joined), BF),
        v((rows, 128), F32),
        v((rows, 128), F32),
        v((lanes_used, rows), F32),
        v((lanes_used, rows), F32),
        v((lanes_used, rows), F32),
        v((rows, 128), F32),
        v((rows, 2 * payload.shape[1]), BF),
        v((2, groups, gw, STATE), F32),
        v((2, groups, gw, STATE), BF),
        v((2, groups, gw, STATE), BF),
        v((count, 8, 128), F32),
        v((2, gw, STATE), BF),
        v((nz, gw, STATE), BF),
        v((2, gw, STATE), F32),
        v((2, groups, gw, STATE), BF),
        v((2, groups, gw, STATE), BF),
        v((rows, rows), F32),
        v((rows, payload.shape[1]), F32),
        v((rows, width), BF),
        v((rows, cols), BF),
        v((width, cols), BF),
        v((tall, width), BF),
        v((width, hid), BF),
        v((width, hid), BF),
        v((count, hid, ob), BF),
        v((tall, hid), F32),
        v((tall, hid), F32),
        v((ny * rows, hid), BF),
        v((count, ny * rows, ob), BF),
        v((2, rows, ob), F32),
        v((count, rows, ob), BF),
        v((ny, rows, ob), F32),
        v((ny * nx, ny, rows, ob), BF),
        sem((2, 3)),
        sem((2, 3)),
        sem((groups, 3)),
        sem((groups, 3)),
        sem((3, count)),
        sem((3, count)),
        sem((3,)),
        sem((3, 4 * (nz - 2))),
        sem((nx * nc,)),
        sem((nx * nc,)),
        sem((count,)),
        sem((count,)),
        sem(()),
        sem(()),
        sem((nz,)),
        sem((nz,)),
        sem((2,)),
        sem((2,)),
        sem((4,)),
        sem((4,)),
        sem((4,)),
        sem((4,)),
        sem((2,)),
        sem((2,)),
        sem((count,)),
        sem((count,)),
        sem((count,)),
        sem((ny * nx, ny)),
        sem((4,)),
    ]
    operands = [
        *(skip, valve, payload, ingest, observe),
        *(jnp.swapaxes(pre, 1, 2), rate, jnp.swapaxes(extra, 1, 2)),
        *(tp_taps, ti_taps, to_taps, gain.reshape(1, -1), closing, norm_gain.reshape(1, -1)),
        *(gate_w, value_w, gate_taps, value_taps, down_w),
    ]
    staged = [i for i in range(len(operands)) if i not in (12, 14, 15, 18)]
    scratch += [v(operands[i].shape, operands[i].dtype) for i in staged]
    scratch.append(sem((len(staged),)))

    def entry(*refs):
        ins, rest = list(refs[: len(operands)]), refs[len(operands) :]
        held, arrived = rest[-len(staged) - 1 : -1], rest[-1]
        loads = []
        for k, i in enumerate(staged):
            loads.append(pltpu.make_async_copy(ins[i], held[k], arrived.at[k]))
            ins[i] = held[k]
        layer(loads, *ins, *rest[: -len(staged) - 1])

    flops = 2 * rows * width * (width + 3 * hid * ny)
    return pl.pallas_call(
        entry,
        out_shape=jax.ShapeDtypeStruct((rows, cols), BF),
        in_specs=[anywhere] * len(operands),
        out_specs=vmem,
        scratch_shapes=scratch,
        compiler_params=pltpu.CompilerParams(
            collective_id=0, has_side_effects=True, vmem_limit_bytes=67043328
        ),
        cost_estimate=pl.CostEstimate(flops=flops, bytes_accessed=2**24, transcendentals=0),
        name="layer",
    )(*operands)


def body_for(grid):
    sizes = tuple(grid.shape[a] for a in ("z", "y", "x", "core"))
    return one_kernel if sizes == (4, 2, 2, 2) else shards


def solution(mesh):
    sp, tp = mesh.shape["sp"], mesh.shape["tp"]
    ny = 2 ** (int(math.log2(sp)) // 2)
    nc = 2 if tp % 2 == 0 else 1
    grid = Mesh(
        mesh.devices.reshape(sp // ny, ny, tp // nc, nc), ("z", "y", "x", "core")
    )
    return jax.shard_map(
        body_for(grid),
        mesh=grid,
        in_specs=(
            P(SP, TP),
            P(SP, TP),
            P(SP, TP),
            P(SP, TP),
            P(SP, TP),
            P(None, SP, TP),
            P(None, TP),
            P(None, SP, TP),
            P(None, TP),
            P(None, TP),
            P(None, TP),
            P(TP),
            P(TP, None),
            P(),
            P(SP, TP),
            P(SP, TP),
            P(None, TP),
            P(None, TP),
            P(TP, SP),
        ),
        out_specs=P(SP, TP),
        check_vma=False,
    )
```

```python
import functools
import math

import jax
import jax.numpy as jnp
from jax import lax
from jax.experimental import pallas as pl
from jax.experimental.pallas import tpu as pltpu
from jax.sharding import Mesh
from jax.sharding import PartitionSpec as P

HEADS = 32
GROUPS = 8
STATE = 128
EPSILON = 1e-06
SP = ("z", "y")
TP = ("x", "core")


def shifted(block, axis, step):
    count = lax.axis_size(axis)
    return lax.ppermute(block, axis, [(i, (i + step) % count) for i in range(count)])


def moved(block, axis, step):
    count = lax.axis_size(axis)
    pairs = [(i, i + step) for i in range(count) if 0 <= i + step < count]
    return lax.ppermute(block, axis, pairs)


def grid_shifted(block, axes, steps):
    sizes = [lax.axis_size(a) for a in axes]
    pairs = []
    for source in range(sizes[0] * sizes[1]):
        first, second = divmod(source, sizes[1])
        target = ((first + steps[0]) % sizes[0]) * sizes[1] + (second + steps[1]) % sizes[1]
        pairs.append((source, target))
    return lax.ppermute(block, axes, pairs)


def ordered(by_step, index):
    count = len(by_step)
    result = []
    for owner in range(count):
        back = lax.rem(index - owner + count, count)
        block = by_step[0]
        for step in range(1, count):
            block = jnp.where(back == step, by_step[step], block)
        result.append(block)
    return result


def extended(block, axis, width):
    low = moved(block[-width:], axis, 1)
    high = moved(block[:width], axis, -1)
    return jnp.concatenate([low, block, high], axis=0)


def conv_rows(padded, kernel, length):
    summed = padded[0:length] * kernel[0]
    for offset in range(1, kernel.shape[0]):
        summed = summed + padded[offset : offset + length] * kernel[offset]
    return summed


def bdot(pattern, one, two):
    return jnp.einsum(pattern, one, two, preferred_element_type=jnp.float32)


def pack(decay, state):
    heads, width, depth = state.shape
    rows = jnp.broadcast_to(decay[:, None, None], (heads, 16, depth)).astype(jnp.bfloat16)
    return jnp.concatenate([state.astype(jnp.bfloat16), rows], axis=1)


def unpack(packed, width):
    body = packed.astype(jnp.float32)
    return body[:, width, 0], body[:, :width]


def carried_in(decay, state, sign):
    width = state.shape[1]
    count = lax.axis_size(SP)
    own = pack(decay, state)
    index = lax.axis_index(SP)

    def from_back(array, step):
        back, value = unpack(moved(array, SP, sign * step), width)
        source = index - sign * step
        inside = (source >= 0) & (source < count)
        return jnp.where(inside, back, 1.0), value

    near, far = from_back(own, 1), from_back(own, 2)
    total = near[1] + near[0][:, None, None] * far[1]
    product = near[0] * far[0]
    covered = 2
    while covered < count - 1:
        back, value = from_back(pack(product, total), covered)
        total = total + product[:, None, None] * value
        product = product * back
        covered *= 2
    return total


def tied(value, *others):
    marks = [other[(slice(0, 1),) * other.ndim] for other in others]
    return lax.optimization_barrier((value, *marks))[0]


def shared_rows(weight, axis_dim, out_dim, mark):
    count = lax.axis_size("y")
    index = lax.axis_index("y")
    part = weight.shape[axis_dim] // count
    received = []
    for step in range(count):
        at = lax.rem(index + step, count) * part
        block = lax.dynamic_slice_in_dim(weight, at, part, axis_dim)
        received.append(shifted(block, "y", step) if step else block)
    received = [tied(block, mark) for block in received]
    return jnp.concatenate(ordered(received, index), axis=out_dim)


def shards(
    skip_trunk_vector,
    valve_preactivation,
    projected_heads_payload,
    cluster_ingests,
    cluster_observers,
    pre_softplus_increments,
    attenuation_ln_rate,
    additional_attenuation,
    payload_conv_weights,
    ingest_conv_weights,
    observer_conv_weights,
    valved_cluster_factor,
    closing_map_matrix,
    dense_standardize_factor,
    dense_valve_map,
    dense_payload_map,
    valve_series_smoother,
    payload_series_smoother,
    dense_contract_map,
):
    rows = skip_trunk_vector.shape[0]
    own_cols = skip_trunk_vector.shape[1]
    head_count = pre_softplus_increments.shape[2]
    per_group = HEADS // GROUPS
    nx, nc, ny = lax.axis_size("x"), lax.axis_size("core"), lax.axis_size("y")
    ix, ic, iy = lax.axis_index("x"), lax.axis_index("core"), lax.axis_index("y")

    joined = jnp.concatenate([projected_heads_payload, cluster_ingests, cluster_observers], axis=1)
    taps_all = jnp.concatenate(
        [payload_conv_weights, ingest_conv_weights, observer_conv_weights], axis=1
    )
    padded = extended(joined, SP, taps_all.shape[0] // 2)

    convolved = jax.nn.silu(conv_rows(padded.astype(jnp.float32), taps_all, rows)).astype(
        jnp.bfloat16
    )
    gate_w = lax.all_gather(shared_rows(dense_valve_map, 1, 0, convolved), "z", axis=0, tiled=True)
    value_w = lax.all_gather(
        shared_rows(dense_payload_map, 1, 0, convolved), "z", axis=0, tiled=True
    )

    payload_columns = projected_heads_payload.shape[1]
    input_cols = cluster_ingests.shape[1]
    width = payload_columns // head_count
    groups = input_cols // STATE
    values = convolved[:, :payload_columns]
    inputs_g = convolved[:, payload_columns : payload_columns + input_cols].reshape(
        rows, groups, STATE
    )
    readout_g = convolved[:, payload_columns + input_cols :].reshape(rows, groups, STATE)

    steps = jax.nn.softplus(pre_softplus_increments)
    logs = additional_attenuation - steps * jnp.exp(attenuation_ln_rate)[:, None, :]
    running = jnp.cumsum(logs, axis=1)
    run_f = running[0]
    exc_b = running[1] - logs[1]
    total_f, total_b = running[0, -1], running[1, -1]

    end_f = jnp.exp(total_f[None] - run_f) * steps[0]
    end_b = jnp.exp(exc_b) * steps[1]
    ends = jnp.stack([end_f, end_b], axis=1)
    scaled = (
        ends[:, :, :, None] * values.astype(jnp.float32).reshape(rows, 1, head_count, width)
    ).astype(jnp.bfloat16)
    scaled = scaled.reshape(rows, 2, groups, per_group, width)
    summary = bdot("sdgep,sgn->dgepn", scaled, inputs_g).reshape(2, head_count, width, STATE)
    in_f = carried_in(jnp.exp(total_f), summary[0], 1)
    in_b = carried_in(jnp.exp(total_b), summary[1], -1)

    down_part = shared_rows(dense_contract_map, 0, 1, in_f)
    down_w = lax.all_gather(down_part, "z", axis=1, tiled=True)

    places = jnp.arange(rows, dtype=jnp.int32)
    after = places[:, None] > places[None, :]
    same = places[:, None] == places[None, :]
    run_fT, exc_bT = run_f.T, exc_b.T
    step_f, step_b = steps[0].T, steps[1].T
    gaps = jnp.where(
        after[None],
        run_fT[:, :, None] - run_fT[:, None, :],
        exc_bT[:, None, :] - exc_bT[:, :, None],
    )
    factor = jnp.where(
        after[None],
        step_f[:, None, :],
        jnp.where(same[None], (step_f + step_b)[:, None, :], step_b[:, None, :]),
    )
    scores = jnp.repeat(bdot("tgn,sgn->gts", readout_g, inputs_g), per_group, axis=0)
    weights = (scores * jnp.exp(gaps) * factor).astype(jnp.bfloat16)
    within = bdot("hts,shp->thp", weights, values.reshape(rows, head_count, width))

    def outer(state):
        grouped = state.astype(jnp.bfloat16).reshape(groups, per_group, width, STATE)
        return bdot("gepn,tgn->tgep", grouped, readout_g).reshape(rows, head_count, width)

    mixed = within + outer(in_f) * jnp.exp(run_f)[:, :, None]
    mixed = mixed + outer(in_b) * jnp.exp(total_b[None] - exc_b)[:, :, None]
    gated = mixed.reshape(rows, payload_columns) * jax.nn.silu(
        valve_preactivation.astype(jnp.float32)
    )
    grouped = gated.reshape(rows, groups, per_group * width)
    standardized = grouped * lax.rsqrt(jnp.mean(grouped * grouped, axis=2, keepdims=True) + EPSILON)
    blended = (standardized.reshape(rows, payload_columns) * valved_cluster_factor).astype(
        jnp.bfloat16
    )

    def column_block(matrix, dx, dc):
        at = (lax.rem(ix + dx, nx) * nc + lax.rem(ic + dc, nc)) * own_cols
        return lax.dynamic_slice_in_dim(matrix, at, own_cols, 1)

    def over_cores(terms):
        total = terms[0].astype(jnp.bfloat16).astype(jnp.float32)
        for dc in range(1, nc):
            total = total + shifted(terms[dc].astype(jnp.bfloat16), "core", dc).astype(jnp.float32)
        return total

    mapped = None
    for dx in list(range(1, nx)) + [0]:
        terms = [
            jnp.dot(
                blended,
                column_block(closing_map_matrix, dx, dc),
                preferred_element_type=jnp.float32,
            )
            for dc in range(nc)
        ]
        part = over_cores(terms)
        if dx:
            part = shifted(part.astype(jnp.bfloat16), "x", dx).astype(jnp.float32)
        mapped = part if mapped is None else mapped + part
    middle = (skip_trunk_vector.astype(jnp.float32) + mapped).astype(jnp.bfloat16)

    margin = valve_series_smoother.shape[0] // 2
    room = -(-margin // 16) * 16
    low = moved(middle[-margin:], SP, 1)
    high = moved(middle[:margin], SP, -1)
    blank = jnp.zeros((room - margin, own_cols), middle.dtype)
    wide = jnp.concatenate([blank, low, middle, high, blank], axis=0)

    def everywhere(block):
        by_y = []
        for dy in range(ny):
            by_x = []
            for dx in range(nx):
                got = grid_shifted(block, ("y", "x"), (dy, dx)) if dy or dx else block
                by_core = [got] + [shifted(got, "core", dc) for dc in range(1, nc)]
                by_x.append(jnp.concatenate(ordered(by_core, ic), axis=1))
            by_y.append(jnp.concatenate(ordered(by_x, ix), axis=1))
        return jnp.stack(ordered(by_y, iy))

    line = everywhere(wide).reshape(ny * (rows + 2 * room), -1).astype(jnp.float32)
    inverse = lax.rsqrt(jnp.mean(line * line, axis=1, keepdims=True) + EPSILON)
    normed = (line * inverse * dense_standardize_factor).astype(jnp.bfloat16)

    hidden_cols = gate_w.shape[1]
    gate_taps = lax.dynamic_slice_in_dim(valve_series_smoother, iy * hidden_cols, hidden_cols, 1)
    value_taps = lax.dynamic_slice_in_dim(payload_series_smoother, iy * hidden_cols, hidden_cols, 1)

    def spread(weight, taps):
        made = jnp.dot(normed, weight, preferred_element_type=jnp.float32).astype(jnp.bfloat16)
        made = made.reshape(ny, rows + 2 * room, hidden_cols).astype(jnp.float32)
        summed = None
        for offset in range(taps.shape[0]):
            start = room - margin + offset
            term = made[:, start : start + rows] * taps[offset]
            summed = term if summed is None else summed + term
        return summed

    gate_rows = spread(gate_w, gate_taps)
    value_rows = spread(value_w, value_taps)
    hidden = (jax.nn.silu(gate_rows) * value_rows).astype(jnp.bfloat16)

    order = [(dy, dx) for dy in range(ny) for dx in range(nx)]
    down = None
    for dy, dx in order[1:] + order[:1]:
        wanted = lax.dynamic_index_in_dim(hidden, lax.rem(iy + dy, ny), 0, keepdims=False)
        terms = [
            jnp.dot(wanted, column_block(down_w, dx, dc), preferred_element_type=jnp.float32)
            for dc in range(nc)
        ]
        part = over_cores(terms)
        if dy or dx:
            part = grid_shifted(part.astype(jnp.bfloat16), ("y", "x"), (dy, dx)).astype(jnp.float32)
        down = part if down is None else down + part
    return (middle.astype(jnp.float32) + down).astype(jnp.bfloat16)


MESH = pl.DeviceIdType.MESH
BF = jnp.bfloat16
F32 = jnp.float32


def dot(one, two, dims=((1,), (0,)), precision=None):
    return lax.dot_general(
        one, two, (dims, ((), ())), preferred_element_type=F32, precision=precision
    )


def layer(
    loads,
    skip,
    valve,
    payload,
    ingest,
    observe,
    pre,
    rate,
    extra,
    taps_p,
    taps_i,
    taps_o,
    gain,
    closing,
    norm_gain,
    gate_w,
    value_w,
    gate_taps,
    value_taps,
    down_w,
    out,
    halo,
    wide,
    conv,
    run_s,
    exc_s,
    run_t,
    exc_t,
    step_t,
    ends,
    scaled,
    sum_f,
    sum_h,
    sum_y,
    totals,
    plane_out,
    plane_in,
    carry,
    carry_all,
    entering,
    scores,
    mixed,
    blend,
    mid_own,
    close_all,
    rows_n,
    wg,
    wv,
    wd,
    made_g,
    made_v,
    hidden,
    part,
    part_f,
    part_in,
    own_sum,
    far_in,
    halo_s,
    halo_r,
    tp_s,
    tp_r,
    w_s,
    w_r,
    w_y,
    w_fwd,
    cl_s,
    cl_r,
    tot_s,
    tot_r,
    sy_s,
    sy_r,
    pl_s,
    pl_r,
    ca_s,
    ca_r,
    nb_s,
    nb_r,
    nf_s,
    nf_r,
    edge_s,
    edge_r,
    core_s,
    core_r,
    own_s,
    own_r,
    local,
):
    nz, ny, nx, nc = (lax.axis_size(a) for a in ("z", "y", "x", "core"))
    z, y, x, c = (lax.axis_index(a) for a in ("z", "y", "x", "core"))
    place, lane_at = z * ny + y, x * nc + c
    rows, cols = skip.shape
    width_all = blend.shape[1]
    heads = pre.shape[1]
    groups = ingest.shape[1] // STATE
    per = heads // groups
    head_w = payload.shape[1] // heads
    gw = per * head_w
    hid = wg.shape[1]
    kb = gate_w.shape[0]
    ob = down_w.shape[1]
    tile = 16
    other_y, other_x, other_c = (z, 1 - y, x, c), (z, y, 1 - x, c), (z, y, x, 1 - c)
    half = z // 2
    near = z * (1 - 2 * half) + (nz - 1) * half
    middle = (z > 0) & (z < nz - 1)

    def remote(src, dst, send, recv, to):
        return pltpu.make_async_remote_copy(
            src_ref=src,
            dst_ref=dst,
            send_sem=send,
            recv_sem=recv,
            device_id=to,
            device_id_type=MESH,
        )

    for load in loads:
        load.start()
    barrier = pltpu.get_barrier_semaphore()
    greeted = 0
    for k in range(1, nz * ny):
        to = (lax.rem(z + k // ny, nz), lax.rem(y + k % ny, ny), x, c)
        pl.semaphore_signal(barrier, inc=1, device_id=to, device_id_type=MESH)
        greeted += 1
    for k in range(1, nx * nc):
        for dy in range(ny):
            to = (z, lax.rem(y + dy, ny), lax.rem(x + k // nc, nx), lax.rem(c + k % nc, nc))
            pl.semaphore_signal(barrier, inc=1, device_id=to, device_id_type=MESH)
            greeted += 1
    pl.semaphore_wait(barrier, greeted)
    for load in loads:
        load.wait()

    pieces = []
    at = 0
    for source in (payload, ingest, observe):
        pieces.append((source, at, source.shape[1]))
        at += source.shape[1]

    def halo_copy(side, i):
        source, start, size = pieces[i]
        other = place + 1 if side == 0 else place - 1
        to = (other // ny, lax.rem(other + ny, ny), x, c)
        src = source.at[pl.ds(rows - tile, tile)] if side == 0 else source.at[pl.ds(0, tile)]
        return remote(
            src,
            halo.at[side, :, pl.ds(start, size)],
            halo_s.at[side, i],
            halo_r.at[side, i],
            to,
        )

    last = nz * ny - 1

    @pl.when(place < last)
    def _():
        for i in range(3):
            halo_copy(0, i).start()

    @pl.when(place > 0)
    def _():
        for i in range(3):
            halo_copy(1, i).start()

    def column(ref, to_y, matrix):
        at = pl.multiple_of(to_y * hid, 128)
        if matrix == 2:
            return ref.at[pl.ds(at, hid), :]
        return ref.at[:, pl.ds(at, hid)]

    given = (gate_w, value_w, down_w)

    def landing(matrix, index):
        if matrix == 2:
            return wd.at[index]
        return (wg, wv)[matrix].at[pl.ds(pl.multiple_of(index * kb, kb), kb), :]

    beside = z * ny + 1 - y

    def weight_y(matrix):
        return remote(
            column(given[matrix], 1 - y, matrix),
            landing(matrix, place),
            w_y.at[matrix],
            w_r.at[matrix, place],
            other_y,
        )

    def weight_arrival(matrix, index):
        return remote(
            landing(matrix, index),
            landing(matrix, index),
            w_y.at[matrix],
            w_r.at[matrix, index],
            other_y,
        )

    def weight_copy(matrix, to_z, passed):
        index = beside if passed else place
        source = landing(matrix, index) if passed else column(given[matrix], y, matrix)
        return remote(
            source,
            landing(matrix, index),
            w_s.at[matrix, to_z * ny + passed],
            w_r.at[matrix, index],
            (to_z, y, x, c),
        )

    def weight_relay(matrix, distance, passed, side):
        sign = 1 - 2 * side
        index = (z - sign * distance) * ny + (1 - y if passed else y)
        return remote(
            landing(matrix, index),
            landing(matrix, index),
            w_fwd.at[matrix, (distance - 1) * 4 + passed * 2 + side],
            w_r.at[matrix, index],
            (z + sign, y, x, c),
        )

    def relays(distance, side):
        sign = 1 - 2 * side
        source, to = z - sign * distance, z + sign
        return (source >= 0) & (source < nz) & (to >= 0) & (to < nz)

    def waits(to):
        return middle & (x == half) & ((to == 0) | (to == nz - 1))

    def send_weights(matrix, passed, do, kept=None):
        for sign in (1, -1):
            to = z + sign
            goes = (to >= 0) & (to < nz)
            if kept is not None:
                goes = goes & (waits(to) if kept else jnp.logical_not(waits(to)))

            @pl.when(goes)
            def _():
                do(weight_copy(matrix, to, passed))

    def start(copy):
        copy.start()

    def pass_weights(matrix):
        weight_arrival(matrix, beside).wait_recv()
        send_weights(matrix, 1, start)

    def relay_weights(matrix, distance, passed):
        for side in range(2):

            @pl.when(relays(distance, side))
            def _():
                source = z - distance if side == 0 else z + distance
                weight_arrival(matrix, source * ny + (1 - y if passed else y)).wait_recv()
                weight_relay(matrix, distance, passed, side).start()

    def own_copy(matrix):
        return pltpu.make_async_copy(
            column(given[matrix], y, matrix), landing(matrix, place), local.at[matrix]
        )

    def await_weights(matrix, to_z):
        for to_y in range(ny):

            @pl.when((to_z != z) & jnp.logical_not(middle))
            def _():
                weight_arrival(matrix, to_z * ny + to_y).wait_recv()

    def tp_index(k):
        return lax.rem(x + k // nc, nx), lax.rem(c + k % nc, nc)

    def close_copy(k):
        to_x, to_c = tp_index(k)
        at = pl.ds(pl.multiple_of((to_x * nc + to_c) * cols, 128), cols)
        return remote(
            closing.at[:, at], close_rows(lane_at), cl_s.at[k], cl_r.at[k], (z, y, to_x, to_c)
        )

    def close_rows(index):
        return close_all.at[pl.ds(pl.multiple_of(index * cols, cols), cols), :]

    def close_arrival(k):
        at_x, at_c = tp_index(k)
        view = close_rows(at_x * nc + at_c)
        return remote(view, view, cl_s.at[k], cl_r.at[k], other_c)

    side_x = (1 - x) * nc + c

    def blend_view(g, index):
        return blend.at[:, pl.ds(pl.multiple_of(index * cols + g * gw, 128), gw)]

    def tp_copy(g, which):
        view = blend_view(g, (lane_at, lane_at, side_x)[which])
        to = (other_x, other_c, other_c)[which]
        return remote(view, view, tp_s.at[g, which], tp_r.at[g, which], to)

    def tp_arrival(g, which):
        view = blend_view(g, (side_x, x * nc + 1 - c, (1 - x) * nc + 1 - c)[which])
        return remote(view, view, tp_s.at[g, which], tp_r.at[g, which], other_c)

    weight_y(0).start()
    for matrix in range(2):
        send_weights(matrix, 0, start)
    for k in (2, 3, 1):
        close_copy(k).start()
    for matrix in range(3):
        own_copy(matrix).start()
    close_own = pltpu.make_async_copy(
        closing.at[:, pl.ds(pl.multiple_of(lane_at * cols, 128), cols)],
        close_rows(lane_at),
        local.at[3],
    )
    close_own.start()

    edge = wide.shape[0] - tile
    for source, start_at, size in pieces:
        wide[tile : tile + rows, start_at : start_at + size] = source[...].astype(F32)

    @pl.when(place > 0)
    def _():
        for i in range(3):
            halo_copy(0, i).wait_recv()
        wide[0:tile, :] = halo[0].astype(F32)

    @pl.when(place == 0)
    def _():
        wide[0:tile, :] = jnp.zeros((tile, wide.shape[1]), F32)

    @pl.when(place < last)
    def _():
        for i in range(3):
            halo_copy(1, i).wait_recv()
        wide[edge:, :] = halo[1].astype(F32)

    @pl.when(place == last)
    def _():
        wide[edge:, :] = jnp.zeros((tile, wide.shape[1]), F32)

    margin = taps_p.shape[0] // 2
    for (source, start_at, size), taps in zip(pieces, (taps_p, taps_i, taps_o)):

        def conv_columns(i, carried, start_at=start_at, taps=taps):
            into = pl.ds(pl.multiple_of(start_at + i * 128, 128), 128)
            tap = taps[:, pl.ds(pl.multiple_of(i * 128, 128), 128)]
            for r in range(0, rows, 128):
                summed = None
                for k in range(tap.shape[0]):
                    first = tile - margin + k + r
                    term = wide[first : first + 128, into] * tap[k : k + 1]
                    summed = term if summed is None else summed + term
                conv[r : r + 128, into] = jax.nn.silu(summed).astype(BF)
            return carried

        lax.fori_loop(0, size // 128, conv_columns, 0)

    def upright(row):
        shape = (heads, heads)
        same = lax.broadcasted_iota(jnp.int32, shape, 0) == lax.broadcasted_iota(
            jnp.int32, shape, 1
        )
        return jnp.sum(
            jnp.where(same, jnp.broadcast_to(row, shape), 0.0), axis=1, keepdims=True
        )

    def turned(array):
        blank = jnp.zeros((128 - 2 * heads, rows), F32)
        return jnp.concatenate([array, blank], axis=0).T

    raw = jnp.concatenate([pre[0], pre[1]], axis=0)
    steps_t = jnp.maximum(raw, 0.0) + jnp.log1p(jnp.exp(-jnp.abs(raw)))
    rates = jnp.exp(jnp.concatenate([upright(rate[0:1]), upright(rate[1:2])], axis=0))
    logs_t = jnp.concatenate([extra[0], extra[1]], axis=0) - steps_t * rates
    earlier = lax.broadcasted_iota(jnp.int32, (rows, rows), 0) <= lax.broadcasted_iota(
        jnp.int32, (rows, rows), 1
    )
    running_t = dot(logs_t, earlier.astype(F32), precision=lax.Precision.HIGHEST)
    before_t = running_t - logs_t
    run_t[...] = running_t
    exc_t[...] = before_t
    step_t[...] = steps_t
    running, before, steps = turned(running_t), turned(before_t), turned(steps_t)
    run_s[...] = running
    exc_s[...] = before
    whole = running[rows - 1 : rows]
    lane = lax.broadcasted_iota(jnp.int32, (rows, 128), 1)
    ends[...] = jnp.exp(jnp.where(lane < heads, whole - running, before)) * steps
    totals[place] = jnp.broadcast_to(whole, (8, 128))

    def spread(columns, first):
        low = lax.broadcasted_iota(jnp.int32, (columns.shape[0], 2 * head_w), 1) < head_w
        shape = (columns.shape[0], 2 * head_w)
        return jnp.where(
            low,
            jnp.broadcast_to(columns[:, first : first + 1], shape),
            jnp.broadcast_to(columns[:, first + 1 : first + 2], shape),
        )

    def scale_rows(i, carried):
        at = pl.ds(pl.multiple_of(i * 128, 128), 128)
        factors = ends[at, :]
        for d in range(2):
            for p in range(heads // 2):
                into = slice(p * 2 * head_w, (p + 1) * 2 * head_w)
                made = conv[at, into].astype(F32) * spread(factors, d * heads + 2 * p)
                start_at = d * heads * head_w + p * 2 * head_w
                scaled[at, start_at : start_at + 2 * head_w] = made.astype(BF)
        return carried

    lax.fori_loop(0, rows // 128, scale_rows, 0)
    in_at = payload.shape[1]
    out_at = in_at + ingest.shape[1]
    for d in range(2):
        for g in range(groups):
            first = d * heads * head_w + g * gw
            state = dot(
                scaled[:, first : first + gw],
                conv[:, in_at + g * STATE : in_at + (g + 1) * STATE],
                ((0,), (0,)),
            )
            sum_f[d, g] = state
            sum_h[d, g] = state.astype(BF)

    state_y = remote(sum_h, sum_y, sy_s, sy_r, other_y)
    state_y.start()

    total_y = remote(totals.at[place], totals.at[place], tot_s, tot_r, other_y)
    total_y.start()
    weight_y(1).start()

    state_y.wait_recv()
    remote(totals.at[beside], totals.at[beside], tot_s, tot_r, other_y).wait_recv()

    def head_rows(ref_value, factors):
        return jnp.concatenate(
            [ref_value[e * head_w : (e + 1) * head_w] * factors[e] for e in range(per)], axis=0
        )

    def of_heads(row, d, g=None):
        result = []
        for e in range(per):
            picks = [
                row[:, d * heads + k * per + e : d * heads + k * per + e + 1] for k in range(groups)
            ]
            if g is None:
                result.append(jnp.where(y == 0, picks[0], picks[1]))
            else:
                result.append(picks[g])
        return result

    one_row = jnp.ones((1, 128), F32)
    plane_low = jnp.exp(totals[z * ny, 0:1])
    plane_high = jnp.exp(totals[z * ny + 1, 0:1])
    forward_own = of_heads(jnp.where(y == 0, plane_high, one_row), 0)
    forward_far = of_heads(jnp.where(y == 0, one_row, plane_high), 0)
    back_own = of_heads(jnp.where(y == 0, one_row, plane_low), 1)
    back_far = of_heads(jnp.where(y == 0, plane_low, one_row), 1)
    plane_out[0] = (
        head_rows(sum_f[0, y], forward_own) + head_rows(sum_y[0, y].astype(F32), forward_far)
    ).astype(BF)
    plane_out[1] = (
        head_rows(sum_f[1, y], back_own) + head_rows(sum_y[1, y].astype(F32), back_far)
    ).astype(BF)

    def plane_copy(d):
        to = z + 1 if d == 0 else z - 1
        return remote(
            plane_out.at[d], plane_in.at[d], pl_s.at[d], pl_r.at[d], (to, y, x, c)
        )

    plane_gone = plane_low * plane_high
    ranks = (z, nz - 1 - z)

    def take(d):
        plane_copy(d).wait_recv()
        carry[d] = plane_in[d].astype(F32)

    def hop(step):
        for d in range(2):

            @pl.when(ranks[d] == step)
            def _():
                if step:
                    take(d)
                    grown = head_rows(carry[d], of_heads(plane_gone, d))
                    plane_out[d] = (grown + plane_out[d].astype(F32)).astype(BF)
                plane_copy(d).start()

    carry[...] = jnp.zeros_like(carry)
    hop(0)

    weight_y(2).start()
    relay_weights(0, 1, 0)
    relay_weights(1, 1, 0)

    def within(g):
        read = conv[:, out_at + g * STATE : out_at + (g + 1) * STATE]
        write = conv[:, in_at + g * STATE : in_at + (g + 1) * STATE]
        scores[...] = dot(read, write, ((1,), (1,)))
        for p in range(per // 2):
            pair = g * per + 2 * p
            into = slice(pair * head_w, (pair + 2) * head_w)

            def chunk(i, carried):
                at = pl.ds(pl.multiple_of(i * 128, 128), 128)
                t = lax.broadcasted_iota(jnp.int32, (128, rows), 0) + i * 128
                s = lax.broadcasted_iota(jnp.int32, (128, rows), 1)
                after, same = t > s, t == s
                values = conv[:, into]
                low = lax.broadcasted_iota(jnp.int32, values.shape, 1) < head_w
                summed = None
                for e in range(2):
                    f, b = pair + e, heads + pair + e
                    gap = jnp.where(
                        after,
                        run_s[at, f : f + 1] - run_t[f : f + 1, :],
                        exc_t[b : b + 1, :] - exc_s[at, b : b + 1],
                    )
                    step_f, step_b = step_t[f : f + 1, :], step_t[b : b + 1, :]
                    factor = jnp.where(after, step_f, jnp.where(same, step_f + step_b, step_b))
                    made = (scores[at, :] * jnp.exp(gap) * factor).astype(BF)
                    kept = jnp.where(low if e == 0 else jnp.logical_not(low), values, 0)
                    term = dot(made, kept.astype(BF))
                    summed = term if summed is None else summed + term
                mixed[at, into] = summed
                return carried

            lax.fori_loop(0, rows // 128, chunk, 0)

    within(0)
    hop(1)
    pass_weights(0)
    within(1)
    for step in range(2, nz - 1):
        hop(step)
    pass_weights(1)
    for d in range(2):

        @pl.when(ranks[d] == nz - 1)
        def _():
            take(d)

    for d in range(2):
        carry_all[d, y] = carry[d].astype(BF)

    def carry_copy(d):
        return remote(carry_all.at[d, y], carry_all.at[d, y], ca_s.at[d], ca_r.at[d], other_y)

    for d in range(2):
        carry_copy(d).start()


    for d in range(2):
        remote(
            carry_all.at[d, 1 - y], carry_all.at[d, 1 - y], ca_s.at[d], ca_r.at[d], other_y
        ).wait_recv()
    for g in range(groups):
        for d in range(2):
            through = plane_low if d == 0 else plane_high
            adds = y == 1 if d == 0 else y == 0
            weights = of_heads(jnp.where(adds, through, one_row), d, g)
            body = head_rows(carry_all[d, g].astype(F32), weights)
            entering[d, g] = (body + jnp.where(adds, sum_y[d, g].astype(F32), 0.0)).astype(BF)

    for g in range(groups):

        def finish(i, carried):
            at = pl.ds(pl.multiple_of(i * 128, 128), 128)
            read = conv[at, out_at + g * STATE : out_at + (g + 1) * STATE]
            fore = dot(read, entering[0, g], ((1,), (1,)))
            back = dot(read, entering[1, g], ((1,), (1,)))
            grown = jnp.exp(run_s[at, :])
            shrunk = jnp.exp(run_s[rows - 1 : rows, :] - exc_s[at, :])
            parts = []
            for p in range(per // 2):
                pair = g * per + 2 * p
                into = slice(pair * head_w, (pair + 2) * head_w)
                inner = slice(2 * p * head_w, 2 * (p + 1) * head_w)
                total = mixed[at, into] + fore[:, inner] * spread(grown, pair)
                total = total + back[:, inner] * spread(shrunk, heads + pair)
                parts.append(total * jax.nn.silu(valve[at, into].astype(F32)))
            gated = jnp.concatenate(parts, axis=1)
            mean = jnp.mean(gated * gated, axis=1, keepdims=True)
            made = gated * lax.rsqrt(mean + EPSILON) * gain[:, g * gw : (g + 1) * gw]
            blend[at, pl.ds(pl.multiple_of(lane_at * cols + g * gw, 128), gw)] = made.astype(BF)
            return carried

        lax.fori_loop(0, rows // 128, finish, 0)
        tp_copy(g, 0).start()
        tp_copy(g, 1).start()

    for matrix in range(2):
        relay_weights(matrix, 2, 0)
    relay_weights(0, 1, 1)

    close_own.wait()
    for k in range(1, nx * nc):
        close_arrival(k).wait_recv()
    for g in range(groups):
        tp_arrival(g, 0).wait_recv()
        tp_copy(g, 2).start()
    for g in range(groups):
        tp_arrival(g, 1).wait_recv()
        tp_arrival(g, 2).wait_recv()

    def row_view(which_y, index):
        return rows_n.at[
            pl.ds(pl.multiple_of(tile + which_y * rows, tile), rows),
            pl.ds(pl.multiple_of(index * cols, 128), cols),
        ]

    relay_weights(1, 1, 1)
    made = dot(blend[...], close_all[...]) + skip[...].astype(F32)
    mid_own[...] = made.astype(BF)
    rows_n[
        pl.ds(pl.multiple_of(tile + y * rows, tile), rows),
        pl.ds(pl.multiple_of(lane_at * cols, 128), cols),
    ] = mid_own[...]

    other_xy = (z, 1 - y, 1 - x, c)
    froms = ((y, x), (y, 1 - x), (1 - y, x), (1 - y, 1 - x))

    def row_copy(k):
        view = row_view(y, lane_at)
        to = (other_c, other_x, other_y, other_xy)[k]
        return remote(view, view, nb_s.at[k], nb_r.at[k], to)

    def row_pass(k, core, arriving=False):
        view = row_view(froms[k][0], froms[k][1] * nc + core)
        sem = (nb_r if arriving else nf_r).at[k]
        return remote(view, view, nf_s.at[k], sem, other_c)

    for k in (1, 2, 3, 0):
        row_copy(k).start()
    for k in (1, 2, 3):
        row_pass(k, c, arriving=True).wait_recv()
        row_pass(k, c).start()
        if k == 1:
            relay_weights(0, 2, 1)
            relay_weights(1, 2, 1)
            send_weights(2, 0, start)
    row_pass(0, 1 - c, arriving=True).wait_recv()
    for k in (1, 2, 3):
        row_pass(k, 1 - c).wait_recv()
    for k in range(4):
        row_copy(k).wait_send()
        if k:
            row_pass(k, c).wait_send()

    def normalize(i, carried):
        at = pl.ds(pl.multiple_of(tile + i * 128, tile), 128)
        squares = jnp.zeros((128, 1), F32)
        for first in range(0, width_all, 256):
            piece = rows_n[at, first : first + 256].astype(F32)
            squares = squares + jnp.sum(piece * piece, axis=1, keepdims=True)
        inverse = lax.rsqrt(squares / width_all + EPSILON)
        for first in range(0, width_all, 256):
            piece = rows_n[at, first : first + 256].astype(F32)
            piece = piece * inverse * norm_gain[:, first : first + 256]
            rows_n[at, first : first + 256] = piece.astype(BF)
        return carried

    lax.fori_loop(0, ny * rows // 128, normalize, 0)

    bottom = tile + ny * rows

    def edge_copy(side):
        if side == 0:
            src, dst = rows_n.at[pl.ds(bottom - tile, tile)], rows_n.at[pl.ds(0, tile)]
        else:
            src, dst = rows_n.at[pl.ds(tile, tile)], rows_n.at[pl.ds(bottom, tile)]
        to = (z + 1 if side == 0 else z - 1, y, x, c)
        return remote(src, dst, edge_s.at[side], edge_r.at[side], to)

    sends_up, sends_down = z < nz - 1, z > 0
    for side, cond in ((0, sends_up), (1, sends_down)):

        @pl.when(cond)
        def _():
            edge_copy(side).start()

    weight_arrival(2, beside).wait_recv()
    send_weights(2, 1, start, kept=False)

    for matrix, (weight, made) in enumerate(((wg, made_g), (wv, made_v))):
        if matrix == 1:
            relay_weights(2, 1, 0)
        own_copy(matrix).wait()
        for k in range(nz):
            await_weights(matrix, k)

        def units(i, carried):
            at = pl.ds(pl.multiple_of(tile + i * rows, tile), rows)
            made[at, :] = dot(rows_n[at, :], weight[...]).astype(BF).astype(F32)
            return carried

        lax.fori_loop(0, ny, units, 0)

    relay_weights(2, 2, 0)
    relay_weights(2, 1, 1)

    @pl.when(z > 0)
    def _():
        edge_copy(0).wait_recv()

    @pl.when(z == 0)
    def _():
        rows_n[0:tile, :] = jnp.zeros((tile, width_all), BF)

    @pl.when(z < nz - 1)
    def _():
        edge_copy(1).wait_recv()

    @pl.when(z == nz - 1)
    def _():
        rows_n[bottom:, :] = jnp.zeros((tile, width_all), BF)

    both = jnp.concatenate([rows_n[0:tile, :], rows_n[bottom:, :]], axis=0)
    for weight, made in ((wg, made_g), (wv, made_v)):
        edges = dot(both, weight[...]).astype(BF).astype(F32)
        made[0:tile, :] = edges[0:tile]
        made[bottom:, :] = edges[tile:]

    ff_margin = gate_taps.shape[0] // 2

    def activate(i, carried):
        into = pl.ds(pl.multiple_of(i * 128, 128), 128)
        tap_at = pl.ds(pl.multiple_of(y * hid + i * 128, 128), 128)
        tap_g, tap_v = gate_taps[:, tap_at], value_taps[:, tap_at]
        for r in range(0, ny * rows, 128):
            pair = []
            for made, tap in ((made_g, tap_g), (made_v, tap_v)):
                summed = None
                for k in range(tap.shape[0]):
                    first = tile - ff_margin + k + r
                    term = made[first : first + 128, into] * tap[k : k + 1]
                    summed = term if summed is None else summed + term
                pair.append(summed)
            hidden[r : r + 128, into] = (jax.nn.silu(pair[0]) * pair[1]).astype(BF)
        return carried

    lax.fori_loop(0, hid // 128, activate, 0)

    own_copy(2).wait()

    def order(i):
        k = i % nz
        kept = near * (1 - 2 * k) + k if k < 2 else k
        if i >= nz and k:
            turn = (1 - near) * (1 - jnp.abs(x - half))
            kept = kept + turn * (k % (nz - 1) + 1 - k)
        return kept * (1 - 2 * half) + (nz - 1) * half

    def half_at(core):
        return pl.ds(pl.multiple_of(core * rows, tile), rows)

    def core_copy(i):
        return remote(
            part.at[i, half_at(1 - c)], part_in.at[i], core_s.at[i], core_r.at[i], other_c
        )

    def block_y(i):
        return y if i < nz else 1 - y

    def own_to(i):
        to_z = order(i)
        slot, q = y * nx + x, block_y(i)
        return remote(
            part.at[i, half_at(c)],
            far_in.at[slot, q],
            own_s.at[i],
            own_r.at[slot, q],
            (z, c, to_z // nc, lax.rem(to_z, nc)),
        )

    def stays(i):
        to_z = order(i)
        return (y == c) & (to_z // nc == x) & (lax.rem(to_z, nc) == c)

    count = nz * ny
    early = count // 2

    def settle(i):
        core_copy(i).wait_recv()

        @pl.when(stays(i))
        def _():
            own_sum[block_y(i)] = part_f[i % 2] + part_in[i].astype(F32)

        @pl.when(jnp.logical_not(stays(i)))
        def _():
            part[i, half_at(c)] = (part_f[i % 2] + part_in[i].astype(F32)).astype(BF)
            own_to(i).start()

    for i in range(count):
        to_z, to_y = order(i), block_y(i)
        index = to_z * ny + to_y
        if i >= early:
            settle(i - 1)
        if i == early:
            relay_weights(2, 2, 1)

        @pl.when((to_z != z) & jnp.logical_not(middle))
        def _():
            weight_arrival(2, index).wait_recv()

        made = dot(hidden[...], wd[index])

        for core in range(nc):

            @pl.when(c == core)
            def _():
                away = (1 - core) * rows
                part[i, away : away + rows] = made[away : away + rows].astype(BF)
                core_copy(i).start()
                part_f[i % 2] = made[core * rows : (core + 1) * rows]

        if 0 < i < early:
            settle(i - 1)
    settle(count - 1)
    for side in range(2):

        @pl.when(relays(nz - 2, side) & (x == half))
        def _():
            weight_relay(2, nz - 2, 1, side).wait_send()

    send_weights(2, 1, start, kept=True)

    def far_wait(slot, q):
        view = far_in.at[slot, q]
        remote(view, view, own_s.at[0], own_r.at[slot, q], other_c).wait_recv()

    own_slot = y * nx + x
    for q in range(ny):

        @pl.when(c != y)
        def _():
            far_wait(own_slot, q)
            own_sum[q] = far_in[own_slot, q].astype(F32)

    for q in range(ny):
        total = own_sum[q]
        for k in range(1, ny * nx):
            slot = lax.rem(y + k // nx, ny) * nx + lax.rem(x + k % nx, nx)
            far_wait(slot, q)
            total = total + far_in[slot, q].astype(F32)
        into = slice(q * ob, (q + 1) * ob)
        out[:, into] = (mid_own[:, into].astype(F32) + total).astype(BF)

    def done(copy):
        copy.wait_send()

    @pl.when(place < last)
    def _():
        for i in range(3):
            halo_copy(0, i).wait_send()

    @pl.when(place > 0)
    def _():
        for i in range(3):
            halo_copy(1, i).wait_send()

    for matrix in range(3):
        weight_y(matrix).wait_send()
        for passed in range(2):
            send_weights(matrix, passed, done)

        for distance in range(1, nz - 1):
            for passed in range(2):
                for side in range(2):

                    ended = (matrix, distance, passed) == (2, nz - 2, 1)

                    @pl.when(relays(distance, side) & ((x != half) if ended else True))
                    def _():
                        weight_relay(matrix, distance, passed, side).wait_send()

    for g in range(groups):
        for which in range(3):
            tp_copy(g, which).wait_send()
    for k in range(1, nx * nc):
        close_copy(k).wait_send()
    state_y.wait_send()
    total_y.wait_send()
    for d in range(2):

        @pl.when(ranks[d] < nz - 1)
        def _():
            plane_copy(d).wait_send()

    for d in range(2):
        carry_copy(d).wait_send()
    for side, cond in ((0, sends_up), (1, sends_down)):

        @pl.when(cond)
        def _():
            edge_copy(side).wait_send()

    for i in range(count):
        core_copy(i).wait_send()

        @pl.when(jnp.logical_not(stays(i)))
        def _():
            own_to(i).wait_send()


def one_kernel(*args):
    (skip, valve, payload, ingest, observe, pre, rate, extra, tp_taps, ti_taps, to_taps) = args[:11]
    gain, closing, norm_gain, gate_w, value_w, gate_taps, value_taps, down_w = args[11:]
    nz, ny, nx, nc = (lax.axis_size(a) for a in ("z", "y", "x", "core"))
    rows, cols = skip.shape
    width = norm_gain.shape[0]
    groups = ingest.shape[1] // STATE
    gw = payload.shape[1] // groups
    joined = payload.shape[1] + ingest.shape[1] + observe.shape[1]
    hid = gate_w.shape[1] // ny
    ob = down_w.shape[1]
    count = nz * ny
    lanes_used = 2 * pre.shape[2]
    tile = 16
    tall = ny * rows + 2 * tile
    vmem, anywhere = pl.BlockSpec(memory_space=pltpu.VMEM), pl.BlockSpec(memory_space=pl.ANY)
    v = pltpu.VMEM
    sem = pltpu.SemaphoreType.DMA
    scratch = [
        v((2, tile, joined), BF),
        v((rows + 2 * tile, joined), F32),
        v((rows, joined), BF),
        v((rows, 128), F32),
        v((rows, 128), F32),
        v((lanes_used, rows), F32),
        v((lanes_used, rows), F32),
        v((lanes_used, rows), F32),
        v((rows, 128), F32),
        v((rows, 2 * payload.shape[1]), BF),
        v((2, groups, gw, STATE), F32),
        v((2, groups, gw, STATE), BF),
        v((2, groups, gw, STATE), BF),
        v((count, 8, 128), F32),
        v((2, gw, STATE), BF),
        v((2, gw, STATE), BF),
        v((2, gw, STATE), F32),
        v((2, groups, gw, STATE), BF),
        v((2, groups, gw, STATE), BF),
        v((rows, rows), F32),
        v((rows, payload.shape[1]), F32),
        v((rows, width), BF),
        v((rows, cols), BF),
        v((width, cols), BF),
        v((tall, width), BF),
        v((width, hid), BF),
        v((width, hid), BF),
        v((count, hid, ob), BF),
        v((tall, hid), F32),
        v((tall, hid), F32),
        v((ny * rows, hid), BF),
        v((count, ny * rows, ob), BF),
        v((2, rows, ob), F32),
        v((count, rows, ob), BF),
        v((ny, rows, ob), F32),
        v((ny * nx, ny, rows, ob), BF),
        sem((2, 3)),
        sem((2, 3)),
        sem((groups, 3)),
        sem((groups, 3)),
        sem((3, count)),
        sem((3, count)),
        sem((3,)),
        sem((3, 4 * (nz - 2))),
        sem((nx * nc,)),
        sem((nx * nc,)),
        sem(()),
        sem(()),
        sem(()),
        sem(()),
        sem((2,)),
        sem((2,)),
        sem((2,)),
        sem((2,)),
        sem((4,)),
        sem((4,)),
        sem((4,)),
        sem((4,)),
        sem((2,)),
        sem((2,)),
        sem((count,)),
        sem((count,)),
        sem((count,)),
        sem((ny * nx, ny)),
        sem((4,)),
    ]
    operands = [
        *(skip, valve, payload, ingest, observe),
        *(jnp.swapaxes(pre, 1, 2), rate, jnp.swapaxes(extra, 1, 2)),
        *(tp_taps, ti_taps, to_taps, gain.reshape(1, -1), closing, norm_gain.reshape(1, -1)),
        *(gate_w, value_w, gate_taps, value_taps, down_w),
    ]
    staged = [i for i in range(len(operands)) if i not in (12, 14, 15, 18)]
    scratch += [v(operands[i].shape, operands[i].dtype) for i in staged]
    scratch.append(sem((len(staged),)))

    def entry(*refs):
        ins, rest = list(refs[: len(operands)]), refs[len(operands) :]
        held, arrived = rest[-len(staged) - 1 : -1], rest[-1]
        loads = []
        for k, i in enumerate(staged):
            loads.append(pltpu.make_async_copy(ins[i], held[k], arrived.at[k]))
            ins[i] = held[k]
        layer(loads, *ins, *rest[: -len(staged) - 1])

    flops = 2 * rows * width * (width + 3 * hid * ny)
    return pl.pallas_call(
        entry,
        out_shape=jax.ShapeDtypeStruct((rows, cols), BF),
        in_specs=[anywhere] * len(operands),
        out_specs=vmem,
        scratch_shapes=scratch,
        compiler_params=pltpu.CompilerParams(
            collective_id=0, has_side_effects=True, vmem_limit_bytes=67043328
        ),
        cost_estimate=pl.CostEstimate(flops=flops, bytes_accessed=2**24, transcendentals=0),
        name="layer",
    )(*operands)


def body_for(grid):
    sizes = tuple(grid.shape[a] for a in ("z", "y", "x", "core"))
    return one_kernel if sizes == (4, 2, 2, 2) else shards


def solution(mesh):
    sp, tp = mesh.shape["sp"], mesh.shape["tp"]
    ny = 2 ** (int(math.log2(sp)) // 2)
    nc = 2 if tp % 2 == 0 else 1
    grid = Mesh(
        mesh.devices.reshape(sp // ny, ny, tp // nc, nc), ("z", "y", "x", "core")
    )
    return jax.shard_map(
        body_for(grid),
        mesh=grid,
        in_specs=(
            P(SP, TP),
            P(SP, TP),
            P(SP, TP),
            P(SP, TP),
            P(SP, TP),
            P(None, SP, TP),
            P(None, TP),
            P(None, SP, TP),
            P(None, TP),
            P(None, TP),
            P(None, TP),
            P(TP),
            P(TP, None),
            P(),
            P(SP, TP),
            P(SP, TP),
            P(None, TP),
            P(None, TP),
            P(TP, SP),
        ),
        out_specs=P(SP, TP),
        check_vma=False,
    )
```

```python
import functools
import math

import jax
import jax.numpy as jnp
from jax import lax
from jax.experimental import pallas as pl
from jax.experimental.pallas import tpu as pltpu
from jax.sharding import Mesh
from jax.sharding import PartitionSpec as P

HEADS = 32
GROUPS = 8
STATE = 128
EPSILON = 1e-06
SP = ("z", "y")
TP = ("x", "core")


def shifted(block, axis, step):
    count = lax.axis_size(axis)
    return lax.ppermute(block, axis, [(i, (i + step) % count) for i in range(count)])


def moved(block, axis, step):
    count = lax.axis_size(axis)
    pairs = [(i, i + step) for i in range(count) if 0 <= i + step < count]
    return lax.ppermute(block, axis, pairs)


def grid_shifted(block, axes, steps):
    sizes = [lax.axis_size(a) for a in axes]
    pairs = []
    for source in range(sizes[0] * sizes[1]):
        first, second = divmod(source, sizes[1])
        target = ((first + steps[0]) % sizes[0]) * sizes[1] + (second + steps[1]) % sizes[1]
        pairs.append((source, target))
    return lax.ppermute(block, axes, pairs)


def ordered(by_step, index):
    count = len(by_step)
    result = []
    for owner in range(count):
        back = lax.rem(index - owner + count, count)
        block = by_step[0]
        for step in range(1, count):
            block = jnp.where(back == step, by_step[step], block)
        result.append(block)
    return result


def extended(block, axis, width):
    low = moved(block[-width:], axis, 1)
    high = moved(block[:width], axis, -1)
    return jnp.concatenate([low, block, high], axis=0)


def conv_rows(padded, kernel, length):
    summed = padded[0:length] * kernel[0]
    for offset in range(1, kernel.shape[0]):
        summed = summed + padded[offset : offset + length] * kernel[offset]
    return summed


def bdot(pattern, one, two):
    return jnp.einsum(pattern, one, two, preferred_element_type=jnp.float32)


def pack(decay, state):
    heads, width, depth = state.shape
    rows = jnp.broadcast_to(decay[:, None, None], (heads, 16, depth)).astype(jnp.bfloat16)
    return jnp.concatenate([state.astype(jnp.bfloat16), rows], axis=1)


def unpack(packed, width):
    body = packed.astype(jnp.float32)
    return body[:, width, 0], body[:, :width]


def carried_in(decay, state, sign):
    width = state.shape[1]
    count = lax.axis_size(SP)
    own = pack(decay, state)
    index = lax.axis_index(SP)

    def from_back(array, step):
        back, value = unpack(moved(array, SP, sign * step), width)
        source = index - sign * step
        inside = (source >= 0) & (source < count)
        return jnp.where(inside, back, 1.0), value

    near, far = from_back(own, 1), from_back(own, 2)
    total = near[1] + near[0][:, None, None] * far[1]
    product = near[0] * far[0]
    covered = 2
    while covered < count - 1:
        back, value = from_back(pack(product, total), covered)
        total = total + product[:, None, None] * value
        product = product * back
        covered *= 2
    return total


def tied(value, *others):
    marks = [other[(slice(0, 1),) * other.ndim] for other in others]
    return lax.optimization_barrier((value, *marks))[0]


def shared_rows(weight, axis_dim, out_dim, mark):
    count = lax.axis_size("y")
    index = lax.axis_index("y")
    part = weight.shape[axis_dim] // count
    received = []
    for step in range(count):
        at = lax.rem(index + step, count) * part
        block = lax.dynamic_slice_in_dim(weight, at, part, axis_dim)
        received.append(shifted(block, "y", step) if step else block)
    received = [tied(block, mark) for block in received]
    return jnp.concatenate(ordered(received, index), axis=out_dim)


def shards(
    skip_trunk_vector,
    valve_preactivation,
    projected_heads_payload,
    cluster_ingests,
    cluster_observers,
    pre_softplus_increments,
    attenuation_ln_rate,
    additional_attenuation,
    payload_conv_weights,
    ingest_conv_weights,
    observer_conv_weights,
    valved_cluster_factor,
    closing_map_matrix,
    dense_standardize_factor,
    dense_valve_map,
    dense_payload_map,
    valve_series_smoother,
    payload_series_smoother,
    dense_contract_map,
):
    rows = skip_trunk_vector.shape[0]
    own_cols = skip_trunk_vector.shape[1]
    head_count = pre_softplus_increments.shape[2]
    per_group = HEADS // GROUPS
    nx, nc, ny = lax.axis_size("x"), lax.axis_size("core"), lax.axis_size("y")
    ix, ic, iy = lax.axis_index("x"), lax.axis_index("core"), lax.axis_index("y")

    joined = jnp.concatenate([projected_heads_payload, cluster_ingests, cluster_observers], axis=1)
    taps_all = jnp.concatenate(
        [payload_conv_weights, ingest_conv_weights, observer_conv_weights], axis=1
    )
    padded = extended(joined, SP, taps_all.shape[0] // 2)

    convolved = jax.nn.silu(conv_rows(padded.astype(jnp.float32), taps_all, rows)).astype(
        jnp.bfloat16
    )
    gate_w = lax.all_gather(shared_rows(dense_valve_map, 1, 0, convolved), "z", axis=0, tiled=True)
    value_w = lax.all_gather(
        shared_rows(dense_payload_map, 1, 0, convolved), "z", axis=0, tiled=True
    )

    payload_columns = projected_heads_payload.shape[1]
    input_cols = cluster_ingests.shape[1]
    width = payload_columns // head_count
    groups = input_cols // STATE
    values = convolved[:, :payload_columns]
    inputs_g = convolved[:, payload_columns : payload_columns + input_cols].reshape(
        rows, groups, STATE
    )
    readout_g = convolved[:, payload_columns + input_cols :].reshape(rows, groups, STATE)

    steps = jax.nn.softplus(pre_softplus_increments)
    logs = additional_attenuation - steps * jnp.exp(attenuation_ln_rate)[:, None, :]
    running = jnp.cumsum(logs, axis=1)
    run_f = running[0]
    exc_b = running[1] - logs[1]
    total_f, total_b = running[0, -1], running[1, -1]

    end_f = jnp.exp(total_f[None] - run_f) * steps[0]
    end_b = jnp.exp(exc_b) * steps[1]
    ends = jnp.stack([end_f, end_b], axis=1)
    scaled = (
        ends[:, :, :, None] * values.astype(jnp.float32).reshape(rows, 1, head_count, width)
    ).astype(jnp.bfloat16)
    scaled = scaled.reshape(rows, 2, groups, per_group, width)
    summary = bdot("sdgep,sgn->dgepn", scaled, inputs_g).reshape(2, head_count, width, STATE)
    in_f = carried_in(jnp.exp(total_f), summary[0], 1)
    in_b = carried_in(jnp.exp(total_b), summary[1], -1)

    down_part = shared_rows(dense_contract_map, 0, 1, in_f)
    down_w = lax.all_gather(down_part, "z", axis=1, tiled=True)

    places = jnp.arange(rows, dtype=jnp.int32)
    after = places[:, None] > places[None, :]
    same = places[:, None] == places[None, :]
    run_fT, exc_bT = run_f.T, exc_b.T
    step_f, step_b = steps[0].T, steps[1].T
    gaps = jnp.where(
        after[None],
        run_fT[:, :, None] - run_fT[:, None, :],
        exc_bT[:, None, :] - exc_bT[:, :, None],
    )
    factor = jnp.where(
        after[None],
        step_f[:, None, :],
        jnp.where(same[None], (step_f + step_b)[:, None, :], step_b[:, None, :]),
    )
    scores = jnp.repeat(bdot("tgn,sgn->gts", readout_g, inputs_g), per_group, axis=0)
    weights = (scores * jnp.exp(gaps) * factor).astype(jnp.bfloat16)
    within = bdot("hts,shp->thp", weights, values.reshape(rows, head_count, width))

    def outer(state):
        grouped = state.astype(jnp.bfloat16).reshape(groups, per_group, width, STATE)
        return bdot("gepn,tgn->tgep", grouped, readout_g).reshape(rows, head_count, width)

    mixed = within + outer(in_f) * jnp.exp(run_f)[:, :, None]
    mixed = mixed + outer(in_b) * jnp.exp(total_b[None] - exc_b)[:, :, None]
    gated = mixed.reshape(rows, payload_columns) * jax.nn.silu(
        valve_preactivation.astype(jnp.float32)
    )
    grouped = gated.reshape(rows, groups, per_group * width)
    standardized = grouped * lax.rsqrt(jnp.mean(grouped * grouped, axis=2, keepdims=True) + EPSILON)
    blended = (standardized.reshape(rows, payload_columns) * valved_cluster_factor).astype(
        jnp.bfloat16
    )

    def column_block(matrix, dx, dc):
        at = (lax.rem(ix + dx, nx) * nc + lax.rem(ic + dc, nc)) * own_cols
        return lax.dynamic_slice_in_dim(matrix, at, own_cols, 1)

    def over_cores(terms):
        total = terms[0].astype(jnp.bfloat16).astype(jnp.float32)
        for dc in range(1, nc):
            total = total + shifted(terms[dc].astype(jnp.bfloat16), "core", dc).astype(jnp.float32)
        return total

    mapped = None
    for dx in list(range(1, nx)) + [0]:
        terms = [
            jnp.dot(
                blended,
                column_block(closing_map_matrix, dx, dc),
                preferred_element_type=jnp.float32,
            )
            for dc in range(nc)
        ]
        part = over_cores(terms)
        if dx:
            part = shifted(part.astype(jnp.bfloat16), "x", dx).astype(jnp.float32)
        mapped = part if mapped is None else mapped + part
    middle = (skip_trunk_vector.astype(jnp.float32) + mapped).astype(jnp.bfloat16)

    margin = valve_series_smoother.shape[0] // 2
    room = -(-margin // 16) * 16
    low = moved(middle[-margin:], SP, 1)
    high = moved(middle[:margin], SP, -1)
    blank = jnp.zeros((room - margin, own_cols), middle.dtype)
    wide = jnp.concatenate([blank, low, middle, high, blank], axis=0)

    def everywhere(block):
        by_y = []
        for dy in range(ny):
            by_x = []
            for dx in range(nx):
                got = grid_shifted(block, ("y", "x"), (dy, dx)) if dy or dx else block
                by_core = [got] + [shifted(got, "core", dc) for dc in range(1, nc)]
                by_x.append(jnp.concatenate(ordered(by_core, ic), axis=1))
            by_y.append(jnp.concatenate(ordered(by_x, ix), axis=1))
        return jnp.stack(ordered(by_y, iy))

    line = everywhere(wide).reshape(ny * (rows + 2 * room), -1).astype(jnp.float32)
    inverse = lax.rsqrt(jnp.mean(line * line, axis=1, keepdims=True) + EPSILON)
    normed = (line * inverse * dense_standardize_factor).astype(jnp.bfloat16)

    hidden_cols = gate_w.shape[1]
    gate_taps = lax.dynamic_slice_in_dim(valve_series_smoother, iy * hidden_cols, hidden_cols, 1)
    value_taps = lax.dynamic_slice_in_dim(payload_series_smoother, iy * hidden_cols, hidden_cols, 1)

    def spread(weight, taps):
        made = jnp.dot(normed, weight, preferred_element_type=jnp.float32).astype(jnp.bfloat16)
        made = made.reshape(ny, rows + 2 * room, hidden_cols).astype(jnp.float32)
        summed = None
        for offset in range(taps.shape[0]):
            start = room - margin + offset
            term = made[:, start : start + rows] * taps[offset]
            summed = term if summed is None else summed + term
        return summed

    gate_rows = spread(gate_w, gate_taps)
    value_rows = spread(value_w, value_taps)
    hidden = (jax.nn.silu(gate_rows) * value_rows).astype(jnp.bfloat16)

    order = [(dy, dx) for dy in range(ny) for dx in range(nx)]
    down = None
    for dy, dx in order[1:] + order[:1]:
        wanted = lax.dynamic_index_in_dim(hidden, lax.rem(iy + dy, ny), 0, keepdims=False)
        terms = [
            jnp.dot(wanted, column_block(down_w, dx, dc), preferred_element_type=jnp.float32)
            for dc in range(nc)
        ]
        part = over_cores(terms)
        if dy or dx:
            part = grid_shifted(part.astype(jnp.bfloat16), ("y", "x"), (dy, dx)).astype(jnp.float32)
        down = part if down is None else down + part
    return (middle.astype(jnp.float32) + down).astype(jnp.bfloat16)


MESH = pl.DeviceIdType.MESH
BF = jnp.bfloat16
F32 = jnp.float32


def dot(one, two, dims=((1,), (0,)), precision=None):
    return lax.dot_general(
        one, two, (dims, ((), ())), preferred_element_type=F32, precision=precision
    )


def layer(
    loads,
    skip,
    valve,
    payload,
    ingest,
    observe,
    pre,
    rate,
    extra,
    taps_p,
    taps_i,
    taps_o,
    gain,
    closing,
    norm_gain,
    gate_w,
    value_w,
    gate_taps,
    value_taps,
    down_w,
    out,
    halo,
    wide,
    conv,
    run_s,
    exc_s,
    run_t,
    exc_t,
    step_t,
    ends,
    scaled,
    sum_f,
    sum_h,
    sum_y,
    totals,
    plane_out,
    plane_in,
    carry,
    carry_all,
    entering,
    scores,
    mixed,
    blend,
    mid_own,
    close_all,
    rows_n,
    wg,
    wv,
    wd,
    made_g,
    made_v,
    hidden,
    part,
    part_f,
    part_in,
    own_sum,
    far_in,
    halo_s,
    halo_r,
    tp_s,
    tp_r,
    w_s,
    w_r,
    w_y,
    w_fwd,
    cl_s,
    cl_r,
    tot_s,
    tot_r,
    sy_s,
    sy_r,
    pl_s,
    pl_r,
    ca_s,
    ca_r,
    nb_s,
    nb_r,
    nf_s,
    nf_r,
    edge_s,
    edge_r,
    core_s,
    core_r,
    own_s,
    own_r,
    local,
):
    nz, ny, nx, nc = (lax.axis_size(a) for a in ("z", "y", "x", "core"))
    z, y, x, c = (lax.axis_index(a) for a in ("z", "y", "x", "core"))
    place, lane_at = z * ny + y, x * nc + c
    rows, cols = skip.shape
    width_all = blend.shape[1]
    heads = pre.shape[1]
    groups = ingest.shape[1] // STATE
    per = heads // groups
    head_w = payload.shape[1] // heads
    gw = per * head_w
    hid = wg.shape[1]
    kb = gate_w.shape[0]
    ob = down_w.shape[1]
    tile = 16
    other_y, other_x, other_c = (z, 1 - y, x, c), (z, y, 1 - x, c), (z, y, x, 1 - c)
    half = z // 2
    near = z * (1 - 2 * half) + (nz - 1) * half
    middle = (z > 0) & (z < nz - 1)

    def remote(src, dst, send, recv, to):
        return pltpu.make_async_remote_copy(
            src_ref=src,
            dst_ref=dst,
            send_sem=send,
            recv_sem=recv,
            device_id=to,
            device_id_type=MESH,
        )

    for load in loads:
        load.start()
    barrier = pltpu.get_barrier_semaphore()
    greeted = 0
    for k in range(1, nz * ny):
        to = (lax.rem(z + k // ny, nz), lax.rem(y + k % ny, ny), x, c)
        pl.semaphore_signal(barrier, inc=1, device_id=to, device_id_type=MESH)
        greeted += 1
    for k in range(1, nx * nc):
        for dy in range(ny):
            to = (z, lax.rem(y + dy, ny), lax.rem(x + k // nc, nx), lax.rem(c + k % nc, nc))
            pl.semaphore_signal(barrier, inc=1, device_id=to, device_id_type=MESH)
            greeted += 1
    pl.semaphore_wait(barrier, greeted)
    for load in loads:
        load.wait()

    pieces = []
    at = 0
    for source in (payload, ingest, observe):
        pieces.append((source, at, source.shape[1]))
        at += source.shape[1]

    def halo_copy(side, i):
        source, start, size = pieces[i]
        other = place + 1 if side == 0 else place - 1
        to = (other // ny, lax.rem(other + ny, ny), x, c)
        src = source.at[pl.ds(rows - tile, tile)] if side == 0 else source.at[pl.ds(0, tile)]
        return remote(
            src,
            halo.at[side, :, pl.ds(start, size)],
            halo_s.at[side, i],
            halo_r.at[side, i],
            to,
        )

    last = nz * ny - 1

    @pl.when(place < last)
    def _():
        for i in range(3):
            halo_copy(0, i).start()

    @pl.when(place > 0)
    def _():
        for i in range(3):
            halo_copy(1, i).start()

    def column(ref, to_y, matrix):
        at = pl.multiple_of(to_y * hid, 128)
        if matrix == 2:
            return ref.at[pl.ds(at, hid), :]
        return ref.at[:, pl.ds(at, hid)]

    given = (gate_w, value_w, down_w)

    def landing(matrix, index):
        if matrix == 2:
            return wd.at[index]
        return (wg, wv)[matrix].at[pl.ds(pl.multiple_of(index * kb, kb), kb), :]

    beside = z * ny + 1 - y

    def weight_y(matrix):
        return remote(
            column(given[matrix], 1 - y, matrix),
            landing(matrix, place),
            w_y.at[matrix],
            w_r.at[matrix, place],
            other_y,
        )

    def weight_arrival(matrix, index):
        return remote(
            landing(matrix, index),
            landing(matrix, index),
            w_y.at[matrix],
            w_r.at[matrix, index],
            other_y,
        )

    def weight_copy(matrix, to_z, passed):
        index = beside if passed else place
        source = landing(matrix, index) if passed else column(given[matrix], y, matrix)
        return remote(
            source,
            landing(matrix, index),
            w_s.at[matrix, to_z * ny + passed],
            w_r.at[matrix, index],
            (to_z, y, x, c),
        )

    def weight_relay(matrix, distance, passed, side):
        sign = 1 - 2 * side
        index = (z - sign * distance) * ny + (1 - y if passed else y)
        return remote(
            landing(matrix, index),
            landing(matrix, index),
            w_fwd.at[matrix, (distance - 1) * 4 + passed * 2 + side],
            w_r.at[matrix, index],
            (z + sign, y, x, c),
        )

    def relays(distance, side):
        sign = 1 - 2 * side
        source, to = z - sign * distance, z + sign
        return (source >= 0) & (source < nz) & (to >= 0) & (to < nz)

    def waits(to):
        return middle & (x == half) & ((to == 0) | (to == nz - 1))

    def send_weights(matrix, passed, do, kept=None):
        for sign in (1, -1):
            to = z + sign
            goes = (to >= 0) & (to < nz)
            if kept is not None:
                goes = goes & (waits(to) if kept else jnp.logical_not(waits(to)))

            @pl.when(goes)
            def _():
                do(weight_copy(matrix, to, passed))

    def start(copy):
        copy.start()

    def pass_weights(matrix):
        weight_arrival(matrix, beside).wait_recv()
        send_weights(matrix, 1, start)

    def relay_weights(matrix, distance, passed):
        for side in range(2):

            @pl.when(relays(distance, side))
            def _():
                source = z - distance if side == 0 else z + distance
                weight_arrival(matrix, source * ny + (1 - y if passed else y)).wait_recv()
                weight_relay(matrix, distance, passed, side).start()

    def own_copy(matrix):
        return pltpu.make_async_copy(
            column(given[matrix], y, matrix), landing(matrix, place), local.at[matrix]
        )

    def await_weights(matrix, to_z):
        for to_y in range(ny):

            @pl.when((to_z != z) & jnp.logical_not(middle))
            def _():
                weight_arrival(matrix, to_z * ny + to_y).wait_recv()

    def tp_index(k):
        return lax.rem(x + k // nc, nx), lax.rem(c + k % nc, nc)

    def close_copy(k):
        to_x, to_c = tp_index(k)
        at = pl.ds(pl.multiple_of((to_x * nc + to_c) * cols, 128), cols)
        return remote(
            closing.at[:, at], close_rows(lane_at), cl_s.at[k], cl_r.at[k], (z, y, to_x, to_c)
        )

    def close_rows(index):
        return close_all.at[pl.ds(pl.multiple_of(index * cols, cols), cols), :]

    def close_arrival(k):
        at_x, at_c = tp_index(k)
        view = close_rows(at_x * nc + at_c)
        return remote(view, view, cl_s.at[k], cl_r.at[k], other_c)

    side_x = (1 - x) * nc + c

    def blend_view(g, index):
        return blend.at[:, pl.ds(pl.multiple_of(index * cols + g * gw, 128), gw)]

    def tp_copy(g, which):
        view = blend_view(g, (lane_at, lane_at, side_x)[which])
        to = (other_x, other_c, other_c)[which]
        return remote(view, view, tp_s.at[g, which], tp_r.at[g, which], to)

    def tp_arrival(g, which):
        view = blend_view(g, (side_x, x * nc + 1 - c, (1 - x) * nc + 1 - c)[which])
        return remote(view, view, tp_s.at[g, which], tp_r.at[g, which], other_c)

    weight_y(0).start()
    for matrix in range(2):
        send_weights(matrix, 0, start)
    for k in (2, 3, 1):
        close_copy(k).start()
    for matrix in range(3):
        own_copy(matrix).start()
    close_own = pltpu.make_async_copy(
        closing.at[:, pl.ds(pl.multiple_of(lane_at * cols, 128), cols)],
        close_rows(lane_at),
        local.at[3],
    )
    close_own.start()

    edge = wide.shape[0] - tile
    for source, start_at, size in pieces:
        wide[tile : tile + rows, start_at : start_at + size] = source[...].astype(F32)

    @pl.when(place > 0)
    def _():
        for i in range(3):
            halo_copy(0, i).wait_recv()
        wide[0:tile, :] = halo[0].astype(F32)

    @pl.when(place == 0)
    def _():
        wide[0:tile, :] = jnp.zeros((tile, wide.shape[1]), F32)

    @pl.when(place < last)
    def _():
        for i in range(3):
            halo_copy(1, i).wait_recv()
        wide[edge:, :] = halo[1].astype(F32)

    @pl.when(place == last)
    def _():
        wide[edge:, :] = jnp.zeros((tile, wide.shape[1]), F32)

    margin = taps_p.shape[0] // 2
    for (source, start_at, size), taps in zip(pieces, (taps_p, taps_i, taps_o)):

        def conv_columns(i, carried, start_at=start_at, taps=taps):
            into = pl.ds(pl.multiple_of(start_at + i * 128, 128), 128)
            tap = taps[:, pl.ds(pl.multiple_of(i * 128, 128), 128)]
            for r in range(0, rows, 128):
                summed = None
                for k in range(tap.shape[0]):
                    first = tile - margin + k + r
                    term = wide[first : first + 128, into] * tap[k : k + 1]
                    summed = term if summed is None else summed + term
                conv[r : r + 128, into] = jax.nn.silu(summed).astype(BF)
            return carried

        lax.fori_loop(0, size // 128, conv_columns, 0)

    def upright(row):
        shape = (heads, heads)
        same = lax.broadcasted_iota(jnp.int32, shape, 0) == lax.broadcasted_iota(
            jnp.int32, shape, 1
        )
        return jnp.sum(
            jnp.where(same, jnp.broadcast_to(row, shape), 0.0), axis=1, keepdims=True
        )

    def turned(array):
        blank = jnp.zeros((128 - 2 * heads, rows), F32)
        return jnp.concatenate([array, blank], axis=0).T

    raw = jnp.concatenate([pre[0], pre[1]], axis=0)
    steps_t = jnp.maximum(raw, 0.0) + jnp.log1p(jnp.exp(-jnp.abs(raw)))
    rates = jnp.exp(jnp.concatenate([upright(rate[0:1]), upright(rate[1:2])], axis=0))
    logs_t = jnp.concatenate([extra[0], extra[1]], axis=0) - steps_t * rates
    earlier = lax.broadcasted_iota(jnp.int32, (rows, rows), 0) <= lax.broadcasted_iota(
        jnp.int32, (rows, rows), 1
    )
    running_t = dot(logs_t, earlier.astype(F32), precision=lax.Precision.HIGHEST)
    before_t = running_t - logs_t
    run_t[...] = running_t
    exc_t[...] = before_t
    step_t[...] = steps_t
    running, before, steps = turned(running_t), turned(before_t), turned(steps_t)
    run_s[...] = running
    exc_s[...] = before
    whole = running[rows - 1 : rows]
    lane = lax.broadcasted_iota(jnp.int32, (rows, 128), 1)
    ends[...] = jnp.exp(jnp.where(lane < heads, whole - running, before)) * steps
    totals[place] = jnp.broadcast_to(whole, (8, 128))

    def spread(columns, first):
        low = lax.broadcasted_iota(jnp.int32, (columns.shape[0], 2 * head_w), 1) < head_w
        shape = (columns.shape[0], 2 * head_w)
        return jnp.where(
            low,
            jnp.broadcast_to(columns[:, first : first + 1], shape),
            jnp.broadcast_to(columns[:, first + 1 : first + 2], shape),
        )

    def scale_rows(i, carried):
        at = pl.ds(pl.multiple_of(i * 128, 128), 128)
        factors = ends[at, :]
        for d in range(2):
            for p in range(heads // 2):
                into = slice(p * 2 * head_w, (p + 1) * 2 * head_w)
                made = conv[at, into].astype(F32) * spread(factors, d * heads + 2 * p)
                start_at = d * heads * head_w + p * 2 * head_w
                scaled[at, start_at : start_at + 2 * head_w] = made.astype(BF)
        return carried

    lax.fori_loop(0, rows // 128, scale_rows, 0)
    in_at = payload.shape[1]
    out_at = in_at + ingest.shape[1]
    for d in range(2):
        for g in range(groups):
            first = d * heads * head_w + g * gw
            state = dot(
                scaled[:, first : first + gw],
                conv[:, in_at + g * STATE : in_at + (g + 1) * STATE],
                ((0,), (0,)),
            )
            sum_f[d, g] = state
            sum_h[d, g] = state.astype(BF)

    state_y = remote(sum_h, sum_y, sy_s, sy_r, other_y)
    state_y.start()

    total_y = remote(totals.at[place], totals.at[place], tot_s, tot_r, other_y)
    total_y.start()
    pass_weights(0)
    weight_y(1).start()

    state_y.wait_recv()
    remote(totals.at[beside], totals.at[beside], tot_s, tot_r, other_y).wait_recv()

    def head_rows(ref_value, factors):
        return jnp.concatenate(
            [ref_value[e * head_w : (e + 1) * head_w] * factors[e] for e in range(per)], axis=0
        )

    def of_heads(row, d, g=None):
        result = []
        for e in range(per):
            picks = [
                row[:, d * heads + k * per + e : d * heads + k * per + e + 1] for k in range(groups)
            ]
            if g is None:
                result.append(jnp.where(y == 0, picks[0], picks[1]))
            else:
                result.append(picks[g])
        return result

    one_row = jnp.ones((1, 128), F32)
    plane_low = jnp.exp(totals[z * ny, 0:1])
    plane_high = jnp.exp(totals[z * ny + 1, 0:1])
    forward_own = of_heads(jnp.where(y == 0, plane_high, one_row), 0)
    forward_far = of_heads(jnp.where(y == 0, one_row, plane_high), 0)
    back_own = of_heads(jnp.where(y == 0, one_row, plane_low), 1)
    back_far = of_heads(jnp.where(y == 0, plane_low, one_row), 1)
    plane_out[0] = (
        head_rows(sum_f[0, y], forward_own) + head_rows(sum_y[0, y].astype(F32), forward_far)
    ).astype(BF)
    plane_out[1] = (
        head_rows(sum_f[1, y], back_own) + head_rows(sum_y[1, y].astype(F32), back_far)
    ).astype(BF)

    def plane_copy(d):
        to = z + 1 if d == 0 else z - 1
        return remote(
            plane_out.at[d], plane_in.at[d], pl_s.at[d], pl_r.at[d], (to, y, x, c)
        )

    plane_gone = plane_low * plane_high
    ranks = (z, nz - 1 - z)

    def take(d):
        plane_copy(d).wait_recv()
        carry[d] = plane_in[d].astype(F32)

    def hop(step):
        for d in range(2):

            @pl.when(ranks[d] == step)
            def _():
                if step:
                    take(d)
                    grown = head_rows(carry[d], of_heads(plane_gone, d))
                    plane_out[d] = (grown + plane_out[d].astype(F32)).astype(BF)
                plane_copy(d).start()

    carry[...] = jnp.zeros_like(carry)
    hop(0)

    weight_y(2).start()
    relay_weights(0, 1, 0)
    relay_weights(1, 1, 0)

    def within(g):
        read = conv[:, out_at + g * STATE : out_at + (g + 1) * STATE]
        write = conv[:, in_at + g * STATE : in_at + (g + 1) * STATE]
        scores[...] = dot(read, write, ((1,), (1,)))
        for p in range(per // 2):
            pair = g * per + 2 * p
            into = slice(pair * head_w, (pair + 2) * head_w)

            def chunk(i, carried):
                at = pl.ds(pl.multiple_of(i * 128, 128), 128)
                t = lax.broadcasted_iota(jnp.int32, (128, rows), 0) + i * 128
                s = lax.broadcasted_iota(jnp.int32, (128, rows), 1)
                after, same = t > s, t == s
                values = conv[:, into]
                low = lax.broadcasted_iota(jnp.int32, values.shape, 1) < head_w
                summed = None
                for e in range(2):
                    f, b = pair + e, heads + pair + e
                    gap = jnp.where(
                        after,
                        run_s[at, f : f + 1] - run_t[f : f + 1, :],
                        exc_t[b : b + 1, :] - exc_s[at, b : b + 1],
                    )
                    step_f, step_b = step_t[f : f + 1, :], step_t[b : b + 1, :]
                    factor = jnp.where(after, step_f, jnp.where(same, step_f + step_b, step_b))
                    made = (scores[at, :] * jnp.exp(gap) * factor).astype(BF)
                    kept = jnp.where(low if e == 0 else jnp.logical_not(low), values, 0)
                    term = dot(made, kept.astype(BF))
                    summed = term if summed is None else summed + term
                mixed[at, into] = summed
                return carried

            lax.fori_loop(0, rows // 128, chunk, 0)

    within(0)
    hop(1)
    pass_weights(1)
    within(1)
    for step in range(2, nz - 1):
        hop(step)
    for matrix in range(2):
        relay_weights(matrix, 2, 0)
    relay_weights(0, 1, 1)
    for d in range(2):

        @pl.when(ranks[d] == nz - 1)
        def _():
            take(d)

    for d in range(2):
        carry_all[d, y] = carry[d].astype(BF)

    def carry_copy(d):
        return remote(carry_all.at[d, y], carry_all.at[d, y], ca_s.at[d], ca_r.at[d], other_y)

    for d in range(2):
        carry_copy(d).start()


    for d in range(2):
        remote(
            carry_all.at[d, 1 - y], carry_all.at[d, 1 - y], ca_s.at[d], ca_r.at[d], other_y
        ).wait_recv()
    for g in range(groups):
        for d in range(2):
            through = plane_low if d == 0 else plane_high
            adds = y == 1 if d == 0 else y == 0
            weights = of_heads(jnp.where(adds, through, one_row), d, g)
            body = head_rows(carry_all[d, g].astype(F32), weights)
            entering[d, g] = (body + jnp.where(adds, sum_y[d, g].astype(F32), 0.0)).astype(BF)

    for g in range(groups):

        def finish(i, carried):
            at = pl.ds(pl.multiple_of(i * 128, 128), 128)
            read = conv[at, out_at + g * STATE : out_at + (g + 1) * STATE]
            fore = dot(read, entering[0, g], ((1,), (1,)))
            back = dot(read, entering[1, g], ((1,), (1,)))
            grown = jnp.exp(run_s[at, :])
            shrunk = jnp.exp(run_s[rows - 1 : rows, :] - exc_s[at, :])
            parts = []
            for p in range(per // 2):
                pair = g * per + 2 * p
                into = slice(pair * head_w, (pair + 2) * head_w)
                inner = slice(2 * p * head_w, 2 * (p + 1) * head_w)
                total = mixed[at, into] + fore[:, inner] * spread(grown, pair)
                total = total + back[:, inner] * spread(shrunk, heads + pair)
                parts.append(total * jax.nn.silu(valve[at, into].astype(F32)))
            gated = jnp.concatenate(parts, axis=1)
            mean = jnp.mean(gated * gated, axis=1, keepdims=True)
            made = gated * lax.rsqrt(mean + EPSILON) * gain[:, g * gw : (g + 1) * gw]
            blend[at, pl.ds(pl.multiple_of(lane_at * cols + g * gw, 128), gw)] = made.astype(BF)
            return carried

        lax.fori_loop(0, rows // 128, finish, 0)
        tp_copy(g, 0).start()
        tp_copy(g, 1).start()

    close_own.wait()
    for k in range(1, nx * nc):
        close_arrival(k).wait_recv()
    for g in range(groups):
        tp_arrival(g, 0).wait_recv()
        tp_copy(g, 2).start()
    for g in range(groups):
        tp_arrival(g, 1).wait_recv()
        tp_arrival(g, 2).wait_recv()

    def row_view(which_y, index):
        return rows_n.at[
            pl.ds(pl.multiple_of(tile + which_y * rows, tile), rows),
            pl.ds(pl.multiple_of(index * cols, 128), cols),
        ]

    relay_weights(1, 1, 1)
    made = dot(blend[...], close_all[...]) + skip[...].astype(F32)
    mid_own[...] = made.astype(BF)
    rows_n[
        pl.ds(pl.multiple_of(tile + y * rows, tile), rows),
        pl.ds(pl.multiple_of(lane_at * cols, 128), cols),
    ] = mid_own[...]

    other_xy = (z, 1 - y, 1 - x, c)
    froms = ((y, x), (y, 1 - x), (1 - y, x), (1 - y, 1 - x))

    def row_copy(k):
        view = row_view(y, lane_at)
        to = (other_c, other_x, other_y, other_xy)[k]
        return remote(view, view, nb_s.at[k], nb_r.at[k], to)

    def row_pass(k, core, arriving=False):
        view = row_view(froms[k][0], froms[k][1] * nc + core)
        sem = (nb_r if arriving else nf_r).at[k]
        return remote(view, view, nf_s.at[k], sem, other_c)

    for k in (1, 2, 3, 0):
        row_copy(k).start()
    for k in (1, 2, 3):
        row_pass(k, c, arriving=True).wait_recv()
        row_pass(k, c).start()
        if k == 1:
            relay_weights(0, 2, 1)
            relay_weights(1, 2, 1)
            send_weights(2, 0, start)
    row_pass(0, 1 - c, arriving=True).wait_recv()
    for k in (1, 2, 3):
        row_pass(k, 1 - c).wait_recv()
    for k in range(4):
        row_copy(k).wait_send()
        if k:
            row_pass(k, c).wait_send()

    def normalize(i, carried):
        at = pl.ds(pl.multiple_of(tile + i * 128, tile), 128)
        squares = jnp.zeros((128, 1), F32)
        for first in range(0, width_all, 256):
            piece = rows_n[at, first : first + 256].astype(F32)
            squares = squares + jnp.sum(piece * piece, axis=1, keepdims=True)
        inverse = lax.rsqrt(squares / width_all + EPSILON)
        for first in range(0, width_all, 256):
            piece = rows_n[at, first : first + 256].astype(F32)
            piece = piece * inverse * norm_gain[:, first : first + 256]
            rows_n[at, first : first + 256] = piece.astype(BF)
        return carried

    lax.fori_loop(0, ny * rows // 128, normalize, 0)

    bottom = tile + ny * rows

    def edge_copy(side):
        if side == 0:
            src, dst = rows_n.at[pl.ds(bottom - tile, tile)], rows_n.at[pl.ds(0, tile)]
        else:
            src, dst = rows_n.at[pl.ds(tile, tile)], rows_n.at[pl.ds(bottom, tile)]
        to = (z + 1 if side == 0 else z - 1, y, x, c)
        return remote(src, dst, edge_s.at[side], edge_r.at[side], to)

    sends_up, sends_down = z < nz - 1, z > 0
    for side, cond in ((0, sends_up), (1, sends_down)):

        @pl.when(cond)
        def _():
            edge_copy(side).start()

    weight_arrival(2, beside).wait_recv()
    send_weights(2, 1, start, kept=False)
    relay_weights(2, 1, 0)

    for matrix, (weight, made) in enumerate(((wg, made_g), (wv, made_v))):
        own_copy(matrix).wait()
        for k in range(nz):
            await_weights(matrix, k)

        def units(i, carried):
            at = pl.ds(pl.multiple_of(tile + i * rows, tile), rows)
            made[at, :] = dot(rows_n[at, :], weight[...]).astype(BF).astype(F32)
            return carried

        lax.fori_loop(0, ny, units, 0)

    relay_weights(2, 2, 0)
    relay_weights(2, 1, 1)

    @pl.when(z > 0)
    def _():
        edge_copy(0).wait_recv()

    @pl.when(z == 0)
    def _():
        rows_n[0:tile, :] = jnp.zeros((tile, width_all), BF)

    @pl.when(z < nz - 1)
    def _():
        edge_copy(1).wait_recv()

    @pl.when(z == nz - 1)
    def _():
        rows_n[bottom:, :] = jnp.zeros((tile, width_all), BF)

    both = jnp.concatenate([rows_n[0:tile, :], rows_n[bottom:, :]], axis=0)
    for weight, made in ((wg, made_g), (wv, made_v)):
        edges = dot(both, weight[...]).astype(BF).astype(F32)
        made[0:tile, :] = edges[0:tile]
        made[bottom:, :] = edges[tile:]

    ff_margin = gate_taps.shape[0] // 2

    def activate(i, carried):
        into = pl.ds(pl.multiple_of(i * 128, 128), 128)
        tap_at = pl.ds(pl.multiple_of(y * hid + i * 128, 128), 128)
        tap_g, tap_v = gate_taps[:, tap_at], value_taps[:, tap_at]
        for r in range(0, ny * rows, 128):
            pair = []
            for made, tap in ((made_g, tap_g), (made_v, tap_v)):
                summed = None
                for k in range(tap.shape[0]):
                    first = tile - ff_margin + k + r
                    term = made[first : first + 128, into] * tap[k : k + 1]
                    summed = term if summed is None else summed + term
                pair.append(summed)
            hidden[r : r + 128, into] = (jax.nn.silu(pair[0]) * pair[1]).astype(BF)
        return carried

    lax.fori_loop(0, hid // 128, activate, 0)

    own_copy(2).wait()

    def order(i):
        k = i % nz
        kept = near * (1 - 2 * k) + k if k < 2 else k
        if i >= nz and k:
            turn = (1 - near) * (1 - jnp.abs(x - half))
            kept = kept + turn * (k % (nz - 1) + 1 - k)
        return kept * (1 - 2 * half) + (nz - 1) * half

    def half_at(core):
        return pl.ds(pl.multiple_of(core * rows, tile), rows)

    def core_copy(i):
        return remote(
            part.at[i, half_at(1 - c)], part_in.at[i], core_s.at[i], core_r.at[i], other_c
        )

    def block_y(i):
        return y if i < nz else 1 - y

    def own_to(i):
        to_z = order(i)
        slot, q = y * nx + x, block_y(i)
        return remote(
            part.at[i, half_at(c)],
            far_in.at[slot, q],
            own_s.at[i],
            own_r.at[slot, q],
            (z, c, to_z // nc, lax.rem(to_z, nc)),
        )

    def stays(i):
        to_z = order(i)
        return (y == c) & (to_z // nc == x) & (lax.rem(to_z, nc) == c)

    count = nz * ny
    early = count // 2

    def settle(i):
        core_copy(i).wait_recv()

        @pl.when(stays(i))
        def _():
            own_sum[block_y(i)] = part_f[i % 2] + part_in[i].astype(F32)

        @pl.when(jnp.logical_not(stays(i)))
        def _():
            part[i, half_at(c)] = (part_f[i % 2] + part_in[i].astype(F32)).astype(BF)
            own_to(i).start()

    for i in range(count):
        to_z, to_y = order(i), block_y(i)
        index = to_z * ny + to_y
        if i >= early:
            settle(i - 1)
        if i == early:
            relay_weights(2, 2, 1)

        @pl.when((to_z != z) & jnp.logical_not(middle))
        def _():
            weight_arrival(2, index).wait_recv()

        made = dot(hidden[...], wd[index])

        for core in range(nc):

            @pl.when(c == core)
            def _():
                away = (1 - core) * rows
                part[i, away : away + rows] = made[away : away + rows].astype(BF)
                core_copy(i).start()
                part_f[i % 2] = made[core * rows : (core + 1) * rows]

        if 0 < i < early:
            settle(i - 1)
    settle(count - 1)
    for side in range(2):

        @pl.when(relays(nz - 2, side) & (x == half))
        def _():
            weight_relay(2, nz - 2, 1, side).wait_send()

    send_weights(2, 1, start, kept=True)

    def far_wait(slot, q):
        view = far_in.at[slot, q]
        remote(view, view, own_s.at[0], own_r.at[slot, q], other_c).wait_recv()

    own_slot = y * nx + x
    for q in range(ny):

        @pl.when(c != y)
        def _():
            far_wait(own_slot, q)
            own_sum[q] = far_in[own_slot, q].astype(F32)

    for q in range(ny):
        total = own_sum[q]
        for k in range(1, ny * nx):
            slot = lax.rem(y + k // nx, ny) * nx + lax.rem(x + k % nx, nx)
            far_wait(slot, q)
            total = total + far_in[slot, q].astype(F32)
        into = slice(q * ob, (q + 1) * ob)
        out[:, into] = (mid_own[:, into].astype(F32) + total).astype(BF)

    def done(copy):
        copy.wait_send()

    @pl.when(place < last)
    def _():
        for i in range(3):
            halo_copy(0, i).wait_send()

    @pl.when(place > 0)
    def _():
        for i in range(3):
            halo_copy(1, i).wait_send()

    for matrix in range(3):
        weight_y(matrix).wait_send()
        for passed in range(2):
            send_weights(matrix, passed, done)

        for distance in range(1, nz - 1):
            for passed in range(2):
                for side in range(2):

                    ended = (matrix, distance, passed) == (2, nz - 2, 1)

                    @pl.when(relays(distance, side) & ((x != half) if ended else True))
                    def _():
                        weight_relay(matrix, distance, passed, side).wait_send()

    for g in range(groups):
        for which in range(3):
            tp_copy(g, which).wait_send()
    for k in range(1, nx * nc):
        close_copy(k).wait_send()
    state_y.wait_send()
    total_y.wait_send()
    for d in range(2):

        @pl.when(ranks[d] < nz - 1)
        def _():
            plane_copy(d).wait_send()

    for d in range(2):
        carry_copy(d).wait_send()
    for side, cond in ((0, sends_up), (1, sends_down)):

        @pl.when(cond)
        def _():
            edge_copy(side).wait_send()

    for i in range(count):
        core_copy(i).wait_send()

        @pl.when(jnp.logical_not(stays(i)))
        def _():
            own_to(i).wait_send()


def one_kernel(*args):
    (skip, valve, payload, ingest, observe, pre, rate, extra, tp_taps, ti_taps, to_taps) = args[:11]
    gain, closing, norm_gain, gate_w, value_w, gate_taps, value_taps, down_w = args[11:]
    nz, ny, nx, nc = (lax.axis_size(a) for a in ("z", "y", "x", "core"))
    rows, cols = skip.shape
    width = norm_gain.shape[0]
    groups = ingest.shape[1] // STATE
    gw = payload.shape[1] // groups
    joined = payload.shape[1] + ingest.shape[1] + observe.shape[1]
    hid = gate_w.shape[1] // ny
    ob = down_w.shape[1]
    count = nz * ny
    lanes_used = 2 * pre.shape[2]
    tile = 16
    tall = ny * rows + 2 * tile
    vmem, anywhere = pl.BlockSpec(memory_space=pltpu.VMEM), pl.BlockSpec(memory_space=pl.ANY)
    v = pltpu.VMEM
    sem = pltpu.SemaphoreType.DMA
    scratch = [
        v((2, tile, joined), BF),
        v((rows + 2 * tile, joined), F32),
        v((rows, joined), BF),
        v((rows, 128), F32),
        v((rows, 128), F32),
        v((lanes_used, rows), F32),
        v((lanes_used, rows), F32),
        v((lanes_used, rows), F32),
        v((rows, 128), F32),
        v((rows, 2 * payload.shape[1]), BF),
        v((2, groups, gw, STATE), F32),
        v((2, groups, gw, STATE), BF),
        v((2, groups, gw, STATE), BF),
        v((count, 8, 128), F32),
        v((2, gw, STATE), BF),
        v((2, gw, STATE), BF),
        v((2, gw, STATE), F32),
        v((2, groups, gw, STATE), BF),
        v((2, groups, gw, STATE), BF),
        v((rows, rows), F32),
        v((rows, payload.shape[1]), F32),
        v((rows, width), BF),
        v((rows, cols), BF),
        v((width, cols), BF),
        v((tall, width), BF),
        v((width, hid), BF),
        v((width, hid), BF),
        v((count, hid, ob), BF),
        v((tall, hid), F32),
        v((tall, hid), F32),
        v((ny * rows, hid), BF),
        v((count, ny * rows, ob), BF),
        v((2, rows, ob), F32),
        v((count, rows, ob), BF),
        v((ny, rows, ob), F32),
        v((ny * nx, ny, rows, ob), BF),
        sem((2, 3)),
        sem((2, 3)),
        sem((groups, 3)),
        sem((groups, 3)),
        sem((3, count)),
        sem((3, count)),
        sem((3,)),
        sem((3, 4 * (nz - 2))),
        sem((nx * nc,)),
        sem((nx * nc,)),
        sem(()),
        sem(()),
        sem(()),
        sem(()),
        sem((2,)),
        sem((2,)),
        sem((2,)),
        sem((2,)),
        sem((4,)),
        sem((4,)),
        sem((4,)),
        sem((4,)),
        sem((2,)),
        sem((2,)),
        sem((count,)),
        sem((count,)),
        sem((count,)),
        sem((ny * nx, ny)),
        sem((4,)),
    ]
    operands = [
        *(skip, valve, payload, ingest, observe),
        *(jnp.swapaxes(pre, 1, 2), rate, jnp.swapaxes(extra, 1, 2)),
        *(tp_taps, ti_taps, to_taps, gain.reshape(1, -1), closing, norm_gain.reshape(1, -1)),
        *(gate_w, value_w, gate_taps, value_taps, down_w),
    ]
    staged = [i for i in range(len(operands)) if i not in (12, 14, 15, 18)]
    scratch += [v(operands[i].shape, operands[i].dtype) for i in staged]
    scratch.append(sem((len(staged),)))

    def entry(*refs):
        ins, rest = list(refs[: len(operands)]), refs[len(operands) :]
        held, arrived = rest[-len(staged) - 1 : -1], rest[-1]
        loads = []
        for k, i in enumerate(staged):
            loads.append(pltpu.make_async_copy(ins[i], held[k], arrived.at[k]))
            ins[i] = held[k]
        layer(loads, *ins, *rest[: -len(staged) - 1])

    flops = 2 * rows * width * (width + 3 * hid * ny)
    return pl.pallas_call(
        entry,
        out_shape=jax.ShapeDtypeStruct((rows, cols), BF),
        in_specs=[anywhere] * len(operands),
        out_specs=vmem,
        scratch_shapes=scratch,
        compiler_params=pltpu.CompilerParams(
            collective_id=0, has_side_effects=True, vmem_limit_bytes=67043328
        ),
        cost_estimate=pl.CostEstimate(flops=flops, bytes_accessed=2**24, transcendentals=0),
        name="layer",
    )(*operands)


def body_for(grid):
    sizes = tuple(grid.shape[a] for a in ("z", "y", "x", "core"))
    return one_kernel if sizes == (4, 2, 2, 2) else shards


def solution(mesh):
    sp, tp = mesh.shape["sp"], mesh.shape["tp"]
    ny = 2 ** (int(math.log2(sp)) // 2)
    nc = 2 if tp % 2 == 0 else 1
    grid = Mesh(
        mesh.devices.reshape(sp // ny, ny, tp // nc, nc), ("z", "y", "x", "core")
    )
    return jax.shard_map(
        body_for(grid),
        mesh=grid,
        in_specs=(
            P(SP, TP),
            P(SP, TP),
            P(SP, TP),
            P(SP, TP),
            P(SP, TP),
            P(None, SP, TP),
            P(None, TP),
            P(None, SP, TP),
            P(None, TP),
            P(None, TP),
            P(None, TP),
            P(TP),
            P(TP, None),
            P(),
            P(SP, TP),
            P(SP, TP),
            P(None, TP),
            P(None, TP),
            P(TP, SP),
        ),
        out_specs=P(SP, TP),
        check_vma=False,
    )
```

```python
import functools
import math

import jax
import jax.numpy as jnp
from jax import lax
from jax.experimental import pallas as pl
from jax.experimental.pallas import tpu as pltpu
from jax.sharding import Mesh
from jax.sharding import PartitionSpec as P

HEADS = 32
GROUPS = 8
STATE = 128
EPSILON = 1e-06
SP = ("z", "y")
TP = ("x", "core")


def shifted(block, axis, step):
    count = lax.axis_size(axis)
    return lax.ppermute(block, axis, [(i, (i + step) % count) for i in range(count)])


def moved(block, axis, step):
    count = lax.axis_size(axis)
    pairs = [(i, i + step) for i in range(count) if 0 <= i + step < count]
    return lax.ppermute(block, axis, pairs)


def grid_shifted(block, axes, steps):
    sizes = [lax.axis_size(a) for a in axes]
    pairs = []
    for source in range(sizes[0] * sizes[1]):
        first, second = divmod(source, sizes[1])
        target = ((first + steps[0]) % sizes[0]) * sizes[1] + (second + steps[1]) % sizes[1]
        pairs.append((source, target))
    return lax.ppermute(block, axes, pairs)


def ordered(by_step, index):
    count = len(by_step)
    result = []
    for owner in range(count):
        back = lax.rem(index - owner + count, count)
        block = by_step[0]
        for step in range(1, count):
            block = jnp.where(back == step, by_step[step], block)
        result.append(block)
    return result


def extended(block, axis, width):
    low = moved(block[-width:], axis, 1)
    high = moved(block[:width], axis, -1)
    return jnp.concatenate([low, block, high], axis=0)


def conv_rows(padded, kernel, length):
    summed = padded[0:length] * kernel[0]
    for offset in range(1, kernel.shape[0]):
        summed = summed + padded[offset : offset + length] * kernel[offset]
    return summed


def bdot(pattern, one, two):
    return jnp.einsum(pattern, one, two, preferred_element_type=jnp.float32)


def pack(decay, state):
    heads, width, depth = state.shape
    rows = jnp.broadcast_to(decay[:, None, None], (heads, 16, depth)).astype(jnp.bfloat16)
    return jnp.concatenate([state.astype(jnp.bfloat16), rows], axis=1)


def unpack(packed, width):
    body = packed.astype(jnp.float32)
    return body[:, width, 0], body[:, :width]


def carried_in(decay, state, sign):
    width = state.shape[1]
    count = lax.axis_size(SP)
    own = pack(decay, state)
    index = lax.axis_index(SP)

    def from_back(array, step):
        back, value = unpack(moved(array, SP, sign * step), width)
        source = index - sign * step
        inside = (source >= 0) & (source < count)
        return jnp.where(inside, back, 1.0), value

    near, far = from_back(own, 1), from_back(own, 2)
    total = near[1] + near[0][:, None, None] * far[1]
    product = near[0] * far[0]
    covered = 2
    while covered < count - 1:
        back, value = from_back(pack(product, total), covered)
        total = total + product[:, None, None] * value
        product = product * back
        covered *= 2
    return total


def tied(value, *others):
    marks = [other[(slice(0, 1),) * other.ndim] for other in others]
    return lax.optimization_barrier((value, *marks))[0]


def shared_rows(weight, axis_dim, out_dim, mark):
    count = lax.axis_size("y")
    index = lax.axis_index("y")
    part = weight.shape[axis_dim] // count
    received = []
    for step in range(count):
        at = lax.rem(index + step, count) * part
        block = lax.dynamic_slice_in_dim(weight, at, part, axis_dim)
        received.append(shifted(block, "y", step) if step else block)
    received = [tied(block, mark) for block in received]
    return jnp.concatenate(ordered(received, index), axis=out_dim)


def shards(
    skip_trunk_vector,
    valve_preactivation,
    projected_heads_payload,
    cluster_ingests,
    cluster_observers,
    pre_softplus_increments,
    attenuation_ln_rate,
    additional_attenuation,
    payload_conv_weights,
    ingest_conv_weights,
    observer_conv_weights,
    valved_cluster_factor,
    closing_map_matrix,
    dense_standardize_factor,
    dense_valve_map,
    dense_payload_map,
    valve_series_smoother,
    payload_series_smoother,
    dense_contract_map,
):
    rows = skip_trunk_vector.shape[0]
    own_cols = skip_trunk_vector.shape[1]
    head_count = pre_softplus_increments.shape[2]
    per_group = HEADS // GROUPS
    nx, nc, ny = lax.axis_size("x"), lax.axis_size("core"), lax.axis_size("y")
    ix, ic, iy = lax.axis_index("x"), lax.axis_index("core"), lax.axis_index("y")

    joined = jnp.concatenate([projected_heads_payload, cluster_ingests, cluster_observers], axis=1)
    taps_all = jnp.concatenate(
        [payload_conv_weights, ingest_conv_weights, observer_conv_weights], axis=1
    )
    padded = extended(joined, SP, taps_all.shape[0] // 2)

    convolved = jax.nn.silu(conv_rows(padded.astype(jnp.float32), taps_all, rows)).astype(
        jnp.bfloat16
    )
    gate_w = lax.all_gather(shared_rows(dense_valve_map, 1, 0, convolved), "z", axis=0, tiled=True)
    value_w = lax.all_gather(
        shared_rows(dense_payload_map, 1, 0, convolved), "z", axis=0, tiled=True
    )

    payload_columns = projected_heads_payload.shape[1]
    input_cols = cluster_ingests.shape[1]
    width = payload_columns // head_count
    groups = input_cols // STATE
    values = convolved[:, :payload_columns]
    inputs_g = convolved[:, payload_columns : payload_columns + input_cols].reshape(
        rows, groups, STATE
    )
    readout_g = convolved[:, payload_columns + input_cols :].reshape(rows, groups, STATE)

    steps = jax.nn.softplus(pre_softplus_increments)
    logs = additional_attenuation - steps * jnp.exp(attenuation_ln_rate)[:, None, :]
    running = jnp.cumsum(logs, axis=1)
    run_f = running[0]
    exc_b = running[1] - logs[1]
    total_f, total_b = running[0, -1], running[1, -1]

    end_f = jnp.exp(total_f[None] - run_f) * steps[0]
    end_b = jnp.exp(exc_b) * steps[1]
    ends = jnp.stack([end_f, end_b], axis=1)
    scaled = (
        ends[:, :, :, None] * values.astype(jnp.float32).reshape(rows, 1, head_count, width)
    ).astype(jnp.bfloat16)
    scaled = scaled.reshape(rows, 2, groups, per_group, width)
    summary = bdot("sdgep,sgn->dgepn", scaled, inputs_g).reshape(2, head_count, width, STATE)
    in_f = carried_in(jnp.exp(total_f), summary[0], 1)
    in_b = carried_in(jnp.exp(total_b), summary[1], -1)

    down_part = shared_rows(dense_contract_map, 0, 1, in_f)
    down_w = lax.all_gather(down_part, "z", axis=1, tiled=True)

    places = jnp.arange(rows, dtype=jnp.int32)
    after = places[:, None] > places[None, :]
    same = places[:, None] == places[None, :]
    run_fT, exc_bT = run_f.T, exc_b.T
    step_f, step_b = steps[0].T, steps[1].T
    gaps = jnp.where(
        after[None],
        run_fT[:, :, None] - run_fT[:, None, :],
        exc_bT[:, None, :] - exc_bT[:, :, None],
    )
    factor = jnp.where(
        after[None],
        step_f[:, None, :],
        jnp.where(same[None], (step_f + step_b)[:, None, :], step_b[:, None, :]),
    )
    scores = jnp.repeat(bdot("tgn,sgn->gts", readout_g, inputs_g), per_group, axis=0)
    weights = (scores * jnp.exp(gaps) * factor).astype(jnp.bfloat16)
    within = bdot("hts,shp->thp", weights, values.reshape(rows, head_count, width))

    def outer(state):
        grouped = state.astype(jnp.bfloat16).reshape(groups, per_group, width, STATE)
        return bdot("gepn,tgn->tgep", grouped, readout_g).reshape(rows, head_count, width)

    mixed = within + outer(in_f) * jnp.exp(run_f)[:, :, None]
    mixed = mixed + outer(in_b) * jnp.exp(total_b[None] - exc_b)[:, :, None]
    gated = mixed.reshape(rows, payload_columns) * jax.nn.silu(
        valve_preactivation.astype(jnp.float32)
    )
    grouped = gated.reshape(rows, groups, per_group * width)
    standardized = grouped * lax.rsqrt(jnp.mean(grouped * grouped, axis=2, keepdims=True) + EPSILON)
    blended = (standardized.reshape(rows, payload_columns) * valved_cluster_factor).astype(
        jnp.bfloat16
    )

    def column_block(matrix, dx, dc):
        at = (lax.rem(ix + dx, nx) * nc + lax.rem(ic + dc, nc)) * own_cols
        return lax.dynamic_slice_in_dim(matrix, at, own_cols, 1)

    def over_cores(terms):
        total = terms[0].astype(jnp.bfloat16).astype(jnp.float32)
        for dc in range(1, nc):
            total = total + shifted(terms[dc].astype(jnp.bfloat16), "core", dc).astype(jnp.float32)
        return total

    mapped = None
    for dx in list(range(1, nx)) + [0]:
        terms = [
            jnp.dot(
                blended,
                column_block(closing_map_matrix, dx, dc),
                preferred_element_type=jnp.float32,
            )
            for dc in range(nc)
        ]
        part = over_cores(terms)
        if dx:
            part = shifted(part.astype(jnp.bfloat16), "x", dx).astype(jnp.float32)
        mapped = part if mapped is None else mapped + part
    middle = (skip_trunk_vector.astype(jnp.float32) + mapped).astype(jnp.bfloat16)

    margin = valve_series_smoother.shape[0] // 2
    room = -(-margin // 16) * 16
    low = moved(middle[-margin:], SP, 1)
    high = moved(middle[:margin], SP, -1)
    blank = jnp.zeros((room - margin, own_cols), middle.dtype)
    wide = jnp.concatenate([blank, low, middle, high, blank], axis=0)

    def everywhere(block):
        by_y = []
        for dy in range(ny):
            by_x = []
            for dx in range(nx):
                got = grid_shifted(block, ("y", "x"), (dy, dx)) if dy or dx else block
                by_core = [got] + [shifted(got, "core", dc) for dc in range(1, nc)]
                by_x.append(jnp.concatenate(ordered(by_core, ic), axis=1))
            by_y.append(jnp.concatenate(ordered(by_x, ix), axis=1))
        return jnp.stack(ordered(by_y, iy))

    line = everywhere(wide).reshape(ny * (rows + 2 * room), -1).astype(jnp.float32)
    inverse = lax.rsqrt(jnp.mean(line * line, axis=1, keepdims=True) + EPSILON)
    normed = (line * inverse * dense_standardize_factor).astype(jnp.bfloat16)

    hidden_cols = gate_w.shape[1]
    gate_taps = lax.dynamic_slice_in_dim(valve_series_smoother, iy * hidden_cols, hidden_cols, 1)
    value_taps = lax.dynamic_slice_in_dim(payload_series_smoother, iy * hidden_cols, hidden_cols, 1)

    def spread(weight, taps):
        made = jnp.dot(normed, weight, preferred_element_type=jnp.float32).astype(jnp.bfloat16)
        made = made.reshape(ny, rows + 2 * room, hidden_cols).astype(jnp.float32)
        summed = None
        for offset in range(taps.shape[0]):
            start = room - margin + offset
            term = made[:, start : start + rows] * taps[offset]
            summed = term if summed is None else summed + term
        return summed

    gate_rows = spread(gate_w, gate_taps)
    value_rows = spread(value_w, value_taps)
    hidden = (jax.nn.silu(gate_rows) * value_rows).astype(jnp.bfloat16)

    order = [(dy, dx) for dy in range(ny) for dx in range(nx)]
    down = None
    for dy, dx in order[1:] + order[:1]:
        wanted = lax.dynamic_index_in_dim(hidden, lax.rem(iy + dy, ny), 0, keepdims=False)
        terms = [
            jnp.dot(wanted, column_block(down_w, dx, dc), preferred_element_type=jnp.float32)
            for dc in range(nc)
        ]
        part = over_cores(terms)
        if dy or dx:
            part = grid_shifted(part.astype(jnp.bfloat16), ("y", "x"), (dy, dx)).astype(jnp.float32)
        down = part if down is None else down + part
    return (middle.astype(jnp.float32) + down).astype(jnp.bfloat16)


MESH = pl.DeviceIdType.MESH
BF = jnp.bfloat16
F32 = jnp.float32


def dot(one, two, dims=((1,), (0,)), precision=None):
    return lax.dot_general(
        one, two, (dims, ((), ())), preferred_element_type=F32, precision=precision
    )


def layer(
    loads,
    skip,
    valve,
    payload,
    ingest,
    observe,
    pre,
    rate,
    extra,
    taps_p,
    taps_i,
    taps_o,
    gain,
    closing,
    norm_gain,
    gate_w,
    value_w,
    gate_taps,
    value_taps,
    down_w,
    out,
    halo,
    wide,
    conv,
    run_s,
    exc_s,
    run_t,
    exc_t,
    step_t,
    ends,
    scaled,
    sum_f,
    sum_h,
    sum_y,
    totals,
    plane_out,
    plane_in,
    carry,
    carry_all,
    entering,
    scores,
    mixed,
    blend,
    mid_own,
    close_all,
    rows_n,
    wg,
    wv,
    wd,
    made_g,
    made_v,
    hidden,
    part,
    part_f,
    part_in,
    own_sum,
    far_in,
    halo_s,
    halo_r,
    tp_s,
    tp_r,
    w_s,
    w_r,
    w_y,
    w_fwd,
    cl_s,
    cl_r,
    tot_s,
    tot_r,
    sy_s,
    sy_r,
    pl_s,
    pl_r,
    ca_s,
    ca_r,
    nb_s,
    nb_r,
    nf_s,
    nf_r,
    edge_s,
    edge_r,
    core_s,
    core_r,
    own_s,
    own_r,
    local,
):
    nz, ny, nx, nc = (lax.axis_size(a) for a in ("z", "y", "x", "core"))
    z, y, x, c = (lax.axis_index(a) for a in ("z", "y", "x", "core"))
    place, lane_at = z * ny + y, x * nc + c
    rows, cols = skip.shape
    width_all = blend.shape[1]
    heads = pre.shape[1]
    groups = ingest.shape[1] // STATE
    per = heads // groups
    head_w = payload.shape[1] // heads
    gw = per * head_w
    hid = wg.shape[1]
    kb = gate_w.shape[0]
    ob = down_w.shape[1]
    tile = 16
    other_y, other_x, other_c = (z, 1 - y, x, c), (z, y, 1 - x, c), (z, y, x, 1 - c)
    half = z // 2
    near = z * (1 - 2 * half) + (nz - 1) * half
    middle = (z > 0) & (z < nz - 1)

    def remote(src, dst, send, recv, to):
        return pltpu.make_async_remote_copy(
            src_ref=src,
            dst_ref=dst,
            send_sem=send,
            recv_sem=recv,
            device_id=to,
            device_id_type=MESH,
        )

    for load in loads:
        load.start()
    barrier = pltpu.get_barrier_semaphore()
    greeted = 0
    for k in range(1, nz * ny):
        to = (lax.rem(z + k // ny, nz), lax.rem(y + k % ny, ny), x, c)
        pl.semaphore_signal(barrier, inc=1, device_id=to, device_id_type=MESH)
        greeted += 1
    for k in range(1, nx * nc):
        for dy in range(ny):
            to = (z, lax.rem(y + dy, ny), lax.rem(x + k // nc, nx), lax.rem(c + k % nc, nc))
            pl.semaphore_signal(barrier, inc=1, device_id=to, device_id_type=MESH)
            greeted += 1
    pl.semaphore_wait(barrier, greeted)
    for load in loads:
        load.wait()

    pieces = []
    at = 0
    for source in (payload, ingest, observe):
        pieces.append((source, at, source.shape[1]))
        at += source.shape[1]

    def halo_copy(side, i):
        source, start, size = pieces[i]
        other = place + 1 if side == 0 else place - 1
        to = (other // ny, lax.rem(other + ny, ny), x, c)
        src = source.at[pl.ds(rows - tile, tile)] if side == 0 else source.at[pl.ds(0, tile)]
        return remote(
            src,
            halo.at[side, :, pl.ds(start, size)],
            halo_s.at[side, i],
            halo_r.at[side, i],
            to,
        )

    last = nz * ny - 1

    @pl.when(place < last)
    def _():
        for i in range(3):
            halo_copy(0, i).start()

    @pl.when(place > 0)
    def _():
        for i in range(3):
            halo_copy(1, i).start()

    def column(ref, to_y, matrix):
        at = pl.multiple_of(to_y * hid, 128)
        if matrix == 2:
            return ref.at[pl.ds(at, hid), :]
        return ref.at[:, pl.ds(at, hid)]

    given = (gate_w, value_w, down_w)

    def landing(matrix, index):
        if matrix == 2:
            return wd.at[index]
        return (wg, wv)[matrix].at[pl.ds(pl.multiple_of(index * kb, kb), kb), :]

    beside = z * ny + 1 - y

    def weight_y(matrix):
        return remote(
            column(given[matrix], 1 - y, matrix),
            landing(matrix, place),
            w_y.at[matrix],
            w_r.at[matrix, place],
            other_y,
        )

    def weight_arrival(matrix, index):
        return remote(
            landing(matrix, index),
            landing(matrix, index),
            w_y.at[matrix],
            w_r.at[matrix, index],
            other_y,
        )

    def weight_copy(matrix, to_z, passed):
        index = beside if passed else place
        source = landing(matrix, index) if passed else column(given[matrix], y, matrix)
        return remote(
            source,
            landing(matrix, index),
            w_s.at[matrix, to_z * ny + passed],
            w_r.at[matrix, index],
            (to_z, y, x, c),
        )

    def weight_relay(matrix, distance, passed, side):
        sign = 1 - 2 * side
        index = (z - sign * distance) * ny + (1 - y if passed else y)
        return remote(
            landing(matrix, index),
            landing(matrix, index),
            w_fwd.at[matrix, (distance - 1) * 4 + passed * 2 + side],
            w_r.at[matrix, index],
            (z + sign, y, x, c),
        )

    def relays(distance, side):
        sign = 1 - 2 * side
        source, to = z - sign * distance, z + sign
        return (source >= 0) & (source < nz) & (to >= 0) & (to < nz)

    def waits(to):
        return middle & (x == half) & ((to == 0) | (to == nz - 1))

    def send_weights(matrix, passed, do, kept=None):
        for sign in (1, -1):
            to = z + sign
            goes = (to >= 0) & (to < nz)
            if kept is not None:
                goes = goes & (waits(to) if kept else jnp.logical_not(waits(to)))

            @pl.when(goes)
            def _():
                do(weight_copy(matrix, to, passed))

    def start(copy):
        copy.start()

    def pass_weights(matrix):
        weight_arrival(matrix, beside).wait_recv()
        send_weights(matrix, 1, start)

    def relay_weights(matrix, distance, passed):
        for side in range(2):

            @pl.when(relays(distance, side))
            def _():
                source = z - distance if side == 0 else z + distance
                weight_arrival(matrix, source * ny + (1 - y if passed else y)).wait_recv()
                weight_relay(matrix, distance, passed, side).start()

    def own_copy(matrix):
        return pltpu.make_async_copy(
            column(given[matrix], y, matrix), landing(matrix, place), local.at[matrix]
        )

    def await_weights(matrix, to_z):
        for to_y in range(ny):

            @pl.when((to_z != z) & jnp.logical_not(middle))
            def _():
                weight_arrival(matrix, to_z * ny + to_y).wait_recv()

    def tp_index(k):
        return lax.rem(x + k // nc, nx), lax.rem(c + k % nc, nc)

    def close_copy(k):
        to_x, to_c = tp_index(k)
        at = pl.ds(pl.multiple_of((to_x * nc + to_c) * cols, 128), cols)
        return remote(
            closing.at[:, at], close_rows(lane_at), cl_s.at[k], cl_r.at[k], (z, y, to_x, to_c)
        )

    def close_rows(index):
        return close_all.at[pl.ds(pl.multiple_of(index * cols, cols), cols), :]

    def close_arrival(k):
        at_x, at_c = tp_index(k)
        view = close_rows(at_x * nc + at_c)
        return remote(view, view, cl_s.at[k], cl_r.at[k], other_c)

    side_x = (1 - x) * nc + c

    def blend_view(g, index):
        return blend.at[:, pl.ds(pl.multiple_of(index * cols + g * gw, 128), gw)]

    def tp_copy(g, which):
        view = blend_view(g, (lane_at, lane_at, side_x)[which])
        to = (other_x, other_c, other_c)[which]
        return remote(view, view, tp_s.at[g, which], tp_r.at[g, which], to)

    def tp_arrival(g, which):
        view = blend_view(g, (side_x, x * nc + 1 - c, (1 - x) * nc + 1 - c)[which])
        return remote(view, view, tp_s.at[g, which], tp_r.at[g, which], other_c)

    weight_y(0).start()
    for matrix in range(2):
        send_weights(matrix, 0, start)
    for k in (2, 3, 1):
        close_copy(k).start()
    for matrix in range(3):
        own_copy(matrix).start()
    close_own = pltpu.make_async_copy(
        closing.at[:, pl.ds(pl.multiple_of(lane_at * cols, 128), cols)],
        close_rows(lane_at),
        local.at[3],
    )
    close_own.start()

    edge = wide.shape[0] - tile
    for source, start_at, size in pieces:
        wide[tile : tile + rows, start_at : start_at + size] = source[...].astype(F32)

    @pl.when(place > 0)
    def _():
        for i in range(3):
            halo_copy(0, i).wait_recv()
        wide[0:tile, :] = halo[0].astype(F32)

    @pl.when(place == 0)
    def _():
        wide[0:tile, :] = jnp.zeros((tile, wide.shape[1]), F32)

    @pl.when(place < last)
    def _():
        for i in range(3):
            halo_copy(1, i).wait_recv()
        wide[edge:, :] = halo[1].astype(F32)

    @pl.when(place == last)
    def _():
        wide[edge:, :] = jnp.zeros((tile, wide.shape[1]), F32)

    margin = taps_p.shape[0] // 2
    for (source, start_at, size), taps in zip(pieces, (taps_p, taps_i, taps_o)):

        def conv_columns(i, carried, start_at=start_at, taps=taps):
            into = pl.ds(pl.multiple_of(start_at + i * 128, 128), 128)
            tap = taps[:, pl.ds(pl.multiple_of(i * 128, 128), 128)]
            for r in range(0, rows, 128):
                summed = None
                for k in range(tap.shape[0]):
                    first = tile - margin + k + r
                    term = wide[first : first + 128, into] * tap[k : k + 1]
                    summed = term if summed is None else summed + term
                conv[r : r + 128, into] = jax.nn.silu(summed).astype(BF)
            return carried

        lax.fori_loop(0, size // 128, conv_columns, 0)

    def upright(row):
        shape = (heads, heads)
        same = lax.broadcasted_iota(jnp.int32, shape, 0) == lax.broadcasted_iota(
            jnp.int32, shape, 1
        )
        return jnp.sum(
            jnp.where(same, jnp.broadcast_to(row, shape), 0.0), axis=1, keepdims=True
        )

    def turned(array):
        blank = jnp.zeros((128 - 2 * heads, rows), F32)
        return jnp.concatenate([array, blank], axis=0).T

    raw = jnp.concatenate([pre[0], pre[1]], axis=0)
    steps_t = jnp.maximum(raw, 0.0) + jnp.log1p(jnp.exp(-jnp.abs(raw)))
    rates = jnp.exp(jnp.concatenate([upright(rate[0:1]), upright(rate[1:2])], axis=0))
    logs_t = jnp.concatenate([extra[0], extra[1]], axis=0) - steps_t * rates
    earlier = lax.broadcasted_iota(jnp.int32, (rows, rows), 0) <= lax.broadcasted_iota(
        jnp.int32, (rows, rows), 1
    )
    running_t = dot(logs_t, earlier.astype(F32), precision=lax.Precision.HIGHEST)
    before_t = running_t - logs_t
    run_t[...] = running_t
    exc_t[...] = before_t
    step_t[...] = steps_t
    running, before, steps = turned(running_t), turned(before_t), turned(steps_t)
    run_s[...] = running
    exc_s[...] = before
    whole = running[rows - 1 : rows]
    lane = lax.broadcasted_iota(jnp.int32, (rows, 128), 1)
    ends[...] = jnp.exp(jnp.where(lane < heads, whole - running, before)) * steps
    totals[place] = jnp.broadcast_to(whole, (8, 128))

    def spread(columns, first):
        low = lax.broadcasted_iota(jnp.int32, (columns.shape[0], 2 * head_w), 1) < head_w
        shape = (columns.shape[0], 2 * head_w)
        return jnp.where(
            low,
            jnp.broadcast_to(columns[:, first : first + 1], shape),
            jnp.broadcast_to(columns[:, first + 1 : first + 2], shape),
        )

    def scale_rows(i, carried):
        at = pl.ds(pl.multiple_of(i * 128, 128), 128)
        factors = ends[at, :]
        for d in range(2):
            for p in range(heads // 2):
                into = slice(p * 2 * head_w, (p + 1) * 2 * head_w)
                made = conv[at, into].astype(F32) * spread(factors, d * heads + 2 * p)
                start_at = d * heads * head_w + p * 2 * head_w
                scaled[at, start_at : start_at + 2 * head_w] = made.astype(BF)
        return carried

    lax.fori_loop(0, rows // 128, scale_rows, 0)
    in_at = payload.shape[1]
    out_at = in_at + ingest.shape[1]
    for d in range(2):
        for g in range(groups):
            first = d * heads * head_w + g * gw
            state = dot(
                scaled[:, first : first + gw],
                conv[:, in_at + g * STATE : in_at + (g + 1) * STATE],
                ((0,), (0,)),
            )
            sum_f[d, g] = state
            sum_h[d, g] = state.astype(BF)

    state_y = remote(sum_h, sum_y, sy_s, sy_r, other_y)
    state_y.start()

    total_y = remote(totals.at[place], totals.at[place], tot_s, tot_r, other_y)
    total_y.start()
    pass_weights(0)
    weight_y(1).start()

    state_y.wait_recv()
    remote(totals.at[beside], totals.at[beside], tot_s, tot_r, other_y).wait_recv()

    def head_rows(ref_value, factors):
        return jnp.concatenate(
            [ref_value[e * head_w : (e + 1) * head_w] * factors[e] for e in range(per)], axis=0
        )

    def of_heads(row, d, g=None):
        result = []
        for e in range(per):
            picks = [
                row[:, d * heads + k * per + e : d * heads + k * per + e + 1] for k in range(groups)
            ]
            if g is None:
                result.append(jnp.where(y == 0, picks[0], picks[1]))
            else:
                result.append(picks[g])
        return result

    one_row = jnp.ones((1, 128), F32)
    plane_low = jnp.exp(totals[z * ny, 0:1])
    plane_high = jnp.exp(totals[z * ny + 1, 0:1])
    forward_own = of_heads(jnp.where(y == 0, plane_high, one_row), 0)
    forward_far = of_heads(jnp.where(y == 0, one_row, plane_high), 0)
    back_own = of_heads(jnp.where(y == 0, one_row, plane_low), 1)
    back_far = of_heads(jnp.where(y == 0, plane_low, one_row), 1)
    plane_out[0] = (
        head_rows(sum_f[0, y], forward_own) + head_rows(sum_y[0, y].astype(F32), forward_far)
    ).astype(BF)
    plane_out[1] = (
        head_rows(sum_f[1, y], back_own) + head_rows(sum_y[1, y].astype(F32), back_far)
    ).astype(BF)

    def plane_copy(d):
        to = z + 1 if d == 0 else z - 1
        return remote(
            plane_out.at[d], plane_in.at[d], pl_s.at[d], pl_r.at[d], (to, y, x, c)
        )

    plane_gone = plane_low * plane_high
    ranks = (z, nz - 1 - z)

    def take(d):
        plane_copy(d).wait_recv()
        carry[d] = plane_in[d].astype(F32)

    def hop(step):
        for d in range(2):

            @pl.when(ranks[d] == step)
            def _():
                if step:
                    take(d)
                    grown = head_rows(carry[d], of_heads(plane_gone, d))
                    plane_out[d] = (grown + plane_out[d].astype(F32)).astype(BF)
                plane_copy(d).start()

    carry[...] = jnp.zeros_like(carry)
    hop(0)

    weight_y(2).start()
    relay_weights(0, 1, 0)
    relay_weights(1, 1, 0)

    def within(g):
        read = conv[:, out_at + g * STATE : out_at + (g + 1) * STATE]
        write = conv[:, in_at + g * STATE : in_at + (g + 1) * STATE]
        scores[...] = dot(read, write, ((1,), (1,)))
        for p in range(per // 2):
            pair = g * per + 2 * p
            into = slice(pair * head_w, (pair + 2) * head_w)

            def chunk(i, carried):
                at = pl.ds(pl.multiple_of(i * 128, 128), 128)
                t = lax.broadcasted_iota(jnp.int32, (128, rows), 0) + i * 128
                s = lax.broadcasted_iota(jnp.int32, (128, rows), 1)
                after, same = t > s, t == s
                values = conv[:, into]
                low = lax.broadcasted_iota(jnp.int32, values.shape, 1) < head_w
                summed = None
                for e in range(2):
                    f, b = pair + e, heads + pair + e
                    gap = jnp.where(
                        after,
                        run_s[at, f : f + 1] - run_t[f : f + 1, :],
                        exc_t[b : b + 1, :] - exc_s[at, b : b + 1],
                    )
                    step_f, step_b = step_t[f : f + 1, :], step_t[b : b + 1, :]
                    factor = jnp.where(after, step_f, jnp.where(same, step_f + step_b, step_b))
                    made = (scores[at, :] * jnp.exp(gap) * factor).astype(BF)
                    kept = jnp.where(low if e == 0 else jnp.logical_not(low), values, 0)
                    term = dot(made, kept.astype(BF))
                    summed = term if summed is None else summed + term
                mixed[at, into] = summed
                return carried

            lax.fori_loop(0, rows // 128, chunk, 0)

    within(0)
    hop(1)
    pass_weights(1)
    within(1)
    for step in range(2, nz - 1):
        hop(step)
    for matrix in range(2):
        relay_weights(matrix, 2, 0)
    relay_weights(0, 1, 1)
    for d in range(2):

        @pl.when(ranks[d] == nz - 1)
        def _():
            take(d)

    for d in range(2):
        carry_all[d, y] = carry[d].astype(BF)

    def carry_copy(d):
        return remote(carry_all.at[d, y], carry_all.at[d, y], ca_s.at[d], ca_r.at[d], other_y)

    for d in range(2):
        carry_copy(d).start()


    for d in range(2):
        remote(
            carry_all.at[d, 1 - y], carry_all.at[d, 1 - y], ca_s.at[d], ca_r.at[d], other_y
        ).wait_recv()
    for g in range(groups):
        for d in range(2):
            through = plane_low if d == 0 else plane_high
            adds = y == 1 if d == 0 else y == 0
            weights = of_heads(jnp.where(adds, through, one_row), d, g)
            body = head_rows(carry_all[d, g].astype(F32), weights)
            entering[d, g] = (body + jnp.where(adds, sum_y[d, g].astype(F32), 0.0)).astype(BF)

    for g in range(groups):

        def finish(i, carried):
            at = pl.ds(pl.multiple_of(i * 128, 128), 128)
            read = conv[at, out_at + g * STATE : out_at + (g + 1) * STATE]
            fore = dot(read, entering[0, g], ((1,), (1,)))
            back = dot(read, entering[1, g], ((1,), (1,)))
            grown = jnp.exp(run_s[at, :])
            shrunk = jnp.exp(run_s[rows - 1 : rows, :] - exc_s[at, :])
            parts = []
            for p in range(per // 2):
                pair = g * per + 2 * p
                into = slice(pair * head_w, (pair + 2) * head_w)
                inner = slice(2 * p * head_w, 2 * (p + 1) * head_w)
                total = mixed[at, into] + fore[:, inner] * spread(grown, pair)
                total = total + back[:, inner] * spread(shrunk, heads + pair)
                parts.append(total * jax.nn.silu(valve[at, into].astype(F32)))
            gated = jnp.concatenate(parts, axis=1)
            mean = jnp.mean(gated * gated, axis=1, keepdims=True)
            made = gated * lax.rsqrt(mean + EPSILON) * gain[:, g * gw : (g + 1) * gw]
            blend[at, pl.ds(pl.multiple_of(lane_at * cols + g * gw, 128), gw)] = made.astype(BF)
            return carried

        lax.fori_loop(0, rows // 128, finish, 0)
        tp_copy(g, 0).start()
        tp_copy(g, 1).start()

    close_own.wait()
    for k in range(1, nx * nc):
        close_arrival(k).wait_recv()
    for g in range(groups):
        tp_arrival(g, 0).wait_recv()
        tp_copy(g, 2).start()
    for g in range(groups):
        tp_arrival(g, 1).wait_recv()
        tp_arrival(g, 2).wait_recv()

    def row_view(which_y, index):
        return rows_n.at[
            pl.ds(pl.multiple_of(tile + which_y * rows, tile), rows),
            pl.ds(pl.multiple_of(index * cols, 128), cols),
        ]

    relay_weights(1, 1, 1)
    made = dot(blend[...], close_all[...]) + skip[...].astype(F32)
    mid_own[...] = made.astype(BF)
    rows_n[
        pl.ds(pl.multiple_of(tile + y * rows, tile), rows),
        pl.ds(pl.multiple_of(lane_at * cols, 128), cols),
    ] = mid_own[...]

    other_xy = (z, 1 - y, 1 - x, c)
    froms = ((y, x), (y, 1 - x), (1 - y, x), (1 - y, 1 - x))

    def row_copy(k):
        view = row_view(y, lane_at)
        to = (other_c, other_x, other_y, other_xy)[k]
        return remote(view, view, nb_s.at[k], nb_r.at[k], to)

    def row_pass(k, core, arriving=False):
        view = row_view(froms[k][0], froms[k][1] * nc + core)
        sem = (nb_r if arriving else nf_r).at[k]
        return remote(view, view, nf_s.at[k], sem, other_c)

    for k in (1, 2, 3, 0):
        row_copy(k).start()
    for k in (1, 2, 3):
        row_pass(k, c, arriving=True).wait_recv()
        row_pass(k, c).start()
        if k == 1:
            relay_weights(0, 2, 1)
            relay_weights(1, 2, 1)
            send_weights(2, 0, start)
            weight_arrival(2, beside).wait_recv()
            send_weights(2, 1, start, kept=False)
    row_pass(0, 1 - c, arriving=True).wait_recv()
    for k in (1, 2, 3):
        row_pass(k, 1 - c).wait_recv()
    for k in range(4):
        row_copy(k).wait_send()
        if k:
            row_pass(k, c).wait_send()

    def normalize(i, carried):
        at = pl.ds(pl.multiple_of(tile + i * 128, tile), 128)
        squares = jnp.zeros((128, 1), F32)
        for first in range(0, width_all, 256):
            piece = rows_n[at, first : first + 256].astype(F32)
            squares = squares + jnp.sum(piece * piece, axis=1, keepdims=True)
        inverse = lax.rsqrt(squares / width_all + EPSILON)
        for first in range(0, width_all, 256):
            piece = rows_n[at, first : first + 256].astype(F32)
            piece = piece * inverse * norm_gain[:, first : first + 256]
            rows_n[at, first : first + 256] = piece.astype(BF)
        return carried

    lax.fori_loop(0, ny * rows // 128, normalize, 0)

    bottom = tile + ny * rows

    def edge_copy(side):
        if side == 0:
            src, dst = rows_n.at[pl.ds(bottom - tile, tile)], rows_n.at[pl.ds(0, tile)]
        else:
            src, dst = rows_n.at[pl.ds(tile, tile)], rows_n.at[pl.ds(bottom, tile)]
        to = (z + 1 if side == 0 else z - 1, y, x, c)
        return remote(src, dst, edge_s.at[side], edge_r.at[side], to)

    sends_up, sends_down = z < nz - 1, z > 0
    for side, cond in ((0, sends_up), (1, sends_down)):

        @pl.when(cond)
        def _():
            edge_copy(side).start()

    relay_weights(2, 1, 0)

    for matrix, (weight, made) in enumerate(((wg, made_g), (wv, made_v))):
        own_copy(matrix).wait()
        for k in range(nz):
            await_weights(matrix, k)

        def units(i, carried):
            at = pl.ds(pl.multiple_of(tile + i * rows, tile), rows)
            made[at, :] = dot(rows_n[at, :], weight[...]).astype(BF).astype(F32)
            return carried

        lax.fori_loop(0, ny, units, 0)

    relay_weights(2, 1, 1)
    relay_weights(2, 2, 0)

    @pl.when(z > 0)
    def _():
        edge_copy(0).wait_recv()

    @pl.when(z == 0)
    def _():
        rows_n[0:tile, :] = jnp.zeros((tile, width_all), BF)

    @pl.when(z < nz - 1)
    def _():
        edge_copy(1).wait_recv()

    @pl.when(z == nz - 1)
    def _():
        rows_n[bottom:, :] = jnp.zeros((tile, width_all), BF)

    both = jnp.concatenate([rows_n[0:tile, :], rows_n[bottom:, :]], axis=0)
    for weight, made in ((wg, made_g), (wv, made_v)):
        edges = dot(both, weight[...]).astype(BF).astype(F32)
        made[0:tile, :] = edges[0:tile]
        made[bottom:, :] = edges[tile:]

    ff_margin = gate_taps.shape[0] // 2

    def activate(i, carried):
        into = pl.ds(pl.multiple_of(i * 128, 128), 128)
        tap_at = pl.ds(pl.multiple_of(y * hid + i * 128, 128), 128)
        tap_g, tap_v = gate_taps[:, tap_at], value_taps[:, tap_at]
        for r in range(0, ny * rows, 128):
            pair = []
            for made, tap in ((made_g, tap_g), (made_v, tap_v)):
                summed = None
                for k in range(tap.shape[0]):
                    first = tile - ff_margin + k + r
                    term = made[first : first + 128, into] * tap[k : k + 1]
                    summed = term if summed is None else summed + term
                pair.append(summed)
            hidden[r : r + 128, into] = (jax.nn.silu(pair[0]) * pair[1]).astype(BF)
        return carried

    lax.fori_loop(0, hid // 128, activate, 0)

    own_copy(2).wait()

    def order(i):
        k = i % nz
        kept = near * (1 - 2 * k) + k if k < 2 else k
        if i >= nz and k:
            turn = (1 - near) * (1 - jnp.abs(x - half))
            kept = kept + turn * (k % (nz - 1) + 1 - k)
        return kept * (1 - 2 * half) + (nz - 1) * half

    def half_at(core):
        return pl.ds(pl.multiple_of(core * rows, tile), rows)

    def core_copy(i):
        return remote(
            part.at[i, half_at(1 - c)], part_in.at[i], core_s.at[i], core_r.at[i], other_c
        )

    def block_y(i):
        return y if i < nz else 1 - y

    def own_to(i):
        to_z = order(i)
        slot, q = y * nx + x, block_y(i)
        return remote(
            part.at[i, half_at(c)],
            far_in.at[slot, q],
            own_s.at[i],
            own_r.at[slot, q],
            (z, c, to_z // nc, lax.rem(to_z, nc)),
        )

    def stays(i):
        to_z = order(i)
        return (y == c) & (to_z // nc == x) & (lax.rem(to_z, nc) == c)

    count = nz * ny
    early = count // 2

    def settle(i):
        core_copy(i).wait_recv()

        @pl.when(stays(i))
        def _():
            own_sum[block_y(i)] = part_f[i % 2] + part_in[i].astype(F32)

        @pl.when(jnp.logical_not(stays(i)))
        def _():
            part[i, half_at(c)] = (part_f[i % 2] + part_in[i].astype(F32)).astype(BF)
            own_to(i).start()

    for i in range(count):
        to_z, to_y = order(i), block_y(i)
        index = to_z * ny + to_y
        if i >= early:
            settle(i - 1)
        if i == early:
            relay_weights(2, 2, 1)

        @pl.when((to_z != z) & jnp.logical_not(middle))
        def _():
            weight_arrival(2, index).wait_recv()

        made = dot(hidden[...], wd[index])

        for core in range(nc):

            @pl.when(c == core)
            def _():
                away = (1 - core) * rows
                part[i, away : away + rows] = made[away : away + rows].astype(BF)
                core_copy(i).start()
                part_f[i % 2] = made[core * rows : (core + 1) * rows]

        if 0 < i < early:
            settle(i - 1)
    settle(count - 1)
    for side in range(2):

        @pl.when(relays(nz - 2, side) & (x == half))
        def _():
            weight_relay(2, nz - 2, 1, side).wait_send()

    send_weights(2, 1, start, kept=True)

    def far_wait(slot, q):
        view = far_in.at[slot, q]
        remote(view, view, own_s.at[0], own_r.at[slot, q], other_c).wait_recv()

    own_slot = y * nx + x
    for q in range(ny):

        @pl.when(c != y)
        def _():
            far_wait(own_slot, q)
            own_sum[q] = far_in[own_slot, q].astype(F32)

    for q in range(ny):
        total = own_sum[q]
        for k in range(1, ny * nx):
            slot = lax.rem(y + k // nx, ny) * nx + lax.rem(x + k % nx, nx)
            far_wait(slot, q)
            total = total + far_in[slot, q].astype(F32)
        into = slice(q * ob, (q + 1) * ob)
        out[:, into] = (mid_own[:, into].astype(F32) + total).astype(BF)

    def done(copy):
        copy.wait_send()

    @pl.when(place < last)
    def _():
        for i in range(3):
            halo_copy(0, i).wait_send()

    @pl.when(place > 0)
    def _():
        for i in range(3):
            halo_copy(1, i).wait_send()

    for matrix in range(3):
        weight_y(matrix).wait_send()
        for passed in range(2):
            send_weights(matrix, passed, done)

        for distance in range(1, nz - 1):
            for passed in range(2):
                for side in range(2):

                    ended = (matrix, distance, passed) == (2, nz - 2, 1)

                    @pl.when(relays(distance, side) & ((x != half) if ended else True))
                    def _():
                        weight_relay(matrix, distance, passed, side).wait_send()

    for g in range(groups):
        for which in range(3):
            tp_copy(g, which).wait_send()
    for k in range(1, nx * nc):
        close_copy(k).wait_send()
    state_y.wait_send()
    total_y.wait_send()
    for d in range(2):

        @pl.when(ranks[d] < nz - 1)
        def _():
            plane_copy(d).wait_send()

    for d in range(2):
        carry_copy(d).wait_send()
    for side, cond in ((0, sends_up), (1, sends_down)):

        @pl.when(cond)
        def _():
            edge_copy(side).wait_send()

    for i in range(count):
        core_copy(i).wait_send()

        @pl.when(jnp.logical_not(stays(i)))
        def _():
            own_to(i).wait_send()


def one_kernel(*args):
    (skip, valve, payload, ingest, observe, pre, rate, extra, tp_taps, ti_taps, to_taps) = args[:11]
    gain, closing, norm_gain, gate_w, value_w, gate_taps, value_taps, down_w = args[11:]
    nz, ny, nx, nc = (lax.axis_size(a) for a in ("z", "y", "x", "core"))
    rows, cols = skip.shape
    width = norm_gain.shape[0]
    groups = ingest.shape[1] // STATE
    gw = payload.shape[1] // groups
    joined = payload.shape[1] + ingest.shape[1] + observe.shape[1]
    hid = gate_w.shape[1] // ny
    ob = down_w.shape[1]
    count = nz * ny
    lanes_used = 2 * pre.shape[2]
    tile = 16
    tall = ny * rows + 2 * tile
    vmem, anywhere = pl.BlockSpec(memory_space=pltpu.VMEM), pl.BlockSpec(memory_space=pl.ANY)
    v = pltpu.VMEM
    sem = pltpu.SemaphoreType.DMA
    scratch = [
        v((2, tile, joined), BF),
        v((rows + 2 * tile, joined), F32),
        v((rows, joined), BF),
        v((rows, 128), F32),
        v((rows, 128), F32),
        v((lanes_used, rows), F32),
        v((lanes_used, rows), F32),
        v((lanes_used, rows), F32),
        v((rows, 128), F32),
        v((rows, 2 * payload.shape[1]), BF),
        v((2, groups, gw, STATE), F32),
        v((2, groups, gw, STATE), BF),
        v((2, groups, gw, STATE), BF),
        v((count, 8, 128), F32),
        v((2, gw, STATE), BF),
        v((2, gw, STATE), BF),
        v((2, gw, STATE), F32),
        v((2, groups, gw, STATE), BF),
        v((2, groups, gw, STATE), BF),
        v((rows, rows), F32),
        v((rows, payload.shape[1]), F32),
        v((rows, width), BF),
        v((rows, cols), BF),
        v((width, cols), BF),
        v((tall, width), BF),
        v((width, hid), BF),
        v((width, hid), BF),
        v((count, hid, ob), BF),
        v((tall, hid), F32),
        v((tall, hid), F32),
        v((ny * rows, hid), BF),
        v((count, ny * rows, ob), BF),
        v((2, rows, ob), F32),
        v((count, rows, ob), BF),
        v((ny, rows, ob), F32),
        v((ny * nx, ny, rows, ob), BF),
        sem((2, 3)),
        sem((2, 3)),
        sem((groups, 3)),
        sem((groups, 3)),
        sem((3, count)),
        sem((3, count)),
        sem((3,)),
        sem((3, 4 * (nz - 2))),
        sem((nx * nc,)),
        sem((nx * nc,)),
        sem(()),
        sem(()),
        sem(()),
        sem(()),
        sem((2,)),
        sem((2,)),
        sem((2,)),
        sem((2,)),
        sem((4,)),
        sem((4,)),
        sem((4,)),
        sem((4,)),
        sem((2,)),
        sem((2,)),
        sem((count,)),
        sem((count,)),
        sem((count,)),
        sem((ny * nx, ny)),
        sem((4,)),
    ]
    operands = [
        *(skip, valve, payload, ingest, observe),
        *(jnp.swapaxes(pre, 1, 2), rate, jnp.swapaxes(extra, 1, 2)),
        *(tp_taps, ti_taps, to_taps, gain.reshape(1, -1), closing, norm_gain.reshape(1, -1)),
        *(gate_w, value_w, gate_taps, value_taps, down_w),
    ]
    staged = [i for i in range(len(operands)) if i not in (12, 14, 15, 18)]
    scratch += [v(operands[i].shape, operands[i].dtype) for i in staged]
    scratch.append(sem((len(staged),)))

    def entry(*refs):
        ins, rest = list(refs[: len(operands)]), refs[len(operands) :]
        held, arrived = rest[-len(staged) - 1 : -1], rest[-1]
        loads = []
        for k, i in enumerate(staged):
            loads.append(pltpu.make_async_copy(ins[i], held[k], arrived.at[k]))
            ins[i] = held[k]
        layer(loads, *ins, *rest[: -len(staged) - 1])

    flops = 2 * rows * width * (width + 3 * hid * ny)
    return pl.pallas_call(
        entry,
        out_shape=jax.ShapeDtypeStruct((rows, cols), BF),
        in_specs=[anywhere] * len(operands),
        out_specs=vmem,
        scratch_shapes=scratch,
        compiler_params=pltpu.CompilerParams(
            collective_id=0, has_side_effects=True, vmem_limit_bytes=67043328
        ),
        cost_estimate=pl.CostEstimate(flops=flops, bytes_accessed=2**24, transcendentals=0),
        name="layer",
    )(*operands)


def body_for(grid):
    sizes = tuple(grid.shape[a] for a in ("z", "y", "x", "core"))
    return one_kernel if sizes == (4, 2, 2, 2) else shards


def solution(mesh):
    sp, tp = mesh.shape["sp"], mesh.shape["tp"]
    ny = 2 ** (int(math.log2(sp)) // 2)
    nc = 2 if tp % 2 == 0 else 1
    grid = Mesh(
        mesh.devices.reshape(sp // ny, ny, tp // nc, nc), ("z", "y", "x", "core")
    )
    return jax.shard_map(
        body_for(grid),
        mesh=grid,
        in_specs=(
            P(SP, TP),
            P(SP, TP),
            P(SP, TP),
            P(SP, TP),
            P(SP, TP),
            P(None, SP, TP),
            P(None, TP),
            P(None, SP, TP),
            P(None, TP),
            P(None, TP),
            P(None, TP),
            P(TP),
            P(TP, None),
            P(),
            P(SP, TP),
            P(SP, TP),
            P(None, TP),
            P(None, TP),
            P(TP, SP),
        ),
        out_specs=P(SP, TP),
        check_vma=False,
    )
```
